512 devices in a mesh: dp: 4 (over x), kv: 64 (over z, y), tp: 2 (over core).
Axes of the slice: x: 4, y: 4, z: 16, core: 2. Of those that a mesh axis runs over, the one named last changes fastest.
Arguments:
- tokens: bfloat16 [65536, 4096], P(('dp', 'kv')), parts along dimension 0, may hold values from -16 to 16
- query_weight: bfloat16 [4096, 1024], P('kv', 'tp'), may hold values from -0.09375 to 0.09375
- key_weight: bfloat16 [4096, 256], P('kv', 'tp'), may hold values from -0.09375 to 0.09375
- value_weight: bfloat16 [4096, 256], P('kv', 'tp'), may hold values from -0.09375 to 0.09375
- out_weight: bfloat16 [1024, 4096], P('kv', 'tp'), may hold values from -1.5 to 1.5
- chosen: int32 [2048, 16], P(('dp', 'kv')), parts along dimension 0, may hold values from -1 to 511, as said below
- live_length: int32 [4], P('dp'), parts along dimension 0, may hold values from 2048 to 16384
Outputs:
- mixed: bfloat16 [65536, 4096], P(('dp', 'kv'), 'tp'), parts along dimension 0
The draws below stay inside these ranges and needn't reach their ends.
There are 4 independent parts, one for each index of `dp`. The reference program is written for one: setup_inputs(seed, part) draws one part's arguments, and reference() takes and returns one part's arrays. A program takes and returns all parts, laid end to end along the dimension named above; an argument that names none is the same for every part. Nothing has to cross between parts.
Inputs may be any that keep to these rules, and one draw needn't show every extreme that they name: `chosen`: row j lists 16 entries: entry 0 is j itself, the others are distinct blocks before j, or -1 for unused entries. The query blocks of one device together read at most 2 distinct blocks held by any one other device, and some device reads 2 of another's in every draw.
All inputs are finite; a program needn't handle non-finite values.
Results may differ from the reference program's by a relative error of at most 0.0085.
Values may be sent and summed in bfloat16 or wider, within the bound.
No kernel may reach another device: no remote copies, remote signals or barrier semaphores. Data moves between devices by JAX's collectives and lax.ppermute only.
A program may use at most 64 MiB of HBM per device.

```python
import jax
import jax.numpy as jnp
from jax import lax

D = 4096
HEADS = 8
KV_HEADS = 2
HD = 128
BLOCK = 32
NSEL = 16
CAP = 2
TOK_DEV = 256
TOKENS = 16384
SEGMENT_TOTAL = 512
Q_WIDTH = 1024
KV_WIDTH = 256
N_KV = 64


def draw_tokens(key, part):
    normal_draw = jax.random.normal(key, (TOKENS, D), jnp.float32)
    return jnp.clip(normal_draw, -6.0, 6.0).astype(jnp.bfloat16)


def draw_chosen(key, part):
    owners = TOKENS // TOK_DEV
    per_dev = TOK_DEV // BLOCK
    pick_key = jax.random.fold_in(key, 11)
    noise_key = jax.random.fold_in(key, 13)
    pick_scores = jax.random.randint(pick_key, (owners, owners, per_dev), 0, 1 << 20)
    local_ids = jnp.arange(per_dev, dtype=jnp.int32)
    order = jnp.argsort(pick_scores * per_dev + local_ids[None, None, :], axis=-1, stable=True)
    allowed_local = order[..., :CAP]
    allowed = jnp.any(local_ids[None, None, None, :] == allowed_local[..., None], axis=2)
    allowed = allowed.reshape(owners, SEGMENT_TOTAL)
    stream_segments = jnp.arange(SEGMENT_TOTAL, dtype=jnp.int32)
    segment_loader = stream_segments // per_dev
    segment_retainer = stream_segments // per_dev
    remote_segment = allowed[segment_loader] & (segment_retainer[None, :] < segment_loader[:, None])
    local = (segment_retainer[None, :] == segment_loader[:, None]) & (stream_segments[None, :] < stream_segments[:, None])
    eligible_filter = remote_segment | local
    rating_increment = jnp.where(remote_segment & (segment_retainer[None, :] == 0), 2, jnp.where(remote_segment & (segment_retainer[None, :] == segment_loader[:, None] - 1), 1, 0))
    stochastic_perturbation = jax.random.randint(noise_key, (SEGMENT_TOTAL, SEGMENT_TOTAL), 0, 1 << 12)
    segment_rating = jnp.where(eligible_filter, (stochastic_perturbation + rating_increment * (1 << 12)) * SEGMENT_TOTAL + stream_segments[None, :], -1)
    values, indices = lax.top_k(segment_rating, NSEL - 1)
    picks = jnp.where(values >= 0, indices, -1).astype(jnp.int32)
    return jnp.concatenate([stream_segments[:, None], picks], axis=1).astype(jnp.int32)


def level_of(rng, shape, split, least, high):
    def one(axis_at, parts):
        draws = jax.random.uniform(jax.random.fold_in(jax.random.fold_in(rng, 6), axis_at), (parts,), jnp.float32, least / len(split), high / len(split))
        return jnp.repeat(jnp.exp(draws), shape[axis_at] // parts).reshape((-1,) + (1,) * (len(shape) - axis_at - 1))

    loudness = one(*split[0])
    for cut in split[1:]:
        loudness = loudness * one(*cut)
    return loudness


def scatter_about(key, extent, width, bound, split=(), held_as=jnp.bfloat16):
    values = jax.random.normal(key, extent, jnp.float32) * width
    if len(split) > 0:
        values = level_of(key, extent, split, -0.22, 0.18) * values
    return jnp.clip(values, min=-bound, max=bound).astype(held_as)


def setup_inputs(seed: int = 0, part: int = 0) -> dict:
    key_list = jax.random.split(jax.random.key(seed), 8)
    part_splits = jax.random.split(jax.random.fold_in(key_list[7], part), 8)
    return {
        "tokens": draw_tokens(jax.random.fold_in(jax.random.fold_in(key_list[7], part), 71), part),
        "query_weight": scatter_about(key_list[1], (D, Q_WIDTH), D ** -0.5, 0.09375, ((0, 64), (1, 2))),
        "key_weight": scatter_about(key_list[2], (D, KV_WIDTH), D ** -0.5, 0.09375, ((0, 64), (1, 2))),
        "value_weight": scatter_about(key_list[3], (D, KV_WIDTH), D ** -0.5, 0.09375, ((0, 64), (1, 2))),
        "out_weight": scatter_about(key_list[4], (Q_WIDTH, D), (Q_WIDTH // 64) ** -0.5, 1.5, ((0, 64), (1, 2))),
        "chosen": draw_chosen(jax.random.fold_in(jax.random.fold_in(key_list[7], part), 71), part),
        "live_length": jax.random.randint(part_splits[6], (1,), TOKENS // 8, TOKENS + 1).astype(jnp.int32),
    }


def reference(tokens, query_weight, key_weight, value_weight, out_weight, chosen, live_length):
    queries = jnp.dot(tokens, query_weight, preferred_element_type=jnp.float32).astype(jnp.bfloat16)
    keys = jnp.dot(tokens, key_weight, preferred_element_type=jnp.float32).astype(jnp.bfloat16)
    values = jnp.dot(tokens, value_weight, preferred_element_type=jnp.float32).astype(jnp.bfloat16)
    groups = HEADS // KV_HEADS
    per_dev = TOK_DEV // BLOCK
    key_blocks = keys.reshape(SEGMENT_TOTAL, BLOCK, KV_HEADS, HD)
    value_blocks = values.reshape(SEGMENT_TOTAL, BLOCK, KV_HEADS, HD)
    query_parts = queries.reshape(N_KV, per_dev, BLOCK, KV_HEADS, groups, HD)
    chosen_parts = chosen.reshape(N_KV, per_dev, NSEL)
    firsts = (jnp.arange(N_KV) * per_dev).astype(jnp.int32)
    limit = live_length[0]

    def attend(item):
        q_part, picks, first = item
        valid = picks >= 0
        safe = jnp.maximum(picks, 0)
        near_keys = key_blocks[safe].astype(jnp.float32)
        near_values = value_blocks[safe].astype(jnp.float32)
        scores = jnp.einsum("jqkgd,jnbkd->jkgqnb", q_part.astype(jnp.float32), near_keys) * (HD ** -0.5)
        query_pos = (first + jnp.arange(per_dev, dtype=jnp.int32))[:, None] * BLOCK + jnp.arange(BLOCK, dtype=jnp.int32)[None, :]
        key_pos = safe[:, :, None] * BLOCK + jnp.arange(BLOCK, dtype=jnp.int32)[None, None, :]
        allowed = valid[:, None, :, None] & (key_pos[:, None, :, :] <= query_pos[:, :, None, None])
        masked = jnp.where(allowed[:, None, None], scores, -jnp.inf)
        top = jnp.max(masked, axis=(4, 5), keepdims=True)
        weights = jnp.exp(masked - top)
        total = jnp.sum(weights, axis=(4, 5))
        rounded = lax.optimization_barrier(weights.astype(jnp.bfloat16)).astype(jnp.float32)
        summed = jnp.einsum("jkgqnb,jnbkd->jqkgd", rounded, near_values)
        result = summed / jnp.transpose(total, (0, 3, 1, 2))[..., None]
        live = query_pos < limit
        result = jnp.where(live[:, :, None, None, None], result, 0.0)
        return result.astype(jnp.bfloat16)

    attended = lax.map(attend, (query_parts, chosen_parts, firsts)).reshape(TOKENS, Q_WIDTH)
    return jnp.dot(attended, out_weight, preferred_element_type=jnp.float32).astype(jnp.bfloat16)
```

```python
import jax
import jax.numpy as jnp
from jax import lax
from jax.sharding import Mesh
from jax.sharding import PartitionSpec as P

HD = 128
BLOCK = 32
CAP = 2
KV = ("kv_0", "kv_1")
DP_KV = ("dp", "kv_0", "kv_1")


def copy_for_each(shard, axis):
    count = lax.axis_size(axis)
    return lax.all_to_all(
        jnp.broadcast_to(shard[None], (count, *shard.shape)), axis, 0, 0, tiled=True
    )


def laid_out(blocks, dim):
    lengths = list(blocks.shape[1:])
    lengths[dim] *= blocks.shape[0]
    return jnp.moveaxis(blocks, 0, dim).reshape(lengths)


def gathered_copies(shard, axis, dim):
    blocks = copy_for_each(shard, axis)
    return laid_out(blocks, dim)


def spread_rows(shard):
    planes = lax.axis_size("dp")
    rows = shard.shape[0] // planes
    mine = lax.dynamic_slice_in_dim(shard, lax.axis_index("dp") * rows, rows, axis=0)
    column = copy_for_each(mine, "kv_0")
    every = copy_for_each(column, ("dp", "kv_1"))
    tall, wide = column.shape[0], lax.axis_size("kv_1")
    every = every.reshape(planes, wide, tall, rows, -1)
    return jnp.transpose(every, (2, 1, 0, 3, 4)).reshape(tall * wide * planes * rows, -1)


def body(tokens, query_weight, key_weight, value_weight, out_weight, chosen, live_length):
    rows = tokens.shape[0]
    per_dev = rows // BLOCK
    owners = lax.axis_size(KV)
    me = lax.axis_index(KV)

    def add_rows(piece):
        return jnp.dot(tokens, piece, preferred_element_type=jnp.float32)

    paired = add_rows(
        spread_rows(jnp.concatenate([key_weight, value_weight], axis=1))
    ).astype(jnp.bfloat16)
    queries = add_rows(lax.all_gather(query_weight, KV, axis=0, tiled=True)).astype(jnp.bfloat16)
    width = paired.shape[1]
    local_blocks = paired.reshape(per_dev, BLOCK, width)
    valid = chosen >= 0
    safe = jnp.maximum(chosen, 0)
    blocks_all = owners * per_dev
    hits = (safe[:, :, None] == jnp.arange(blocks_all, dtype=jnp.int32)[None, None, :]) & valid[
        :, :, None
    ]
    needed = jnp.any(hits, axis=(0, 1)).reshape(owners, per_dev)
    needed = needed & (jnp.arange(owners, dtype=jnp.int32) != me)[:, None]
    ranks = jnp.cumsum(needed.astype(jnp.int32), axis=1)
    local_ids = jnp.arange(per_dev, dtype=jnp.int32)
    slot_lists = []
    for slot in range(CAP):
        marked = needed & (ranks == slot + 1)
        found = jnp.any(marked, axis=1)
        where_at = jnp.sum(jnp.where(marked, local_ids[None, :], 0), axis=1)
        slot_lists.append(jnp.where(found, where_at, -1))
    wanted = jnp.stack(slot_lists, axis=1)
    requested = lax.all_to_all(wanted, KV, split_axis=0, concat_axis=0, tiled=True)
    outgoing = local_blocks[jnp.maximum(requested, 0)]
    outgoing = jnp.where((requested >= 0)[:, :, None, None], outgoing, jnp.zeros((), jnp.bfloat16))
    incoming = lax.all_to_all(outgoing, KV, split_axis=0, concat_axis=0, tiled=True)
    table = jnp.concatenate([incoming.reshape(owners * CAP, BLOCK, width), local_blocks], axis=0)
    segment_retainer = safe // per_dev
    local_of = safe % per_dev
    match = (wanted[None, None, :, :] == local_of[:, :, None, None]) & (
        jnp.arange(owners, dtype=jnp.int32)[None, None, :, None]
        == segment_retainer[:, :, None, None]
    )
    slot_index = jnp.arange(owners * CAP, dtype=jnp.int32).reshape(owners, CAP)
    remote_at = jnp.sum(jnp.where(match, slot_index[None, None], 0), axis=(2, 3))
    position = jnp.where(segment_retainer == me, owners * CAP + local_of, remote_at)
    picked = table[position]
    near_keys = picked[..., :HD]
    near_values = picked[..., HD:]
    grouped = queries.reshape(per_dev, BLOCK, -1, HD)
    scores = jnp.einsum(
        "jqhd,jnbd->jhqnb", grouped, near_keys, preferred_element_type=jnp.float32
    ) * HD ** (-0.5)
    query_pos = (me * per_dev + jnp.arange(per_dev, dtype=jnp.int32))[:, None] * BLOCK + jnp.arange(
        BLOCK, dtype=jnp.int32
    )[None, :]
    key_pos = safe[:, :, None] * BLOCK + jnp.arange(BLOCK, dtype=jnp.int32)[None, None, :]
    allowed = valid[:, None, :, None] & (key_pos[:, None, :, :] <= query_pos[:, :, None, None])
    masked = jnp.where(allowed[:, None], scores, -jnp.inf)
    top = jnp.max(masked, axis=(3, 4), keepdims=True)
    weights = jnp.exp(masked - top)
    total = jnp.sum(weights, axis=(3, 4))
    summed = jnp.einsum(
        "jhqnb,jnbd->jqhd",
        weights.astype(jnp.bfloat16),
        near_values,
        preferred_element_type=jnp.float32,
    )
    result = summed / jnp.transpose(total, (0, 2, 1))[..., None]
    live = query_pos < live_length[0]
    result = jnp.where(live[:, :, None, None], result, 0.0)
    attended = result.astype(jnp.bfloat16).reshape(rows, -1)
    every_head = gathered_copies(attended, "tp", 1)
    mixed = jnp.dot(
        every_head, lax.all_gather(out_weight, KV, axis=0, tiled=True), preferred_element_type=jnp.float32
    )
    return mixed.astype(jnp.bfloat16)


def solution(mesh):
    split = Mesh(
        mesh.devices.reshape(mesh.shape["dp"], 16, 4, mesh.shape["tp"]),
        ("dp", "kv_0", "kv_1", "tp"),
    )
    placed = (
        P(DP_KV, None),
        P(KV, "tp"),
        P(KV, "tp"),
        P(KV, "tp"),
        P(KV, "tp"),
        P(DP_KV, None),
        P("dp"),
    )
    return jax.shard_map(
        body, mesh=split, in_specs=placed, out_specs=P(DP_KV, "tp"), check_vma=False
    )
```

```python
import jax
import jax.numpy as jnp
from jax import lax
from jax.sharding import Mesh
from jax.sharding import PartitionSpec as P

HD = 128
BLOCK = 32
CAP = 2
KV = ("kv_0", "kv_1")
DP_KV = ("dp", "kv_0", "kv_1")


def copy_for_each(shard, axis):
    count = lax.axis_size(axis)
    return lax.all_to_all(
        jnp.broadcast_to(shard[None], (count, *shard.shape)), axis, 0, 0, tiled=True
    )


def from_ahead(x, axis, step):
    n = lax.axis_size(axis)
    return lax.ppermute(x, axis, [((i + step) % n, i) for i in range(n)])


def turned(pieces, axis_name, dim):
    n = len(pieces)
    twice = jnp.concatenate([*pieces, *pieces[:-1]], axis=dim)
    width = pieces[0].shape[dim]
    first = (n - lax.axis_index(axis_name)) % n
    return lax.dynamic_slice_in_dim(twice, first * width, n * width, axis=dim)


def around(x, axis):
    n = lax.axis_size(axis)
    return [x, *(from_ahead(x, axis, s) for s in range(1, n))]


def slots_wanted(chosen, owners, per_dev, me):
    ids = owners[:, None] * per_dev + jnp.arange(per_dev, dtype=jnp.int32)[None, :]
    hits = chosen.reshape(-1)[:, None, None] == ids[None]
    needed = jnp.any(hits, axis=0) & (owners != me)[:, None]
    ranks = jnp.cumsum(needed.astype(jnp.int32), axis=1)
    local_ids = jnp.arange(per_dev, dtype=jnp.int32)[None, :]
    lists = []
    for slot in range(CAP):
        marked = needed & (ranks == slot + 1)
        found = jnp.any(marked, axis=1)
        lists.append(jnp.where(found, jnp.sum(jnp.where(marked, local_ids, 0), axis=1), -1))
    return jnp.stack(lists, axis=1)


def body(tokens, query_weight, key_weight, value_weight, out_weight, chosen, live_length):
    rows = tokens.shape[0]
    per_dev = rows // BLOCK
    planes, tall, wide = (lax.axis_size(a) for a in ("dp", "kv_0", "kv_1"))
    x_at, z_at, y_at = (lax.axis_index(a) for a in ("dp", "kv_0", "kv_1"))
    owners = tall * wide
    me = lax.axis_index(KV)
    nsel = chosen.shape[1]

    def part(w, dim):
        size = w.shape[dim] // planes
        return lax.dynamic_slice_in_dim(w, x_at * size, size, axis=dim)

    def stacked(w):
        return jnp.concatenate(
            [w[:, i * HD : (i + 1) * HD] for i in range(w.shape[1] // HD)], axis=0
        )

    small = part(key_weight, 0).shape[0]
    valid = chosen >= 0
    safe = jnp.maximum(chosen, 0)
    notes = jnp.concatenate(
        [
            jnp.where(valid, chosen // per_dev, -1).reshape(-1, HD),
            jnp.where(valid, chosen % per_dev, -1).reshape(-1, HD),
        ],
        axis=0,
    ).astype(jnp.bfloat16)
    note_rows = notes.shape[0]
    notes = jnp.pad(notes, ((0, 16 - note_rows), (0, 0)))
    q_part = stacked(part(query_weight, 1))
    o_part = stacked(part(out_weight, 1))
    cargo = jnp.concatenate(
        [part(key_weight, 0), part(value_weight, 0), notes, q_part, o_part], axis=0
    )
    column = copy_for_each(cargo, "kv_0")
    head = 2 * small + 16
    every = copy_for_each(column[:, :head], ("dp", "kv_1"))
    every = every.reshape(planes, wide, tall, head, HD)

    def full_rows(piece):
        return jnp.transpose(piece, (2, 1, 0, 3, 4)).reshape(-1, HD)

    pair_weight = jnp.concatenate(
        [full_rows(every[:, :, :, :small]), full_rows(every[:, :, :, small : 2 * small])], axis=1
    )
    paired = jnp.dot(tokens, pair_weight, preferred_element_type=jnp.float32).astype(jnp.bfloat16)
    width = paired.shape[1]
    local_blocks = paired.reshape(per_dev, BLOCK, width)

    mates = lax.dynamic_index_in_dim(every[:, :, :, 2 * small : head], x_at, 0, keepdims=False)
    mates = lax.dynamic_index_in_dim(mates, z_at, 1, keepdims=False)
    half = note_rows // 2
    mate_owner = mates[:, :half].astype(jnp.int32)
    mate_local = mates[:, half:note_rows].astype(jnp.int32)
    mate_chosen = jnp.where(mate_owner >= 0, mate_owner * per_dev + mate_local, -1)

    pieces = [None] * tall
    pieces[0] = local_blocks
    up = down = local_blocks
    for s in range(1, tall // 2 + 1):
        up = from_ahead(up, "kv_0", -1)
        pieces[s] = up
        if s < tall - s:
            down = from_ahead(down, "kv_0", 1)
            pieces[tall - s] = down
    column_blocks = jnp.stack(pieces)

    back = jnp.arange(tall, dtype=jnp.int32)
    column_owners = ((z_at - back) % tall) * wide + y_at
    asked = jnp.stack(
        [
            slots_wanted(mate_chosen[i], column_owners, per_dev, z_at * wide + i)
            for i in range(wide)
        ]
    )
    pick = back[None, :, None] * per_dev + jnp.maximum(asked, 0)
    outgoing = column_blocks.reshape(tall * per_dev, BLOCK, width)[pick.reshape(wide, -1)]
    incoming = lax.all_to_all(outgoing, "kv_1", split_axis=0, concat_axis=0, tiled=True)
    far = wide * tall * CAP
    table = jnp.concatenate([incoming.reshape(far, BLOCK, width), local_blocks], axis=0)

    wanted = slots_wanted(chosen, jnp.arange(owners, dtype=jnp.int32), per_dev, me)
    holder = safe // per_dev
    local_of = safe % per_dev
    match = (wanted[None, None, :, :] == local_of[:, :, None, None]) & (
        jnp.arange(owners, dtype=jnp.int32)[None, None, :, None] == holder[:, :, None, None]
    )
    slot = jnp.sum(
        jnp.where(match, jnp.arange(CAP, dtype=jnp.int32)[None, None, None], 0), axis=(2, 3)
    )
    step = (z_at - holder // wide) % tall
    remote_at = ((holder % wide) * tall + step) * CAP + slot
    position = jnp.where(holder == me, far + local_of, remote_at)
    picked = table[position]
    near_keys = picked[..., :HD]
    near_values = picked[..., HD:]

    q_small = column[:, head : head + q_part.shape[0]]
    o_small = column[:, head + q_part.shape[0] :]
    q_tall = turned([p[:, None] for p in around(q_small, "kv_1")], "kv_1", 1).reshape(-1, HD)
    query_full = turned(around(q_tall, "dp"), "dp", 1)
    lines = out_weight.shape[0]
    o_small = jnp.concatenate(
        [o_small[:, i * lines : (i + 1) * lines] for i in range(o_small.shape[1] // lines)], axis=2
    )
    o_tall = turned([p[:, None] for p in around(o_small, "kv_1")], "kv_1", 1)
    o_tall = o_tall.reshape(-1, o_small.shape[2])
    out_full = turned(around(o_tall, "dp"), "dp", 1)
    queries = jnp.dot(tokens, query_full, preferred_element_type=jnp.float32).astype(jnp.bfloat16)

    grouped = queries.reshape(per_dev, BLOCK, -1, HD)
    scores = jnp.einsum(
        "jqhd,jnbd->jhqnb", grouped, near_keys, preferred_element_type=jnp.float32
    ) * HD ** (-0.5)
    query_pos = (me * per_dev + jnp.arange(per_dev, dtype=jnp.int32))[:, None] * BLOCK + jnp.arange(
        BLOCK, dtype=jnp.int32
    )[None, :]
    key_pos = safe[:, :, None] * BLOCK + jnp.arange(BLOCK, dtype=jnp.int32)[None, None, :]
    allowed = valid[:, None, :, None] & (key_pos[:, None, :, :] <= query_pos[:, :, None, None])
    masked = jnp.where(allowed[:, None], scores, -jnp.inf)
    top = jnp.max(masked, axis=(3, 4), keepdims=True)
    weights = jnp.exp(masked - top)
    total = jnp.sum(weights, axis=(3, 4))
    summed = jnp.einsum(
        "jhqnb,jnbd->jqhd",
        weights.astype(jnp.bfloat16),
        near_values,
        preferred_element_type=jnp.float32,
    )
    result = summed / jnp.transpose(total, (0, 2, 1))[..., None]
    live = query_pos < live_length[0]
    result = jnp.where(live[:, :, None, None], result, 0.0)
    attended = result.astype(jnp.bfloat16).reshape(rows, -1)
    other = from_ahead(attended, "tp", 1)
    first = lax.axis_index("tp") == 0
    every_head = jnp.concatenate(
        [jnp.where(first, attended, other), jnp.where(first, other, attended)], axis=1
    )
    mixed = jnp.dot(every_head, out_full, preferred_element_type=jnp.float32)
    return mixed.astype(jnp.bfloat16)


def solution(mesh):
    split = Mesh(
        mesh.devices.reshape(mesh.shape["dp"], 16, 4, mesh.shape["tp"]),
        ("dp", "kv_0", "kv_1", "tp"),
    )
    placed = (
        P(DP_KV, None),
        P(KV, "tp"),
        P(KV, "tp"),
        P(KV, "tp"),
        P(KV, "tp"),
        P(DP_KV, None),
        P("dp"),
    )
    return jax.shard_map(
        body, mesh=split, in_specs=placed, out_specs=P(DP_KV, "tp"), check_vma=False
    )
```

```python
import jax
import jax.numpy as jnp
from jax import lax
from jax.experimental import pallas as pl
from jax.experimental.pallas import tpu as pltpu
from jax.sharding import Mesh
from jax.sharding import PartitionSpec as P


HD = 128
BLOCK = 32
CAP = 2
NEVER = 1 << 30
KV = ("kv_0", "kv_1")
DP_KV = ("dp", "kv_0", "kv_1")
F32 = jnp.float32
BF16 = jnp.bfloat16


def call(kernel, out_shape, *args, scratch=(), flops=0):
    spaces = [
        pl.BlockSpec(memory_space=pltpu.SMEM if a.dtype == jnp.int32 and a.ndim < 3 else pltpu.VMEM)
        for a in args
    ]
    return pl.pallas_call(
        kernel,
        out_shape=out_shape,
        in_specs=spaces,
        out_specs=pl.BlockSpec(memory_space=pltpu.VMEM),
        scratch_shapes=list(scratch),
        compiler_params=pltpu.CompilerParams(vmem_limit_bytes=40 << 20),
        cost_estimate=pl.CostEstimate(flops=flops, bytes_accessed=0, transcendentals=0),
    )(*args)


def copy_for_each(shard, axis):
    count = lax.axis_size(axis)
    return lax.all_to_all(
        jnp.broadcast_to(shard[None], (count, *shard.shape)), axis, 0, 0, tiled=True
    )


def from_ahead(x, axis, step):
    n = lax.axis_size(axis)
    return lax.ppermute(x, axis, [((i + step) % n, i) for i in range(n)])


def spread(x, axis):
    steps = range(1, lax.axis_size(axis))
    return [x, *(from_ahead(x, axis, s) for s in steps)]


def after(*values):
    return lax.optimization_barrier(values)


def slots_wanted(chosen, owners, per_dev, me):
    ids = owners[:, None] * per_dev + jnp.arange(per_dev, dtype=jnp.int32)[None, :]
    hits = chosen.reshape(-1)[:, None, None] == ids[None]
    needed = jnp.any(hits, axis=0) & (owners != me)[:, None]
    ranks = jnp.cumsum(needed.astype(jnp.int32), axis=1)
    local_ids = jnp.arange(per_dev, dtype=jnp.int32)[None, :]
    lists = []
    for slot in range(CAP):
        marked = needed & (ranks == slot + 1)
        found = jnp.any(marked, axis=1)
        lists.append(jnp.where(found, jnp.sum(jnp.where(marked, local_ids, 0), axis=1), -1))
    return jnp.stack(lists, axis=1)


def project_pair(tokens, every):
    planes, wide, tall, both, _ = every.shape
    small = both // 2
    deep = planes * wide * small

    def kernel(t_ref, w_ref, o_ref):
        total = jnp.zeros(o_ref.shape, F32)
        for z in range(tall):
            lines = [(x, y) for y in range(wide) for x in range(planes)]
            keys = jnp.concatenate([w_ref[x, y, z, :small] for x, y in lines], axis=0)
            values = jnp.concatenate([w_ref[x, y, z, small:] for x, y in lines], axis=0)
            total += jnp.dot(
                t_ref[:, z * deep : (z + 1) * deep],
                jnp.concatenate([keys, values], axis=1),
                preferred_element_type=F32,
            )
        o_ref[...] = total.astype(BF16)

    out = jax.ShapeDtypeStruct((tokens.shape[0], 2 * HD), BF16)
    flops = 2 * tokens.size * 2 * HD
    return call(kernel, out, tokens, every, flops=flops)


def project_queries(tokens, pieces, tile):
    def kernel(t_ref, *refs):
        o_ref = refs[-1]
        for i in range(0, len(pieces), 2):
            w = jnp.concatenate([refs[i][...], refs[i + 1][...]], axis=1)
            o_ref[:, i * HD : (i + 2) * HD] = jnp.dot(
                t_ref[...], w, preferred_element_type=F32
            ).astype(BF16)

    width = len(pieces) * HD
    out = jax.ShapeDtypeStruct((tokens.shape[0], width), BF16)
    flops = 2 * tokens.size * width
    return call(kernel, out, tokens, *pieces, tile, flops=flops)


def turned(pieces, at):
    n = len(pieces)
    tall, rows, width = pieces[0].shape

    def kernel(at_ref, *refs):
        for s in range(n):
            refs[-1][:, (at_ref[0] + s) % n] = refs[s][...]

    out = jax.ShapeDtypeStruct((tall, n, rows, width), BF16)
    return call(kernel, out, at[None], *pieces)


def turned_columns(pieces, at):
    n = len(pieces)
    tall, rows, width = pieces[0].shape

    def kernel(at_ref, *refs):
        for s in range(n):
            first = pl.multiple_of(((at_ref[0] + s) % n) * width, width)
            refs[-1][:, :, pl.ds(first, width)] = refs[s][...]

    out = jax.ShapeDtypeStruct((tall, rows, n * width), BF16)
    return call(kernel, out, at[None], *pieces)


def pick_blocks(pieces, asked):
    wide, count = asked.shape

    def kernel(asked_ref, *refs):
        for y in range(wide):
            for i in range(count):
                refs[-1][y, i] = refs[i // CAP][asked_ref[y, i]]

    out = jax.ShapeDtypeStruct((wide, count, *pieces[0].shape[1:]), BF16)
    return call(kernel, out, asked, *pieces)


def attend(queries, incoming, local_blocks, position, key_pos, facts):
    rows, width = queries.shape
    heads = width // HD
    far = incoming.shape[0]
    per_dev, nsel = position.shape
    keys = nsel * BLOCK

    def kernel(f_ref, p_ref, q_ref, in_ref, own_ref, kp_ref, o_ref, tab, k_s, v_s):
        tab[:far] = in_ref[...]
        tab[far:] = own_ref[...]
        for j in range(per_dev):
            for n in range(nsel):
                block = tab[p_ref[j, n]]
                k_s[j % 2, n * BLOCK : (n + 1) * BLOCK] = block[:, :HD]
                v_s[j % 2, n * BLOCK : (n + 1) * BLOCK] = block[:, HD:]
            mine = slice(j * BLOCK, (j + 1) * BLOCK)
            q = jnp.concatenate(
                [q_ref[mine, h * HD : (h + 1) * HD] for h in range(heads)], axis=0
            )
            scores = lax.dot_general(
                q, k_s[j % 2], (((1,), (1,)), ((), ())), preferred_element_type=F32
            ) * HD ** (-0.5)
            line = lax.broadcasted_iota(jnp.int32, (heads * BLOCK, 1), 0) % BLOCK
            at = f_ref[0] + j * BLOCK + line
            masked = jnp.where(kp_ref[j] <= at, scores, -jnp.inf)
            top = jnp.max(masked, axis=1, keepdims=True)
            weights = jnp.exp(masked - top)
            total = jnp.sum(weights, axis=1, keepdims=True)
            summed = jnp.dot(weights.astype(BF16), v_s[j % 2], preferred_element_type=F32)
            result = jnp.where(at < f_ref[1], summed / total, 0.0).astype(BF16)
            for h in range(heads):
                first = pl.multiple_of(((f_ref[2] + h) % heads) * HD, HD)
                o_ref[mine, pl.ds(first, HD)] = result[h * BLOCK : (h + 1) * BLOCK]

    return call(
        kernel,
        jax.ShapeDtypeStruct((rows, width), BF16),
        facts,
        position,
        queries,
        incoming,
        local_blocks,
        key_pos,
        scratch=(
            pltpu.VMEM((far + per_dev, BLOCK, 2 * HD), BF16),
            pltpu.VMEM((2, keys, HD), BF16),
            pltpu.VMEM((2, keys, HD), BF16),
        ),
        flops=4 * rows * keys * width,
    )


def mix(mine, other, pieces, places):
    n = len(pieces)
    tall, lines, width = pieces[0].shape
    half = tall // 2

    def kernel(p_ref, m_ref, t_ref, *refs):
        o_ref, w_s = refs[n], refs[n + 1]
        for s in range(n):
            w_s[:, (p_ref[0] + s) % n] = refs[s][...]
        first = w_s[pl.ds(p_ref[1] * half, half)].reshape(half * n * lines, width)
        second = w_s[pl.ds((1 - p_ref[1]) * half, half)].reshape(half * n * lines, width)
        o_ref[...] = (
            jnp.dot(m_ref[...], first, preferred_element_type=F32)
            + jnp.dot(t_ref[...], second, preferred_element_type=F32)
        ).astype(BF16)

    out = jax.ShapeDtypeStruct((mine.shape[0], width), BF16)
    scratch = (pltpu.VMEM((tall, n, lines, width), BF16),)
    flops = 4 * mine.size * width
    return call(kernel, out, places, mine, other, *pieces, scratch=scratch, flops=flops)


def body(tokens, query_weight, key_weight, value_weight, out_weight, chosen, live_length):
    rows = tokens.shape[0]
    per_dev = rows // BLOCK
    planes, tall, wide = (lax.axis_size(a) for a in ("dp", "kv_0", "kv_1"))
    x_at, z_at, y_at = (lax.axis_index(a) for a in ("dp", "kv_0", "kv_1"))
    owners = tall * wide
    me = z_at * wide + y_at

    def part(w, dim):
        size = w.shape[dim] // planes
        return lax.dynamic_slice_in_dim(w, x_at * size, size, axis=dim)

    pair_rows = 2 * (key_weight.shape[0] // planes)
    cargo = jnp.concatenate(
        [part(key_weight, 0), part(value_weight, 0), part(query_weight, 1)], axis=0
    )
    column = copy_for_each(cargo, "kv_0")
    every = copy_for_each(column[:, :pair_rows], ("dp", "kv_1"))
    every = every.reshape(planes, wide, tall, pair_rows, HD)
    q_small = column[:, pair_rows:]
    o_part = part(out_weight, 1)

    mates = spread(chosen, "kv_1")
    back = jnp.arange(tall, dtype=jnp.int32)
    column_owners = ((z_at - back) % tall) * wide + y_at
    asked = jnp.stack(
        [
            slots_wanted(mates[s], column_owners, per_dev, z_at * wide + (y_at + s) % wide)
            for s in range(wide)
        ]
    )
    asked = jnp.roll(jnp.maximum(asked, 0).reshape(wide, tall * CAP), y_at, axis=0)
    valid = chosen >= 0
    safe = jnp.maximum(chosen, 0)
    wanted = slots_wanted(chosen, jnp.arange(owners, dtype=jnp.int32), per_dev, me)
    holder = safe // per_dev
    local_of = safe % per_dev
    match = (wanted[None, None, :, :] == local_of[:, :, None, None]) & (
        jnp.arange(owners, dtype=jnp.int32)[None, None, :, None] == holder[:, :, None, None]
    )
    slot = jnp.sum(
        jnp.where(match, jnp.arange(CAP, dtype=jnp.int32)[None, None, None], 0), axis=(2, 3)
    )
    step = (z_at - holder // wide) % tall
    far = wide * tall * CAP
    remote_at = ((holder % wide) * tall + step) * CAP + slot
    position = jnp.where(holder == me, far + local_of, remote_at)
    key_pos = safe[:, :, None] * BLOCK + jnp.arange(BLOCK, dtype=jnp.int32)[None, None, :]
    key_pos = jnp.where(valid[:, :, None], key_pos, NEVER).reshape(per_dev, 1, -1)
    facts = jnp.stack([me * rows, live_length[0], x_at]).astype(jnp.int32)

    paired = project_pair(tokens, every)
    local_blocks = paired.reshape(per_dev, BLOCK, paired.shape[1])

    pieces = [None] * tall
    pieces[0] = up = down = local_blocks
    for s in range(1, tall // 2 + 1):
        up = from_ahead(up, "kv_0", -1)
        if s < tall - s:
            down = from_ahead(down, "kv_0", 1)
        if s == 1:
            up, down, q_small, o_part = after(up, down, q_small, o_part)
            q_pieces = spread(q_small, "kv_1")
            o_small = copy_for_each(o_part, "kv_0")
        if s == 3:
            up, down, *q_pieces = after(up, down, *q_pieces)
            q_tall = turned(q_pieces, y_at).reshape(-1, HD)
            q_pieces = spread(q_tall, "dp")
        if s == 4:
            up, down, o_small = after(up, down, o_small)
            o_pieces = spread(o_small, "dp")
        if s == 6:
            up, down, *o_pieces = after(up, down, *o_pieces)
            o_full = turned_columns(o_pieces, x_at)
            o_pieces = spread(o_full, "kv_1")
        pieces[s] = up
        if s < tall - s:
            pieces[tall - s] = down
    outgoing = pick_blocks(pieces, asked)
    incoming = lax.all_to_all(outgoing, "kv_1", split_axis=0, concat_axis=0, tiled=True)
    queries = project_queries(tokens, q_pieces, outgoing[0, 0, :16, :HD])
    attended = attend(
        queries,
        incoming.reshape(far, BLOCK, paired.shape[1]),
        local_blocks,
        position,
        key_pos,
        facts,
    )
    other = from_ahead(attended, "tp", 1)
    places = jnp.stack([y_at, lax.axis_index("tp")]).astype(jnp.int32)
    return mix(attended, other, o_pieces, places)


def solution(mesh):
    split = Mesh(
        mesh.devices.reshape(mesh.shape["dp"], 16, 4, mesh.shape["tp"]),
        ("dp", "kv_0", "kv_1", "tp"),
    )
    placed = (
        P(DP_KV, None),
        P(KV, "tp"),
        P(KV, "tp"),
        P(KV, "tp"),
        P(KV, "tp"),
        P(DP_KV, None),
        P("dp"),
    )

    return jax.shard_map(
        body, mesh=split, in_specs=placed, out_specs=P(DP_KV, "tp"), check_vma=False
    )
```

```python
import jax
import jax.numpy as jnp
from jax import lax
from jax.experimental import pallas as pl
from jax.experimental.pallas import tpu as pltpu
from jax.sharding import Mesh
from jax.sharding import PartitionSpec as P


HD = 128
BLOCK = 32
CAP = 2
NEVER = 1 << 30
KV = ("kv_0", "kv_1")
DP_KV = ("dp", "kv_0", "kv_1")
F32 = jnp.float32
BF16 = jnp.bfloat16


def call(kernel, out_shape, *args, scratch=(), flops=0):
    spaces = [
        pl.BlockSpec(memory_space=pltpu.SMEM if a.dtype == jnp.int32 and a.ndim < 3 else pltpu.VMEM)
        for a in args
    ]
    return pl.pallas_call(
        kernel,
        out_shape=out_shape,
        in_specs=spaces,
        out_specs=pl.BlockSpec(memory_space=pltpu.VMEM),
        scratch_shapes=list(scratch),
        compiler_params=pltpu.CompilerParams(vmem_limit_bytes=40 << 20),
        cost_estimate=pl.CostEstimate(flops=flops, bytes_accessed=0, transcendentals=0),
    )(*args)


def copy_for_each(shard, axis):
    count = lax.axis_size(axis)
    return lax.all_to_all(
        jnp.broadcast_to(shard[None], (count, *shard.shape)), axis, 0, 0, tiled=True
    )


def from_ahead(x, axis, step):
    n = lax.axis_size(axis)
    return lax.ppermute(x, axis, [((i + step) % n, i) for i in range(n)])


def spread(x, axis):
    steps = range(1, lax.axis_size(axis))
    return [x, *(from_ahead(x, axis, s) for s in steps)]


def after(*values):
    return lax.optimization_barrier(values)


def slots_wanted(chosen, owners, per_dev, me):
    ids = owners[:, None] * per_dev + jnp.arange(per_dev, dtype=jnp.int32)[None, :]
    hits = chosen.reshape(-1)[:, None, None] == ids[None]
    needed = jnp.any(hits, axis=0) & (owners != me)[:, None]
    ranks = jnp.cumsum(needed.astype(jnp.int32), axis=1)
    local_ids = jnp.arange(per_dev, dtype=jnp.int32)[None, :]
    lists = []
    for slot in range(CAP):
        marked = needed & (ranks == slot + 1)
        found = jnp.any(marked, axis=1)
        lists.append(jnp.where(found, jnp.sum(jnp.where(marked, local_ids, 0), axis=1), -1))
    return jnp.stack(lists, axis=1)


def project_pair(tokens, every):
    planes, wide, tall, both, _ = every.shape
    small = both // 2
    deep = planes * wide * small

    def kernel(t_ref, w_ref, o_ref):
        total = jnp.zeros(o_ref.shape, F32)
        for z in range(tall):
            lines = [(x, y) for y in range(wide) for x in range(planes)]
            keys = jnp.concatenate([w_ref[x, y, z, :small] for x, y in lines], axis=0)
            values = jnp.concatenate([w_ref[x, y, z, small:] for x, y in lines], axis=0)
            total += jnp.dot(
                t_ref[:, z * deep : (z + 1) * deep],
                jnp.concatenate([keys, values], axis=1),
                preferred_element_type=F32,
            )
        o_ref[...] = total.astype(BF16)

    out = jax.ShapeDtypeStruct((tokens.shape[0], 2 * HD), BF16)
    flops = 2 * tokens.size * 2 * HD
    return call(kernel, out, tokens, every, flops=flops)


def project_queries(tokens, pieces, tile):
    def kernel(t_ref, *refs):
        o_ref = refs[-1]
        for i in range(0, len(pieces), 2):
            w = jnp.concatenate([refs[i][...], refs[i + 1][...]], axis=1)
            o_ref[:, i * HD : (i + 2) * HD] = jnp.dot(
                t_ref[...], w, preferred_element_type=F32
            ).astype(BF16)

    width = len(pieces) * HD
    out = jax.ShapeDtypeStruct((tokens.shape[0], width), BF16)
    flops = 2 * tokens.size * width
    return call(kernel, out, tokens, *pieces, tile, flops=flops)


def turned(pieces, at):
    n = len(pieces)
    tall, lines, _ = pieces[0].shape
    columns = 2
    rows = lines // columns

    def kernel(at_ref, *refs):
        for s in range(n):
            y = (at_ref[0] + s) % n
            for i in range(columns):
                refs[-1][i, :, y] = refs[s][:, i * rows : (i + 1) * rows]

    out = jax.ShapeDtypeStruct((columns, tall, n, rows, HD), BF16)
    return call(kernel, out, at[None], *pieces)


def full_columns(own, ahead, behind, lines, parity):
    tall, held, _ = own.shape
    groups = held // lines

    def kernel(p_ref, own_ref, ahead_ref, behind_ref, o_ref):
        def put(half, i, value):
            first = pl.multiple_of((half * groups + i) * HD, HD)
            o_ref[:, :, pl.ds(first, HD)] = value

        for i in range(groups):
            put(p_ref[0], i, own_ref[:, i * lines : (i + 1) * lines])
        for i in range(groups // 2):
            cut = slice(i * lines, (i + 1) * lines)
            put(1 - p_ref[0], i, ahead_ref[:, cut])
            put(1 - p_ref[0], i + groups // 2, behind_ref[:, cut])

    out = jax.ShapeDtypeStruct((tall, lines, 2 * groups * HD), BF16)
    return call(kernel, out, parity[None], own, ahead, behind)


def key_positions(chosen):
    per_dev, nsel = chosen.shape

    def kernel(c_ref, o_ref):
        lane = lax.broadcasted_iota(jnp.int32, (1, nsel * BLOCK), 1)
        for j in range(per_dev):
            row = jnp.zeros((1, nsel * BLOCK), jnp.int32)
            for n in range(nsel):
                first = jnp.where(c_ref[j, n] >= 0, c_ref[j, n] * BLOCK, NEVER)
                row = jnp.where(lane // BLOCK == n, first, row)
            o_ref[j] = row + lane % BLOCK

    out = jax.ShapeDtypeStruct((per_dev, 1, nsel * BLOCK), jnp.int32)
    return call(kernel, out, chosen)


def pick_blocks(blocks, asked):
    wide, count = asked.shape

    def kernel(asked_ref, b_ref, o_ref):
        for y in range(wide):
            for i in range(count):
                o_ref[y, i] = b_ref[asked_ref[y, i]]

    out = jax.ShapeDtypeStruct((wide, count, *blocks.shape[1:]), BF16)
    return call(kernel, out, asked, blocks)


def attend(queries, incoming, local_blocks, position, key_pos, facts):
    rows, width = queries.shape
    heads = width // HD
    far = incoming.shape[0]
    per_dev, nsel = position.shape
    keys = nsel * BLOCK

    def kernel(f_ref, p_ref, q_ref, in_ref, own_ref, kp_ref, o_ref, tab, k_s, v_s):
        tab[:far] = in_ref[...]
        tab[far:] = own_ref[...]
        for j in range(per_dev):
            for n in range(nsel):
                block = tab[p_ref[j, n]]
                k_s[j % 2, n * BLOCK : (n + 1) * BLOCK] = block[:, :HD]
                v_s[j % 2, n * BLOCK : (n + 1) * BLOCK] = block[:, HD:]
            mine = slice(j * BLOCK, (j + 1) * BLOCK)
            q = jnp.concatenate(
                [q_ref[mine, h * HD : (h + 1) * HD] for h in range(heads)], axis=0
            )
            scores = lax.dot_general(
                q, k_s[j % 2], (((1,), (1,)), ((), ())), preferred_element_type=F32
            ) * HD ** (-0.5)
            line = lax.broadcasted_iota(jnp.int32, (heads * BLOCK, 1), 0) % BLOCK
            at = f_ref[0] + j * BLOCK + line
            masked = jnp.where(kp_ref[j] <= at, scores, -jnp.inf)
            top = jnp.max(masked, axis=1, keepdims=True)
            weights = jnp.exp(masked - top)
            total = jnp.sum(weights, axis=1, keepdims=True)
            summed = jnp.dot(weights.astype(BF16), v_s[j % 2], preferred_element_type=F32)
            result = jnp.where(at < f_ref[1], summed / total, 0.0).astype(BF16)
            for h in range(heads):
                first = pl.multiple_of(((f_ref[2] + h) % heads) * HD, HD)
                o_ref[mine, pl.ds(first, HD)] = result[h * BLOCK : (h + 1) * BLOCK]

    return call(
        kernel,
        jax.ShapeDtypeStruct((rows, width), BF16),
        facts,
        position,
        queries,
        incoming,
        local_blocks,
        key_pos,
        scratch=(
            pltpu.VMEM((far + per_dev, BLOCK, 2 * HD), BF16),
            pltpu.VMEM((2, keys, HD), BF16),
            pltpu.VMEM((2, keys, HD), BF16),
        ),
        flops=4 * rows * keys * width,
    )


def mix(mine, other, pieces, places):
    n = len(pieces)
    tall, lines, width = pieces[0].shape
    half = tall // 2

    def kernel(p_ref, m_ref, t_ref, *refs):
        o_ref, w_s = refs[n], refs[n + 1]
        for s in range(n):
            w_s[:, (p_ref[0] + s) % n] = refs[s][...]
        first = w_s[pl.ds(p_ref[1] * half, half)].reshape(half * n * lines, width)
        second = w_s[pl.ds((1 - p_ref[1]) * half, half)].reshape(half * n * lines, width)
        o_ref[...] = (
            jnp.dot(m_ref[...], first, preferred_element_type=F32)
            + jnp.dot(t_ref[...], second, preferred_element_type=F32)
        ).astype(BF16)

    out = jax.ShapeDtypeStruct((mine.shape[0], width), BF16)
    scratch = (pltpu.VMEM((tall, n, lines, width), BF16),)
    flops = 4 * mine.size * width
    return call(kernel, out, places, mine, other, *pieces, scratch=scratch, flops=flops)


def body(tokens, query_weight, key_weight, value_weight, out_weight, chosen, live_length):
    rows = tokens.shape[0]
    per_dev = rows // BLOCK
    planes, tall, wide = (lax.axis_size(a) for a in ("dp", "kv_0", "kv_1"))
    x_at, z_at, y_at = (lax.axis_index(a) for a in ("dp", "kv_0", "kv_1"))
    owners = tall * wide
    me = z_at * wide + y_at

    def stacked(w):
        return jnp.concatenate(
            [w[:, i * HD : (i + 1) * HD] for i in range(w.shape[1] // HD)], axis=0
        )

    def part(w, dim):
        size = w.shape[dim] // planes
        return lax.dynamic_slice_in_dim(w, x_at * size, size, axis=dim)

    parity = x_at % 2
    lines = out_weight.shape[0]
    q_half = lax.dynamic_slice_in_dim(
        query_weight, parity * (query_weight.shape[1] // 2), query_weight.shape[1] // 2, axis=1
    )
    o_half = lax.dynamic_slice_in_dim(
        out_weight, parity * (out_weight.shape[1] // 2), out_weight.shape[1] // 2, axis=1
    )
    halves = jnp.concatenate([stacked(q_half), stacked(o_half)], axis=0)
    halves = lax.all_gather(halves, "kv_0", axis=0, tiled=False)

    pair_rows = 2 * (key_weight.shape[0] // planes)
    cargo = jnp.concatenate([part(key_weight, 0), part(value_weight, 0)], axis=0)
    column = copy_for_each(cargo, "kv_0")
    every = copy_for_each(column, ("dp", "kv_1"))
    every = every.reshape(planes, wide, tall, pair_rows, HD)
    paired = project_pair(tokens, every)
    paired, halves, late_chosen = after(paired, halves, chosen)
    local_blocks = paired.reshape(per_dev, BLOCK, paired.shape[1])
    column_blocks = lax.all_gather(local_blocks, "kv_0", axis=0, tiled=True)

    q_lines = halves.shape[1] // 2
    q_pieces = spread(halves[:, :q_lines], "kv_1")
    o_own = halves[:, q_lines:]
    cut = o_own.shape[1] // 2
    o_ahead = from_ahead(o_own[:, :cut], "dp", 1)
    o_behind = from_ahead(o_own[:, cut:], "dp", -1)
    q_tall = turned(q_pieces, y_at).reshape(2, -1, HD)
    q_pieces = [
        q_tall[0], q_tall[1], from_ahead(q_tall[0], "dp", 1), from_ahead(q_tall[1], "dp", -1)
    ]
    o_pieces = spread(full_columns(o_own, o_ahead, o_behind, lines, parity), "kv_1")

    mates = spread(late_chosen, "kv_1")
    column_owners = jnp.arange(tall, dtype=jnp.int32) * wide + y_at
    asked = jnp.stack(
        [
            slots_wanted(mates[s], column_owners, per_dev, z_at * wide + (y_at + s) % wide)
            for s in range(wide)
        ]
    )
    asked = jnp.maximum(asked, 0) + (jnp.arange(tall, dtype=jnp.int32) * per_dev)[None, :, None]
    asked = jnp.roll(asked.reshape(wide, tall * CAP), y_at, axis=0)
    safe = jnp.maximum(late_chosen, 0)
    wanted = slots_wanted(late_chosen, jnp.arange(owners, dtype=jnp.int32), per_dev, me)
    holder = safe // per_dev
    local_of = safe % per_dev
    match = (wanted[None, None, :, :] == local_of[:, :, None, None]) & (
        jnp.arange(owners, dtype=jnp.int32)[None, None, :, None] == holder[:, :, None, None]
    )
    slot = jnp.sum(
        jnp.where(match, jnp.arange(CAP, dtype=jnp.int32)[None, None, None], 0), axis=(2, 3)
    )
    far = wide * tall * CAP
    remote_at = ((holder % wide) * tall + holder // wide) * CAP + slot
    position = jnp.where(holder == me, far + local_of, remote_at)
    key_pos = key_positions(late_chosen)
    facts = jnp.stack([me * rows, live_length[0], 2 * parity]).astype(jnp.int32)

    outgoing = pick_blocks(column_blocks, asked)
    incoming = lax.all_to_all(outgoing, "kv_1", split_axis=0, concat_axis=0, tiled=True)
    queries = project_queries(tokens, q_pieces, outgoing[0, 0, :16, :HD])
    attended = attend(
        queries,
        incoming.reshape(far, BLOCK, paired.shape[1]),
        local_blocks,
        position,
        key_pos,
        facts,
    )
    other = from_ahead(attended, "tp", 1)
    places = jnp.stack([y_at, lax.axis_index("tp")]).astype(jnp.int32)
    return mix(attended, other, o_pieces, places)


def solution(mesh):
    split = Mesh(
        mesh.devices.reshape(mesh.shape["dp"], 16, 4, mesh.shape["tp"]),
        ("dp", "kv_0", "kv_1", "tp"),
    )
    placed = (
        P(DP_KV, None),
        P(KV, "tp"),
        P(KV, "tp"),
        P(KV, "tp"),
        P(KV, "tp"),
        P(DP_KV, None),
        P("dp"),
    )

    return jax.shard_map(
        body, mesh=split, in_specs=placed, out_specs=P(DP_KV, "tp"), check_vma=False
    )
```

```python
import jax
import jax.numpy as jnp
from jax import lax
from jax.experimental import pallas as pl
from jax.experimental.pallas import tpu as pltpu
from jax.sharding import Mesh
from jax.sharding import PartitionSpec as P


HD = 128
BLOCK = 32
CAP = 2
NEVER = 1 << 30
KV = ("kv_0", "kv_1")
DP_KV = ("dp", "kv_0", "kv_1")
F32 = jnp.float32
BF16 = jnp.bfloat16


def call(kernel, out_shape, *args, scratch=(), flops=0):
    spaces = [
        pl.BlockSpec(memory_space=pltpu.SMEM if a.dtype == jnp.int32 and a.ndim < 3 else pltpu.VMEM)
        for a in args
    ]
    return pl.pallas_call(
        kernel,
        out_shape=out_shape,
        in_specs=spaces,
        out_specs=jax.tree.map(lambda _: pl.BlockSpec(memory_space=pltpu.VMEM), out_shape),
        scratch_shapes=list(scratch),
        compiler_params=pltpu.CompilerParams(vmem_limit_bytes=40 << 20),
        cost_estimate=pl.CostEstimate(flops=flops, bytes_accessed=0, transcendentals=0),
    )(*args)


def copy_for_each(shard, axis):
    count = lax.axis_size(axis)
    return lax.all_to_all(
        jnp.broadcast_to(shard[None], (count, *shard.shape)), axis, 0, 0, tiled=True
    )


def from_ahead(x, axis, step):
    n = lax.axis_size(axis)
    return lax.ppermute(x, axis, [((i + step) % n, i) for i in range(n)])


def spread(x, axis):
    steps = range(1, lax.axis_size(axis))
    return [x, *(from_ahead(x, axis, s) for s in steps)]


def after(*values):
    return lax.optimization_barrier(values)


def slots_wanted(chosen, owners, per_dev, me):
    ids = owners[:, None] * per_dev + jnp.arange(per_dev, dtype=jnp.int32)[None, :]
    hits = chosen.reshape(-1)[:, None, None] == ids[None]
    needed = jnp.any(hits, axis=0) & (owners != me)[:, None]
    ranks = jnp.cumsum(needed.astype(jnp.int32), axis=1)
    local_ids = jnp.arange(per_dev, dtype=jnp.int32)[None, :]
    lists = []
    for slot in range(CAP):
        marked = needed & (ranks == slot + 1)
        found = jnp.any(marked, axis=1)
        lists.append(jnp.where(found, jnp.sum(jnp.where(marked, local_ids, 0), axis=1), -1))
    return jnp.stack(lists, axis=1)


def pack(query_weight, key_weight, value_weight, out_weight, x_at, planes, tall):
    rows = key_weight.shape[0]
    lines, wide_out = out_weight.shape
    small = rows // planes
    q_groups = query_weight.shape[1] // 2 // HD
    o_groups = wide_out // 2 // HD

    def kernel(x_ref, q_ref, k_ref, v_ref, o_ref, half_ref, cargo_ref):
        parity = x_ref[0] % 2
        for i in range(q_groups):
            first = pl.multiple_of((parity * q_groups + i) * HD, HD)
            half_ref[i * rows : (i + 1) * rows] = q_ref[:, pl.ds(first, HD)]
        base = q_groups * rows
        for i in range(o_groups):
            first = pl.multiple_of((parity * o_groups + i) * HD, HD)
            half_ref[base + i * lines : base + (i + 1) * lines] = o_ref[:, pl.ds(first, HD)]
        first = pl.multiple_of(x_ref[0] * small, small)
        keys = k_ref[pl.ds(first, small)]
        values = v_ref[pl.ds(first, small)]
        for z in range(tall):
            cargo_ref[z, :small] = keys
            cargo_ref[z, small:] = values

    outs = (
        jax.ShapeDtypeStruct((q_groups * rows + o_groups * lines, HD), BF16),
        jax.ShapeDtypeStruct((tall, 2 * small, HD), BF16),
    )
    return call(kernel, outs, x_at[None], query_weight, key_weight, value_weight, out_weight)


def project_pair(tokens, every):
    planes, wide, tall, both, _ = every.shape
    small = both // 2
    deep = planes * wide * small

    def kernel(t_ref, w_ref, o_ref):
        total = jnp.zeros(o_ref.shape, F32)
        for z in range(tall):
            lines = [(x, y) for y in range(wide) for x in range(planes)]
            keys = jnp.concatenate([w_ref[x, y, z, :small] for x, y in lines], axis=0)
            values = jnp.concatenate([w_ref[x, y, z, small:] for x, y in lines], axis=0)
            total += jnp.dot(
                t_ref[:, z * deep : (z + 1) * deep],
                jnp.concatenate([keys, values], axis=1),
                preferred_element_type=F32,
            )
        o_ref[...] = total.astype(BF16)

    out = jax.ShapeDtypeStruct((tokens.shape[0], 2 * HD), BF16)
    flops = 2 * tokens.size * 2 * HD
    return call(kernel, out, tokens, every, flops=flops)


def project_queries(tokens, pieces, tile):
    def kernel(t_ref, *refs):
        o_ref = refs[-1]
        for i in range(0, len(pieces), 2):
            w = jnp.concatenate([refs[i][...], refs[i + 1][...]], axis=1)
            o_ref[:, i * HD : (i + 2) * HD] = jnp.dot(
                t_ref[...], w, preferred_element_type=F32
            ).astype(BF16)

    width = len(pieces) * HD
    out = jax.ShapeDtypeStruct((tokens.shape[0], width), BF16)
    flops = 2 * tokens.size * width
    return call(kernel, out, tokens, *pieces, tile, flops=flops)


def turned(pieces, at):
    n = len(pieces)
    tall, lines, _ = pieces[0].shape
    columns = 2
    rows = lines // columns

    def kernel(at_ref, *refs):
        for s in range(n):
            y = (at_ref[0] + s) % n
            for i in range(columns):
                refs[-1][i, :, y] = refs[s][:, i * rows : (i + 1) * rows]

    out = jax.ShapeDtypeStruct((columns, tall, n, rows, HD), BF16)
    return call(kernel, out, at[None], *pieces)


def full_columns(own, ahead, behind, lines, parity):
    tall, held, _ = own.shape
    groups = held // lines

    def kernel(p_ref, own_ref, ahead_ref, behind_ref, o_ref):
        def put(half, i, value):
            first = pl.multiple_of((half * groups + i) * HD, HD)
            o_ref[:, :, pl.ds(first, HD)] = value

        for i in range(groups):
            put(p_ref[0], i, own_ref[:, i * lines : (i + 1) * lines])
        for i in range(groups // 2):
            cut = slice(i * lines, (i + 1) * lines)
            put(1 - p_ref[0], i, ahead_ref[:, cut])
            put(1 - p_ref[0], i + groups // 2, behind_ref[:, cut])

    out = jax.ShapeDtypeStruct((tall, lines, 2 * groups * HD), BF16)
    return call(kernel, out, parity[None], own, ahead, behind)


def key_positions(chosen):
    per_dev, nsel = chosen.shape

    def kernel(c_ref, o_ref):
        lane = lax.broadcasted_iota(jnp.int32, (1, nsel * BLOCK), 1)
        for j in range(per_dev):
            row = jnp.zeros((1, nsel * BLOCK), jnp.int32)
            for n in range(nsel):
                first = jnp.where(c_ref[j, n] >= 0, c_ref[j, n] * BLOCK, NEVER)
                row = jnp.where(lane // BLOCK == n, first, row)
            o_ref[j] = row + lane % BLOCK

    out = jax.ShapeDtypeStruct((per_dev, 1, nsel * BLOCK), jnp.int32)
    return call(kernel, out, chosen)


def pick_blocks(blocks, asked):
    wide, count = asked.shape

    def kernel(asked_ref, b_ref, o_ref):
        for y in range(wide):
            for i in range(count):
                o_ref[y, i] = b_ref[asked_ref[y, i]]

    out = jax.ShapeDtypeStruct((wide, count, *blocks.shape[1:]), BF16)
    return call(kernel, out, asked, blocks)


def attend(queries, incoming, local_blocks, position, key_pos, facts):
    rows, width = queries.shape
    heads = width // HD
    far = incoming.shape[0]
    per_dev, nsel = position.shape
    keys = nsel * BLOCK

    def kernel(f_ref, p_ref, q_ref, in_ref, own_ref, kp_ref, o_ref, tab, k_s, v_s):
        tab[:far] = in_ref[...]
        tab[far:] = own_ref[...]
        for j in range(per_dev):
            for n in range(nsel):
                block = tab[p_ref[j, n]]
                k_s[j % 2, n * BLOCK : (n + 1) * BLOCK] = block[:, :HD]
                v_s[j % 2, n * BLOCK : (n + 1) * BLOCK] = block[:, HD:]
            mine = slice(j * BLOCK, (j + 1) * BLOCK)
            q = jnp.concatenate(
                [q_ref[mine, h * HD : (h + 1) * HD] for h in range(heads)], axis=0
            )
            scores = lax.dot_general(
                q, k_s[j % 2], (((1,), (1,)), ((), ())), preferred_element_type=F32
            ) * HD ** (-0.5)
            line = lax.broadcasted_iota(jnp.int32, (heads * BLOCK, 1), 0) % BLOCK
            at = f_ref[0] + j * BLOCK + line
            masked = jnp.where(kp_ref[j] <= at, scores, -jnp.inf)
            top = jnp.max(masked, axis=1, keepdims=True)
            weights = jnp.exp(masked - top)
            total = jnp.sum(weights, axis=1, keepdims=True)
            summed = jnp.dot(weights.astype(BF16), v_s[j % 2], preferred_element_type=F32)
            result = jnp.where(at < f_ref[1], summed / total, 0.0).astype(BF16)
            for h in range(heads):
                first = pl.multiple_of(((f_ref[2] + h) % heads) * HD, HD)
                o_ref[mine, pl.ds(first, HD)] = result[h * BLOCK : (h + 1) * BLOCK]

    return call(
        kernel,
        jax.ShapeDtypeStruct((rows, width), BF16),
        facts,
        position,
        queries,
        incoming,
        local_blocks,
        key_pos,
        scratch=(
            pltpu.VMEM((far + per_dev, BLOCK, 2 * HD), BF16),
            pltpu.VMEM((2, keys, HD), BF16),
            pltpu.VMEM((2, keys, HD), BF16),
        ),
        flops=4 * rows * keys * width,
    )


def mix(mine, other, pieces, places):
    n = len(pieces)
    tall, lines, width = pieces[0].shape
    half = tall // 2

    def kernel(p_ref, m_ref, t_ref, *refs):
        o_ref, w_s = refs[n], refs[n + 1]
        for s in range(n):
            w_s[:, (p_ref[0] + s) % n] = refs[s][...]
        first = w_s[pl.ds(p_ref[1] * half, half)].reshape(half * n * lines, width)
        second = w_s[pl.ds((1 - p_ref[1]) * half, half)].reshape(half * n * lines, width)
        o_ref[...] = (
            jnp.dot(m_ref[...], first, preferred_element_type=F32)
            + jnp.dot(t_ref[...], second, preferred_element_type=F32)
        ).astype(BF16)

    out = jax.ShapeDtypeStruct((mine.shape[0], width), BF16)
    scratch = (pltpu.VMEM((tall, n, lines, width), BF16),)
    flops = 4 * mine.size * width
    return call(kernel, out, places, mine, other, *pieces, scratch=scratch, flops=flops)


def body(tokens, query_weight, key_weight, value_weight, out_weight, chosen, live_length):
    rows = tokens.shape[0]
    per_dev = rows // BLOCK
    planes, tall, wide = (lax.axis_size(a) for a in ("dp", "kv_0", "kv_1"))
    x_at, z_at, y_at = (lax.axis_index(a) for a in ("dp", "kv_0", "kv_1"))
    owners = tall * wide
    me = z_at * wide + y_at

    parity = x_at % 2
    lines = out_weight.shape[0]
    halves, cargo = pack(query_weight, key_weight, value_weight, out_weight, x_at, planes, tall)
    halves = lax.all_gather(halves, "kv_0", axis=0, tiled=False)

    pair_rows = cargo.shape[1]
    column = lax.all_to_all(cargo, "kv_0", 0, 0, tiled=True)
    every = copy_for_each(column, ("dp", "kv_1"))
    every = every.reshape(planes, wide, tall, pair_rows, HD)
    paired = project_pair(tokens, every)
    paired, halves, late_chosen = after(paired, halves, chosen)
    local_blocks = paired.reshape(per_dev, BLOCK, paired.shape[1])
    column_blocks = lax.all_gather(local_blocks, "kv_0", axis=0, tiled=True)

    q_lines = halves.shape[1] // 2
    q_pieces = spread(halves[:, :q_lines], "kv_1")
    o_own = halves[:, q_lines:]
    cut = o_own.shape[1] // 2
    o_ahead = from_ahead(o_own[:, :cut], "dp", 1)
    o_behind = from_ahead(o_own[:, cut:], "dp", -1)
    q_tall = turned(q_pieces, y_at).reshape(2, -1, HD)
    q_pieces = [
        q_tall[0], q_tall[1], from_ahead(q_tall[0], "dp", 1), from_ahead(q_tall[1], "dp", -1)
    ]
    o_pieces = spread(full_columns(o_own, o_ahead, o_behind, lines, parity), "kv_1")

    mates = spread(late_chosen, "kv_1")
    column_owners = jnp.arange(tall, dtype=jnp.int32) * wide + y_at
    asked = jnp.stack(
        [
            slots_wanted(mates[s], column_owners, per_dev, z_at * wide + (y_at + s) % wide)
            for s in range(wide)
        ]
    )
    asked = jnp.maximum(asked, 0) + (jnp.arange(tall, dtype=jnp.int32) * per_dev)[None, :, None]
    asked = jnp.roll(asked.reshape(wide, tall * CAP), y_at, axis=0)
    safe = jnp.maximum(late_chosen, 0)
    wanted = slots_wanted(late_chosen, jnp.arange(owners, dtype=jnp.int32), per_dev, me)
    holder = safe // per_dev
    local_of = safe % per_dev
    match = (wanted[None, None, :, :] == local_of[:, :, None, None]) & (
        jnp.arange(owners, dtype=jnp.int32)[None, None, :, None] == holder[:, :, None, None]
    )
    slot = jnp.sum(
        jnp.where(match, jnp.arange(CAP, dtype=jnp.int32)[None, None, None], 0), axis=(2, 3)
    )
    far = wide * tall * CAP
    remote_at = ((holder % wide) * tall + holder // wide) * CAP + slot
    position = jnp.where(holder == me, far + local_of, remote_at)
    key_pos = key_positions(late_chosen)
    facts = jnp.stack([me * rows, live_length[0], 2 * parity]).astype(jnp.int32)

    outgoing = pick_blocks(column_blocks, asked)
    incoming = lax.all_to_all(outgoing, "kv_1", split_axis=0, concat_axis=0, tiled=True)
    queries = project_queries(tokens, q_pieces, outgoing[0, 0, :16, :HD])
    attended = attend(
        queries,
        incoming.reshape(far, BLOCK, paired.shape[1]),
        local_blocks,
        position,
        key_pos,
        facts,
    )
    other = from_ahead(attended, "tp", 1)
    places = jnp.stack([y_at, lax.axis_index("tp")]).astype(jnp.int32)
    return mix(attended, other, o_pieces, places)


def solution(mesh):
    split = Mesh(
        mesh.devices.reshape(mesh.shape["dp"], 16, 4, mesh.shape["tp"]),
        ("dp", "kv_0", "kv_1", "tp"),
    )
    placed = (
        P(DP_KV, None),
        P(KV, "tp"),
        P(KV, "tp"),
        P(KV, "tp"),
        P(KV, "tp"),
        P(DP_KV, None),
        P("dp"),
    )

    return jax.shard_map(
        body, mesh=split, in_specs=placed, out_specs=P(DP_KV, "tp"), check_vma=False
    )
```

```python
import jax
import jax.numpy as jnp
from jax import lax
from jax.experimental import pallas as pl
from jax.experimental.pallas import tpu as pltpu
from jax.sharding import Mesh
from jax.sharding import PartitionSpec as P


HD = 128
BLOCK = 32
CAP = 2
NEVER = 1 << 30
TALL = ("zh", "zl")
NEAR = ("zl", "y")
KV = ("zh", "zl", "y")
DP_KV = ("dp", "zh", "zl", "y")
F32 = jnp.float32
BF16 = jnp.bfloat16


def call(kernel, out_shape, *args, scratch=(), flops=0):
    spaces = [
        pl.BlockSpec(memory_space=pltpu.SMEM if a.dtype == jnp.int32 and a.ndim < 3 else pltpu.VMEM)
        for a in args
    ]
    return pl.pallas_call(
        kernel,
        out_shape=out_shape,
        in_specs=spaces,
        out_specs=jax.tree.map(lambda _: pl.BlockSpec(memory_space=pltpu.VMEM), out_shape),
        scratch_shapes=list(scratch),
        compiler_params=pltpu.CompilerParams(vmem_limit_bytes=40 << 20),
        cost_estimate=pl.CostEstimate(flops=flops, bytes_accessed=0, transcendentals=0),
    )(*args)


def copy_for_each(shard, axis):
    count = lax.axis_size(axis)
    return lax.all_to_all(
        jnp.broadcast_to(shard[None], (count, *shard.shape)), axis, 0, 0, tiled=True
    )


def from_ahead(x, axis, step):
    n = lax.axis_size(axis)
    return lax.ppermute(x, axis, [((i + step) % n, i) for i in range(n)])


def spread(x, axis):
    steps = range(1, lax.axis_size(axis))
    return [x, *(from_ahead(x, axis, s) for s in steps)]


def slots_wanted(chosen, owners, per_dev, readers):
    ids = owners[:, None] * per_dev + jnp.arange(per_dev, dtype=jnp.int32)[None, :]
    hits = chosen[:, :, None, None] == ids[None, None]
    needed = jnp.any(hits, axis=1) & (owners[None, :] != readers[:, None])[:, :, None]
    ranks = jnp.cumsum(needed.astype(jnp.int32), axis=2)
    local_ids = jnp.arange(per_dev, dtype=jnp.int32)
    lists = []
    for slot in range(CAP):
        marked = needed & (ranks == slot + 1)
        found = jnp.any(marked, axis=2)
        lists.append(jnp.where(found, jnp.sum(jnp.where(marked, local_ids, 0), axis=2), -1))
    return jnp.stack(lists, axis=2)


def pack(query_weight, key_weight, value_weight, out_weight, x_at, planes, tall):
    rows = key_weight.shape[0]
    lines, wide_out = out_weight.shape
    small = rows // planes
    groups = wide_out // planes // HD

    def kernel(x_ref, q_ref, k_ref, v_ref, o_ref, part_ref, cargo_ref):
        part_ref[:rows] = q_ref[:, pl.ds(pl.multiple_of(x_ref[0] * HD, HD), HD)]
        for i in range(groups):
            first = pl.multiple_of((x_ref[0] * groups + i) * HD, HD)
            part_ref[rows + i * lines : rows + (i + 1) * lines] = o_ref[:, pl.ds(first, HD)]
        first = pl.multiple_of(x_ref[0] * small, small)
        keys = k_ref[pl.ds(first, small)]
        values = v_ref[pl.ds(first, small)]
        for z in range(tall):
            cargo_ref[z, :small] = keys
            cargo_ref[z, small:] = values

    outs = (
        jax.ShapeDtypeStruct((rows + groups * lines, HD), BF16),
        jax.ShapeDtypeStruct((tall, 2 * small, HD), BF16),
    )
    return call(kernel, outs, x_at[None], query_weight, key_weight, value_weight, out_weight)


def joined(pieces, at):
    n = len(pieces)

    def kernel(at_ref, *refs):
        for s in range(n):
            refs[-1][(at_ref[0] + s) % n] = refs[s][...]

    out = jax.ShapeDtypeStruct((n, *pieces[0].shape), BF16)
    return call(kernel, out, at[None], *pieces)


def columns_of(pieces, at, rows):
    n = len(pieces)
    high, both, _ = pieces[0].shape

    def kernel(at_ref, *refs):
        for s in range(n):
            for h in range(high):
                z = h * n + (at_ref[0] + s) % n
                refs[n][z] = refs[s][h, :rows]
                refs[n + 1][z] = refs[s][h, rows:]

    outs = (
        jax.ShapeDtypeStruct((high * n, rows, HD), BF16),
        jax.ShapeDtypeStruct((high * n, both - rows, HD), BF16),
    )
    return call(kernel, outs, at[None], *pieces)


def project_pair(tokens, every):
    planes, wide, tall, both, _ = every.shape
    small = both // 2
    deep = planes * wide * small

    def kernel(t_ref, w_ref, o_ref):
        total = jnp.zeros(o_ref.shape, F32)
        for z in range(tall):
            lines = [(x, y) for y in range(wide) for x in range(planes)]
            keys = jnp.concatenate([w_ref[x, y, z, :small] for x, y in lines], axis=0)
            values = jnp.concatenate([w_ref[x, y, z, small:] for x, y in lines], axis=0)
            total += jnp.dot(
                t_ref[:, z * deep : (z + 1) * deep],
                jnp.concatenate([keys, values], axis=1),
                preferred_element_type=F32,
            )
        o_ref[...] = total.astype(BF16)

    out = jax.ShapeDtypeStruct((tokens.shape[0], 2 * HD), BF16)
    flops = 2 * tokens.size * 2 * HD
    return call(kernel, out, tokens, every, flops=flops)


def project_queries(tokens, pieces, tile):
    def kernel(t_ref, *refs):
        o_ref = refs[-1]
        for i in range(0, len(pieces), 2):
            w = jnp.concatenate([refs[i][...], refs[i + 1][...]], axis=1)
            o_ref[:, i * HD : (i + 2) * HD] = jnp.dot(
                t_ref[...], w, preferred_element_type=F32
            ).astype(BF16)

    width = len(pieces) * HD
    out = jax.ShapeDtypeStruct((tokens.shape[0], width), BF16)
    flops = 2 * tokens.size * width
    return call(kernel, out, tokens, *pieces, tile, flops=flops)


def turned(pieces, at):
    n = len(pieces)
    tall, rows, _ = pieces[0].shape

    def kernel(at_ref, *refs):
        for s in range(n):
            refs[-1][:, (at_ref[0] + s) % n] = refs[s][...]

    out = jax.ShapeDtypeStruct((tall, n, rows, HD), BF16)
    return call(kernel, out, at[None], *pieces)


def full_columns(pieces, at, lines):
    n = len(pieces)
    tall, held, _ = pieces[0].shape
    groups = held // lines

    def kernel(at_ref, *refs):
        for s in range(n):
            for i in range(groups):
                first = pl.multiple_of((((at_ref[0] + s) % n) * groups + i) * HD, HD)
                refs[n][:, :, pl.ds(first, HD)] = refs[s][:, i * lines : (i + 1) * lines]

    out = jax.ShapeDtypeStruct((tall, lines, n * groups * HD), BF16)
    return call(kernel, out, at[None], *pieces)


def key_positions(chosen):
    per_dev, nsel = chosen.shape

    def kernel(c_ref, o_ref):
        lane = lax.broadcasted_iota(jnp.int32, (1, nsel * BLOCK), 1)
        for j in range(per_dev):
            row = jnp.zeros((1, nsel * BLOCK), jnp.int32)
            for n in range(nsel):
                first = jnp.where(c_ref[j, n] >= 0, c_ref[j, n] * BLOCK, NEVER)
                row = jnp.where(lane // BLOCK == n, first, row)
            o_ref[j] = row + lane % BLOCK

    out = jax.ShapeDtypeStruct((per_dev, 1, nsel * BLOCK), jnp.int32)
    return call(kernel, out, chosen)


def pick_blocks(blocks, asked, places):
    low, wide, count = asked.shape

    def kernel(asked_ref, p_ref, b_ref, o_ref):
        for t in range(low):
            for s in range(wide):
                to = ((p_ref[0] + t) % low) * wide + (p_ref[1] + s) % wide
                for i in range(count):
                    o_ref[to, i] = b_ref[asked_ref[t * wide + s, i]]

    out = jax.ShapeDtypeStruct((low * wide, count, *blocks.shape[1:]), BF16)
    flat = asked.reshape(low * wide, count)
    return call(kernel, out, flat, places, blocks)


def attend(queries, incoming, local_blocks, position, key_pos, facts):
    rows, width = queries.shape
    heads = width // HD
    far = incoming.shape[0]
    per_dev, nsel = position.shape
    keys = nsel * BLOCK

    def kernel(f_ref, p_ref, q_ref, in_ref, own_ref, kp_ref, o_ref, tab, k_s, v_s):
        tab[:far] = in_ref[...]
        tab[far:] = own_ref[...]
        for j in range(per_dev):
            for n in range(nsel):
                block = tab[p_ref[j, n]]
                k_s[j % 2, n * BLOCK : (n + 1) * BLOCK] = block[:, :HD]
                v_s[j % 2, n * BLOCK : (n + 1) * BLOCK] = block[:, HD:]
            mine = slice(j * BLOCK, (j + 1) * BLOCK)
            q = jnp.concatenate(
                [q_ref[mine, h * HD : (h + 1) * HD] for h in range(heads)], axis=0
            )
            scores = lax.dot_general(
                q, k_s[j % 2], (((1,), (1,)), ((), ())), preferred_element_type=F32
            ) * HD ** (-0.5)
            line = lax.broadcasted_iota(jnp.int32, (heads * BLOCK, 1), 0) % BLOCK
            at = f_ref[0] + j * BLOCK + line
            masked = jnp.where(kp_ref[j] <= at, scores, -jnp.inf)
            top = jnp.max(masked, axis=1, keepdims=True)
            weights = jnp.exp(masked - top)
            total = jnp.sum(weights, axis=1, keepdims=True)
            summed = jnp.dot(weights.astype(BF16), v_s[j % 2], preferred_element_type=F32)
            result = jnp.where(at < f_ref[1], summed / total, 0.0).astype(BF16)
            for h in range(heads):
                first = pl.multiple_of(((f_ref[2] + h) % heads) * HD, HD)
                o_ref[mine, pl.ds(first, HD)] = result[h * BLOCK : (h + 1) * BLOCK]

    return call(
        kernel,
        jax.ShapeDtypeStruct((rows, width), BF16),
        facts,
        position,
        queries,
        incoming,
        local_blocks,
        key_pos,
        scratch=(
            pltpu.VMEM((far + per_dev, BLOCK, 2 * HD), BF16),
            pltpu.VMEM((2, keys, HD), BF16),
            pltpu.VMEM((2, keys, HD), BF16),
        ),
        flops=4 * rows * keys * width,
    )


def mix(mine, other, pieces, places):
    n = len(pieces)
    tall, lines, width = pieces[0].shape
    half = tall // 2

    def kernel(p_ref, m_ref, t_ref, *refs):
        o_ref, w_s = refs[n], refs[n + 1]
        for s in range(n):
            w_s[:, (p_ref[0] + s) % n] = refs[s][...]
        first = w_s[pl.ds(p_ref[1] * half, half)].reshape(half * n * lines, width)
        second = w_s[pl.ds((1 - p_ref[1]) * half, half)].reshape(half * n * lines, width)
        o_ref[...] = (
            jnp.dot(m_ref[...], first, preferred_element_type=F32)
            + jnp.dot(t_ref[...], second, preferred_element_type=F32)
        ).astype(BF16)

    out = jax.ShapeDtypeStruct((mine.shape[0], width), BF16)
    scratch = (pltpu.VMEM((tall, n, lines, width), BF16),)
    flops = 4 * mine.size * width
    return call(kernel, out, places, mine, other, *pieces, scratch=scratch, flops=flops)


def body(tokens, query_weight, key_weight, value_weight, out_weight, chosen, live_length):
    rows = tokens.shape[0]
    per_dev = rows // BLOCK
    planes, high, low, wide = (lax.axis_size(a) for a in ("dp", "zh", "zl", "y"))
    x_at, h_at, l_at, y_at = (lax.axis_index(a) for a in ("dp", "zh", "zl", "y"))
    tall = high * low
    owners = tall * wide
    me = lax.axis_index(KV)
    places = jnp.stack([l_at, y_at])

    part, cargo = pack(query_weight, key_weight, value_weight, out_weight, x_at, planes, tall)
    column = lax.all_to_all(cargo, TALL, 0, 0, tiled=True)
    parts = spread(part, "zh")
    every = copy_for_each(column, ("dp", "y"))
    every = every.reshape(planes, wide, tall, cargo.shape[1], HD)
    parts = spread(joined(parts, h_at), "zl")
    paired = project_pair(tokens, every)
    local_blocks = paired.reshape(per_dev, BLOCK, paired.shape[1])
    class_blocks = copy_for_each(local_blocks, "zh")

    q_small, o_small = columns_of(parts, l_at, query_weight.shape[0])
    q_pieces = spread(q_small, "y")
    o_pieces = spread(o_small, "dp")
    q_pieces = spread(turned(q_pieces, y_at).reshape(-1, HD), "dp")
    o_pieces = spread(full_columns(o_pieces, x_at, out_weight.shape[0]), "y")

    mates = jnp.stack(spread(chosen.reshape(-1), "y"))
    mates = jnp.stack(spread(mates, "zl"))
    ahead = jnp.arange(low, dtype=jnp.int32)[:, None], jnp.arange(wide, dtype=jnp.int32)[None, :]
    readers = (h_at * low + (l_at + ahead[0]) % low) * wide + (y_at + ahead[1]) % wide
    highs = jnp.arange(high, dtype=jnp.int32)
    asked = slots_wanted(
        mates.reshape(low * wide, -1),
        (highs * low + l_at) * wide + y_at,
        per_dev,
        readers.reshape(-1),
    )
    asked = jnp.maximum(asked, 0) + (highs * per_dev)[None, :, None]
    outgoing = pick_blocks(
        class_blocks.reshape(high * per_dev, BLOCK, paired.shape[1]),
        asked.reshape(low, wide, high * CAP),
        places,
    )
    incoming = lax.all_to_all(outgoing, NEAR, split_axis=0, concat_axis=0, tiled=True)

    safe = jnp.maximum(chosen, 0)
    wanted = slots_wanted(
        chosen.reshape(1, -1), jnp.arange(owners, dtype=jnp.int32), per_dev, me[None]
    )[0]
    holder = safe // per_dev
    local_of = safe % per_dev
    match = (wanted[None, None, :, :] == local_of[:, :, None, None]) & (
        jnp.arange(owners, dtype=jnp.int32)[None, None, :, None] == holder[:, :, None, None]
    )
    slot = jnp.sum(
        jnp.where(match, jnp.arange(CAP, dtype=jnp.int32)[None, None, None], 0), axis=(2, 3)
    )
    far = owners * CAP
    remote_at = ((holder % (low * wide)) * high + holder // (low * wide)) * CAP + slot
    position = jnp.where(holder == me, far + local_of, remote_at)
    key_pos = key_positions(chosen)
    facts = jnp.stack([me * rows, live_length[0], x_at]).astype(jnp.int32)

    queries = project_queries(tokens, q_pieces, outgoing[0, 0, :16, :HD])
    attended = attend(
        queries,
        incoming.reshape(far, BLOCK, paired.shape[1]),
        local_blocks,
        position,
        key_pos,
        facts,
    )
    other = from_ahead(attended, "tp", 1)
    cores = jnp.stack([y_at, lax.axis_index("tp")])
    return mix(attended, other, o_pieces, cores)


def solution(mesh):
    split = Mesh(
        mesh.devices.reshape(mesh.shape["dp"], 4, 4, 4, mesh.shape["tp"]),
        ("dp", "zh", "zl", "y", "tp"),
    )
    placed = (
        P(DP_KV, None),
        P(KV, "tp"),
        P(KV, "tp"),
        P(KV, "tp"),
        P(KV, "tp"),
        P(DP_KV, None),
        P("dp"),
    )

    return jax.shard_map(
        body, mesh=split, in_specs=placed, out_specs=P(DP_KV, "tp"), check_vma=False
    )
```

```python
import jax
import jax.numpy as jnp
from jax import lax
from jax.experimental import pallas as pl
from jax.experimental.pallas import tpu as pltpu
from jax.sharding import Mesh
from jax.sharding import PartitionSpec as P


HD = 128
BLOCK = 32
CAP = 2
NEVER = 1 << 30
TALL = ("zh", "zl")
KV = ("zh", "zl", "y")
DP_KV = ("dp", "zh", "zl", "y")
F32 = jnp.float32
BF16 = jnp.bfloat16


def call(kernel, out_shape, *args, scratch=(), flops=0):
    spaces = [
        pl.BlockSpec(memory_space=pltpu.SMEM if a.dtype == jnp.int32 and a.ndim < 3 else pltpu.VMEM)
        for a in args
    ]
    return pl.pallas_call(
        kernel,
        out_shape=out_shape,
        in_specs=spaces,
        out_specs=jax.tree.map(lambda _: pl.BlockSpec(memory_space=pltpu.VMEM), out_shape),
        scratch_shapes=list(scratch),
        compiler_params=pltpu.CompilerParams(vmem_limit_bytes=40 << 20),
        cost_estimate=pl.CostEstimate(flops=flops, bytes_accessed=0, transcendentals=0),
    )(*args)


def copy_for_each(shard, axis):
    count = lax.axis_size(axis)
    return lax.all_to_all(
        jnp.broadcast_to(shard[None], (count, *shard.shape)), axis, 0, 0, tiled=True
    )


def from_ahead(x, axis, step):
    n = lax.axis_size(axis)
    return lax.ppermute(x, axis, [((i + step) % n, i) for i in range(n)])


def spread(x, axis):
    steps = range(1, lax.axis_size(axis))
    return [x, *(from_ahead(x, axis, s) for s in steps)]


def slots_wanted(chosen, owners, per_dev, readers):
    ids = owners[:, None] * per_dev + jnp.arange(per_dev, dtype=jnp.int32)[None, :]
    hits = chosen[:, :, None, None] == ids[None, None]
    needed = jnp.any(hits, axis=1) & (owners[None, :] != readers[:, None])[:, :, None]
    ranks = jnp.cumsum(needed.astype(jnp.int32), axis=2)
    local_ids = jnp.arange(per_dev, dtype=jnp.int32)
    lists = []
    for slot in range(CAP):
        marked = needed & (ranks == slot + 1)
        found = jnp.any(marked, axis=2)
        lists.append(jnp.where(found, jnp.sum(jnp.where(marked, local_ids, 0), axis=2), -1))
    return jnp.stack(lists, axis=2)


def pack(query_weight, key_weight, value_weight, out_weight, x_at, planes, tall):
    rows = key_weight.shape[0]
    lines, wide_out = out_weight.shape
    small = rows // planes
    groups = wide_out // planes // HD

    def kernel(x_ref, q_hbm, k_hbm, v_hbm, o_hbm, part_ref, cargo_ref, *scratch):
        held, sems = scratch[:4], scratch[4]
        copies = [
            pltpu.make_async_copy(src, dst, sems.at[i])
            for i, (src, dst) in enumerate(zip((q_hbm, k_hbm, v_hbm, o_hbm), held, strict=True))
        ]
        for copy in copies:
            copy.start()
        for copy in copies:
            copy.wait()
        q_ref, k_ref, v_ref, o_ref = held
        part_ref[:rows] = q_ref[:, pl.ds(pl.multiple_of(x_ref[0] * HD, HD), HD)]
        for i in range(groups):
            first = pl.multiple_of((x_ref[0] * groups + i) * HD, HD)
            part_ref[rows + i * lines : rows + (i + 1) * lines] = o_ref[:, pl.ds(first, HD)]
        first = pl.multiple_of(x_ref[0] * small, small)
        keys = k_ref[pl.ds(first, small)]
        values = v_ref[pl.ds(first, small)]
        for z in range(tall):
            cargo_ref[z, :small] = keys
            cargo_ref[z, small:] = values

    weights = (query_weight, key_weight, value_weight, out_weight)
    outs = (
        jax.ShapeDtypeStruct((rows + groups * lines, HD), BF16),
        jax.ShapeDtypeStruct((tall, 2 * small, HD), BF16),
    )
    return pl.pallas_call(
        kernel,
        out_shape=outs,
        in_specs=[pl.BlockSpec(memory_space=pltpu.SMEM)] + [pl.BlockSpec(memory_space=pl.ANY)] * 4,
        out_specs=(pl.BlockSpec(memory_space=pltpu.VMEM),) * 2,
        scratch_shapes=[pltpu.VMEM(w.shape, BF16) for w in weights]
        + [pltpu.SemaphoreType.DMA((4,))],
        name="pack",
    )(x_at[None], *weights)


def joined(pieces, at):
    n = len(pieces)

    def kernel(at_ref, *refs):
        for s in range(n):
            refs[-1][(at_ref[0] + s) % n] = refs[s][...]

    out = jax.ShapeDtypeStruct((n, *pieces[0].shape), BF16)
    return call(kernel, out, at[None], *pieces)


def columns_of(pieces, at, rows):
    n = len(pieces)
    high, both, _ = pieces[0].shape

    def kernel(at_ref, *refs):
        for s in range(n):
            for h in range(high):
                z = h * n + (at_ref[0] + s) % n
                refs[n][z] = refs[s][h, :rows]
                refs[n + 1][z] = refs[s][h, rows:]

    outs = (
        jax.ShapeDtypeStruct((high * n, rows, HD), BF16),
        jax.ShapeDtypeStruct((high * n, both - rows, HD), BF16),
    )
    return call(kernel, outs, at[None], *pieces)


def project_pair(tokens, every):
    planes, wide, tall, both, _ = every.shape
    small = both // 2
    deep = planes * wide * small

    def kernel(t_ref, w_ref, o_ref):
        total = jnp.zeros(o_ref.shape, F32)
        for z in range(tall):
            lines = [(x, y) for y in range(wide) for x in range(planes)]
            keys = jnp.concatenate([w_ref[x, y, z, :small] for x, y in lines], axis=0)
            values = jnp.concatenate([w_ref[x, y, z, small:] for x, y in lines], axis=0)
            total += jnp.dot(
                t_ref[:, z * deep : (z + 1) * deep],
                jnp.concatenate([keys, values], axis=1),
                preferred_element_type=F32,
            )
        o_ref[...] = total.astype(BF16)

    out = jax.ShapeDtypeStruct((tokens.shape[0], 2 * HD), BF16)
    flops = 2 * tokens.size * 2 * HD
    return call(kernel, out, tokens, every, flops=flops)


def project_queries(tokens, pieces, tile):
    def kernel(t_ref, *refs):
        o_ref = refs[-1]
        for i in range(0, len(pieces), 2):
            w = jnp.concatenate([refs[i][...], refs[i + 1][...]], axis=1)
            o_ref[:, i * HD : (i + 2) * HD] = jnp.dot(
                t_ref[...], w, preferred_element_type=F32
            ).astype(BF16)

    width = len(pieces) * HD
    out = jax.ShapeDtypeStruct((tokens.shape[0], width), BF16)
    flops = 2 * tokens.size * width
    return call(kernel, out, tokens, *pieces, tile, flops=flops)


def turned(pieces, at):
    n = len(pieces)
    tall, rows, _ = pieces[0].shape

    def kernel(at_ref, *refs):
        for s in range(n):
            refs[-1][:, (at_ref[0] + s) % n] = refs[s][...]

    out = jax.ShapeDtypeStruct((tall, n, rows, HD), BF16)
    return call(kernel, out, at[None], *pieces)


def full_columns(pieces, at, lines):
    n = len(pieces)
    tall, held, _ = pieces[0].shape
    groups = held // lines

    def kernel(at_ref, *refs):
        for s in range(n):
            for i in range(groups):
                first = pl.multiple_of((((at_ref[0] + s) % n) * groups + i) * HD, HD)
                refs[n][:, :, pl.ds(first, HD)] = refs[s][:, i * lines : (i + 1) * lines]

    out = jax.ShapeDtypeStruct((tall, lines, n * groups * HD), BF16)
    return call(kernel, out, at[None], *pieces)


def key_positions(chosen):
    per_dev, nsel = chosen.shape

    def kernel(c_ref, o_ref):
        lane = lax.broadcasted_iota(jnp.int32, (1, nsel * BLOCK), 1)
        for j in range(per_dev):
            row = jnp.zeros((1, nsel * BLOCK), jnp.int32)
            for n in range(nsel):
                first = jnp.where(c_ref[j, n] >= 0, c_ref[j, n] * BLOCK, NEVER)
                row = jnp.where(lane // BLOCK == n, first, row)
            o_ref[j] = row + lane % BLOCK

    out = jax.ShapeDtypeStruct((per_dev, 1, nsel * BLOCK), jnp.int32)
    return call(kernel, out, chosen)


def pick_blocks(blocks, asked, at):
    wide, count = asked.shape

    def kernel(asked_ref, at_ref, b_ref, o_ref):
        for s in range(wide):
            for i in range(count):
                o_ref[(at_ref[0] + s) % wide, i] = b_ref[asked_ref[s, i]]

    out = jax.ShapeDtypeStruct((wide, count, *blocks.shape[1:]), BF16)
    return call(kernel, out, asked, at[None], blocks)


def attend(queries, incoming, local_blocks, position, key_pos, facts):
    rows, width = queries.shape
    heads = width // HD
    far = incoming.shape[0]
    per_dev, nsel = position.shape
    keys = nsel * BLOCK

    def kernel(f_ref, p_ref, q_ref, in_ref, own_ref, kp_ref, o_ref, tab, k_s, v_s):
        tab[:far] = in_ref[...]
        tab[far:] = own_ref[...]
        for j in range(per_dev):
            for n in range(nsel):
                block = tab[p_ref[j, n]]
                k_s[j % 2, n * BLOCK : (n + 1) * BLOCK] = block[:, :HD]
                v_s[j % 2, n * BLOCK : (n + 1) * BLOCK] = block[:, HD:]
            mine = slice(j * BLOCK, (j + 1) * BLOCK)
            q = jnp.concatenate(
                [q_ref[mine, h * HD : (h + 1) * HD] for h in range(heads)], axis=0
            )
            scores = lax.dot_general(
                q, k_s[j % 2], (((1,), (1,)), ((), ())), preferred_element_type=F32
            ) * HD ** (-0.5)
            line = lax.broadcasted_iota(jnp.int32, (heads * BLOCK, 1), 0) % BLOCK
            at = f_ref[0] + j * BLOCK + line
            masked = jnp.where(kp_ref[j] <= at, scores, -jnp.inf)
            top = jnp.max(masked, axis=1, keepdims=True)
            weights = jnp.exp(masked - top)
            total = jnp.sum(weights, axis=1, keepdims=True)
            summed = jnp.dot(weights.astype(BF16), v_s[j % 2], preferred_element_type=F32)
            result = jnp.where(at < f_ref[1], summed / total, 0.0).astype(BF16)
            for h in range(heads):
                first = pl.multiple_of(((f_ref[2] + h) % heads) * HD, HD)
                o_ref[mine, pl.ds(first, HD)] = result[h * BLOCK : (h + 1) * BLOCK]

    return call(
        kernel,
        jax.ShapeDtypeStruct((rows, width), BF16),
        facts,
        position,
        queries,
        incoming,
        local_blocks,
        key_pos,
        scratch=(
            pltpu.VMEM((far + per_dev, BLOCK, 2 * HD), BF16),
            pltpu.VMEM((2, keys, HD), BF16),
            pltpu.VMEM((2, keys, HD), BF16),
        ),
        flops=4 * rows * keys * width,
    )


def whole_rows(pieces, at):
    n = len(pieces)
    tall, lines, width = pieces[0].shape

    def kernel(at_ref, *refs):
        for s in range(n):
            refs[-1][:, (at_ref[0] + s) % n] = refs[s][...]

    out = jax.ShapeDtypeStruct((tall, n, lines, width), BF16)
    return call(kernel, out, at[None], *pieces)


def mix(mine, other, weight, core):
    half = weight.shape[0] // 2

    def kernel(c_ref, m_ref, t_ref, w_ref, o_ref):
        first = w_ref[pl.ds(c_ref[0] * half, half)]
        second = w_ref[pl.ds((1 - c_ref[0]) * half, half)]
        o_ref[...] = (
            jnp.dot(m_ref[...], first, preferred_element_type=F32)
            + jnp.dot(t_ref[...], second, preferred_element_type=F32)
        ).astype(BF16)

    out = jax.ShapeDtypeStruct((mine.shape[0], weight.shape[1]), BF16)
    flops = 4 * mine.size * weight.shape[1]
    return call(kernel, out, core[None], mine, other, weight, flops=flops)


def body(tokens, query_weight, key_weight, value_weight, out_weight, chosen, live_length):
    rows = tokens.shape[0]
    per_dev = rows // BLOCK
    planes, high, low, wide = (lax.axis_size(a) for a in ("dp", "zh", "zl", "y"))
    x_at, h_at, l_at, y_at = (lax.axis_index(a) for a in ("dp", "zh", "zl", "y"))
    tall = high * low
    owners = tall * wide
    me = lax.axis_index(KV)

    part, cargo = pack(query_weight, key_weight, value_weight, out_weight, x_at, planes, tall)
    column = lax.all_to_all(cargo, TALL, 0, 0, tiled=True)
    parts = spread(part, "zh")
    every = copy_for_each(column, ("dp", "y"))
    every = every.reshape(planes, wide, tall, cargo.shape[1], HD)
    parts = spread(joined(parts, h_at), "zl")
    paired = project_pair(tokens, every)
    local_blocks = paired.reshape(per_dev, BLOCK, paired.shape[1])
    column_blocks = lax.all_gather(local_blocks, TALL, axis=0, tiled=True)

    q_small, o_small = columns_of(parts, l_at, query_weight.shape[0])
    q_pieces = spread(q_small, "y")
    o_pieces = spread(o_small, "dp")
    q_pieces = spread(turned(q_pieces, y_at).reshape(-1, HD), "dp")
    o_pieces = spread(full_columns(o_pieces, x_at, out_weight.shape[0]), "y")

    mates = jnp.stack(spread(chosen.reshape(-1), "y"))
    mates, chosen = lax.optimization_barrier((mates, chosen))
    depth = jnp.arange(tall, dtype=jnp.int32)
    readers = (h_at * low + l_at) * wide + (y_at + jnp.arange(wide, dtype=jnp.int32)) % wide
    asked = slots_wanted(mates, depth * wide + y_at, per_dev, readers)
    asked = jnp.maximum(asked, 0) + (depth * per_dev)[None, :, None]
    outgoing = pick_blocks(column_blocks, asked.reshape(wide, tall * CAP), y_at)
    incoming = lax.all_to_all(outgoing, "y", split_axis=0, concat_axis=0, tiled=True)

    safe = jnp.maximum(chosen, 0)
    wanted = slots_wanted(
        chosen.reshape(1, -1), jnp.arange(owners, dtype=jnp.int32), per_dev, me[None]
    )[0]
    holder = safe // per_dev
    local_of = safe % per_dev
    match = (wanted[None, None, :, :] == local_of[:, :, None, None]) & (
        jnp.arange(owners, dtype=jnp.int32)[None, None, :, None] == holder[:, :, None, None]
    )
    slot = jnp.sum(
        jnp.where(match, jnp.arange(CAP, dtype=jnp.int32)[None, None, None], 0), axis=(2, 3)
    )
    far = owners * CAP
    remote_at = ((holder % wide) * tall + holder // wide) * CAP + slot
    position = jnp.where(holder == me, far + local_of, remote_at)
    key_pos = key_positions(chosen)
    facts = jnp.stack([me * rows, live_length[0], x_at]).astype(jnp.int32)

    queries = project_queries(tokens, q_pieces, outgoing[0, 0, :16, :HD])
    attended = attend(
        queries,
        incoming.reshape(far, BLOCK, paired.shape[1]),
        local_blocks,
        position,
        key_pos,
        facts,
    )
    other = from_ahead(attended, "tp", 1)
    out_full = whole_rows(o_pieces, y_at)
    out_full = out_full.reshape(-1, out_full.shape[-1])
    return mix(attended, other, out_full, lax.axis_index("tp"))


def solution(mesh):
    split = Mesh(
        mesh.devices.reshape(mesh.shape["dp"], 4, 4, 4, mesh.shape["tp"]),
        ("dp", "zh", "zl", "y", "tp"),
    )
    placed = (
        P(DP_KV, None),
        P(KV, "tp"),
        P(KV, "tp"),
        P(KV, "tp"),
        P(KV, "tp"),
        P(DP_KV, None),
        P("dp"),
    )

    return jax.shard_map(
        body, mesh=split, in_specs=placed, out_specs=P(DP_KV, "tp"), check_vma=False
    )
```

```python
import jax
import jax.numpy as jnp
from jax import lax
from jax.experimental import pallas as pl
from jax.experimental.pallas import tpu as pltpu
from jax.sharding import Mesh
from jax.sharding import PartitionSpec as P


HD = 128
BLOCK = 32
CAP = 2
NEVER = 1 << 30
TALL = ("zh", "zl")
KV = ("zh", "zl", "y")
DP_KV = ("dp", "zh", "zl", "y")
F32 = jnp.float32
BF16 = jnp.bfloat16


def call(kernel, out_shape, *args, scratch=(), flops=0):
    spaces = [
        pl.BlockSpec(memory_space=pltpu.SMEM if a.dtype == jnp.int32 and a.ndim < 3 else pltpu.VMEM)
        for a in args
    ]
    return pl.pallas_call(
        kernel,
        out_shape=out_shape,
        in_specs=spaces,
        out_specs=jax.tree.map(lambda _: pl.BlockSpec(memory_space=pltpu.VMEM), out_shape),
        scratch_shapes=list(scratch),
        compiler_params=pltpu.CompilerParams(vmem_limit_bytes=40 << 20),
        cost_estimate=pl.CostEstimate(flops=flops, bytes_accessed=0, transcendentals=0),
    )(*args)


def copy_for_each(shard, axis):
    count = lax.axis_size(axis)
    return lax.all_to_all(
        jnp.broadcast_to(shard[None], (count, *shard.shape)), axis, 0, 0, tiled=True
    )


def from_ahead(x, axis, step):
    n = lax.axis_size(axis)
    return lax.ppermute(x, axis, [((i + step) % n, i) for i in range(n)])


def spread(x, axis):
    steps = range(1, lax.axis_size(axis))
    return [x, *(from_ahead(x, axis, s) for s in steps)]


def slots_wanted(chosen, owners, per_dev, readers):
    ids = owners[:, None] * per_dev + jnp.arange(per_dev, dtype=jnp.int32)[None, :]
    hits = chosen[:, :, None, None] == ids[None, None]
    needed = jnp.any(hits, axis=1) & (owners[None, :] != readers[:, None])[:, :, None]
    ranks = jnp.cumsum(needed.astype(jnp.int32), axis=2)
    local_ids = jnp.arange(per_dev, dtype=jnp.int32)
    lists = []
    for slot in range(CAP):
        marked = needed & (ranks == slot + 1)
        found = jnp.any(marked, axis=2)
        lists.append(jnp.where(found, jnp.sum(jnp.where(marked, local_ids, 0), axis=2), -1))
    return jnp.stack(lists, axis=2)


def pack(query_weight, key_weight, value_weight, out_weight, x_at, planes, tall):
    rows = key_weight.shape[0]
    lines, wide_out = out_weight.shape
    small = rows // planes
    groups = wide_out // planes // HD

    def kernel(x_ref, q_hbm, k_hbm, v_hbm, o_hbm, part_ref, cargo_ref, *scratch):
        held, sems = scratch[:4], scratch[4]
        copies = [
            pltpu.make_async_copy(src, dst, sems.at[i])
            for i, (src, dst) in enumerate(zip((q_hbm, k_hbm, v_hbm, o_hbm), held, strict=True))
        ]
        for copy in copies:
            copy.start()
        for copy in copies:
            copy.wait()
        q_ref, k_ref, v_ref, o_ref = held
        part_ref[:rows] = q_ref[:, pl.ds(pl.multiple_of(x_ref[0] * HD, HD), HD)]
        for i in range(groups):
            first = pl.multiple_of((x_ref[0] * groups + i) * HD, HD)
            part_ref[rows + i * lines : rows + (i + 1) * lines] = o_ref[:, pl.ds(first, HD)]
        first = pl.multiple_of(x_ref[0] * small, small)
        keys = k_ref[pl.ds(first, small)]
        values = v_ref[pl.ds(first, small)]
        for z in range(tall):
            cargo_ref[z, :small] = keys
            cargo_ref[z, small:] = values

    weights = (query_weight, key_weight, value_weight, out_weight)
    outs = (
        jax.ShapeDtypeStruct((rows + groups * lines, HD), BF16),
        jax.ShapeDtypeStruct((tall, 2 * small, HD), BF16),
    )
    return pl.pallas_call(
        kernel,
        out_shape=outs,
        in_specs=[pl.BlockSpec(memory_space=pltpu.SMEM)] + [pl.BlockSpec(memory_space=pl.ANY)] * 4,
        out_specs=(pl.BlockSpec(memory_space=pltpu.VMEM),) * 2,
        scratch_shapes=[pltpu.VMEM(w.shape, BF16) for w in weights]
        + [pltpu.SemaphoreType.DMA((4,))],
        name="pack",
    )(x_at[None], *weights)


def joined(pieces, at):
    n = len(pieces)

    def kernel(at_ref, *refs):
        for s in range(n):
            refs[-1][(at_ref[0] + s) % n] = refs[s][...]

    out = jax.ShapeDtypeStruct((n, *pieces[0].shape), BF16)
    return call(kernel, out, at[None], *pieces)


def columns_of(pieces, at, rows):
    n = len(pieces)
    high, both, _ = pieces[0].shape

    def kernel(at_ref, *refs):
        for s in range(n):
            for h in range(high):
                z = h * n + (at_ref[0] + s) % n
                refs[n][z] = refs[s][h, :rows]
                refs[n + 1][z] = refs[s][h, rows:]

    outs = (
        jax.ShapeDtypeStruct((high * n, rows, HD), BF16),
        jax.ShapeDtypeStruct((high * n, both - rows, HD), BF16),
    )
    return call(kernel, outs, at[None], *pieces)


def project_pair(tokens, every):
    planes, wide, tall, both, _ = every.shape
    small = both // 2
    deep = planes * wide * small

    chunk = 4

    def kernel(t_ref, w_hbm, o_ref, w_ref, sems):
        copies = [
            pltpu.make_async_copy(
                w_hbm.at[:, :, pl.ds(i * chunk, chunk)], w_ref.at[i], sems.at[i]
            )
            for i in range(tall // chunk)
        ]
        for copy in copies:
            copy.start()
        total = jnp.zeros(o_ref.shape, F32)
        lines = [(x, y) for y in range(wide) for x in range(planes)]
        for z in range(tall):
            i, j = z // chunk, z % chunk
            if j == 0:
                copies[i].wait()
            keys = jnp.concatenate([w_ref[i, x, y, j, :small] for x, y in lines], axis=0)
            values = jnp.concatenate([w_ref[i, x, y, j, small:] for x, y in lines], axis=0)
            total += jnp.dot(
                t_ref[:, z * deep : (z + 1) * deep],
                jnp.concatenate([keys, values], axis=1),
                preferred_element_type=F32,
            )
        o_ref[...] = total.astype(BF16)

    return pl.pallas_call(
        kernel,
        out_shape=jax.ShapeDtypeStruct((tokens.shape[0], 2 * HD), BF16),
        in_specs=[pl.BlockSpec(memory_space=pltpu.VMEM), pl.BlockSpec(memory_space=pl.ANY)],
        out_specs=pl.BlockSpec(memory_space=pltpu.VMEM),
        scratch_shapes=[
            pltpu.VMEM((tall // chunk, planes, wide, chunk, both, HD), BF16),
            pltpu.SemaphoreType.DMA((tall // chunk,)),
        ],
        compiler_params=pltpu.CompilerParams(vmem_limit_bytes=40 << 20),
        cost_estimate=pl.CostEstimate(
            flops=4 * tokens.size * HD, bytes_accessed=0, transcendentals=0
        ),
        name="project_pair",
    )(tokens, every)


def project_queries(tokens, pieces, tile):
    def kernel(t_ref, *refs):
        o_ref = refs[-1]
        for i in range(0, len(pieces), 2):
            w = jnp.concatenate([refs[i][...], refs[i + 1][...]], axis=1)
            o_ref[:, i * HD : (i + 2) * HD] = jnp.dot(
                t_ref[...], w, preferred_element_type=F32
            ).astype(BF16)

    width = len(pieces) * HD
    out = jax.ShapeDtypeStruct((tokens.shape[0], width), BF16)
    flops = 2 * tokens.size * width
    return call(kernel, out, tokens, *pieces, tile, flops=flops)


def turned(pieces, at):
    n = len(pieces)
    tall, rows, _ = pieces[0].shape

    def kernel(at_ref, *refs):
        for s in range(n):
            refs[-1][:, (at_ref[0] + s) % n] = refs[s][...]

    out = jax.ShapeDtypeStruct((tall, n, rows, HD), BF16)
    return call(kernel, out, at[None], *pieces)


def full_columns(pieces, at, lines):
    n = len(pieces)
    tall, held, _ = pieces[0].shape
    groups = held // lines

    def kernel(at_ref, *refs):
        for s in range(n):
            for i in range(groups):
                first = pl.multiple_of((((at_ref[0] + s) % n) * groups + i) * HD, HD)
                refs[n][:, :, pl.ds(first, HD)] = refs[s][:, i * lines : (i + 1) * lines]

    out = jax.ShapeDtypeStruct((tall, lines, n * groups * HD), BF16)
    return call(kernel, out, at[None], *pieces)


def key_positions(chosen):
    per_dev, nsel = chosen.shape

    def kernel(c_ref, o_ref):
        lane = lax.broadcasted_iota(jnp.int32, (1, nsel * BLOCK), 1)
        for j in range(per_dev):
            row = jnp.zeros((1, nsel * BLOCK), jnp.int32)
            for n in range(nsel):
                first = jnp.where(c_ref[j, n] >= 0, c_ref[j, n] * BLOCK, NEVER)
                row = jnp.where(lane // BLOCK == n, first, row)
            o_ref[j] = row + lane % BLOCK

    out = jax.ShapeDtypeStruct((per_dev, 1, nsel * BLOCK), jnp.int32)
    return call(kernel, out, chosen)


def pick_blocks(blocks, asked, at):
    wide, count = asked.shape

    def kernel(asked_ref, at_ref, b_hbm, o_ref, sem):
        for s in range(wide):
            to = (at_ref[0] + s) % wide
            for i in range(count):
                pltpu.make_async_copy(b_hbm.at[asked_ref[s, i]], o_ref.at[to, i], sem).start()
        pltpu.make_async_copy(o_ref, o_ref, sem).wait()

    return pl.pallas_call(
        kernel,
        out_shape=jax.ShapeDtypeStruct((wide, count, *blocks.shape[1:]), BF16),
        in_specs=[
            pl.BlockSpec(memory_space=pltpu.SMEM),
            pl.BlockSpec(memory_space=pltpu.SMEM),
            pl.BlockSpec(memory_space=pl.ANY),
        ],
        out_specs=pl.BlockSpec(memory_space=pltpu.VMEM),
        scratch_shapes=[pltpu.SemaphoreType.DMA],
        name="pick_blocks",
    )(asked, at[None], blocks)


def attend(queries, incoming, local_blocks, position, key_pos, facts):
    rows, width = queries.shape
    heads = width // HD
    far = incoming.shape[0]
    per_dev, nsel = position.shape
    keys = nsel * BLOCK

    def kernel(f_ref, p_ref, q_ref, in_ref, own_ref, kp_ref, o_ref, tab, k_s, v_s):
        tab[:far] = in_ref[...]
        tab[far:] = own_ref[...]
        for j in range(per_dev):
            for n in range(nsel):
                block = tab[p_ref[j, n]]
                k_s[j % 2, n * BLOCK : (n + 1) * BLOCK] = block[:, :HD]
                v_s[j % 2, n * BLOCK : (n + 1) * BLOCK] = block[:, HD:]
            mine = slice(j * BLOCK, (j + 1) * BLOCK)
            q = jnp.concatenate(
                [q_ref[mine, h * HD : (h + 1) * HD] for h in range(heads)], axis=0
            )
            scores = lax.dot_general(
                q, k_s[j % 2], (((1,), (1,)), ((), ())), preferred_element_type=F32
            ) * HD ** (-0.5)
            line = lax.broadcasted_iota(jnp.int32, (heads * BLOCK, 1), 0) % BLOCK
            at = f_ref[0] + j * BLOCK + line
            masked = jnp.where(kp_ref[j] <= at, scores, -jnp.inf)
            top = jnp.max(masked, axis=1, keepdims=True)
            weights = jnp.exp(masked - top)
            total = jnp.sum(weights, axis=1, keepdims=True)
            summed = jnp.dot(weights.astype(BF16), v_s[j % 2], preferred_element_type=F32)
            result = jnp.where(at < f_ref[1], summed / total, 0.0).astype(BF16)
            for h in range(heads):
                first = pl.multiple_of(((f_ref[2] + h) % heads) * HD, HD)
                o_ref[mine, pl.ds(first, HD)] = result[h * BLOCK : (h + 1) * BLOCK]

    return call(
        kernel,
        jax.ShapeDtypeStruct((rows, width), BF16),
        facts,
        position,
        queries,
        incoming,
        local_blocks,
        key_pos,
        scratch=(
            pltpu.VMEM((far + per_dev, BLOCK, 2 * HD), BF16),
            pltpu.VMEM((2, keys, HD), BF16),
            pltpu.VMEM((2, keys, HD), BF16),
        ),
        flops=4 * rows * keys * width,
    )


def whole_rows(pieces, at):
    n = len(pieces)
    tall, lines, width = pieces[0].shape

    def kernel(at_ref, *refs):
        for s in range(n):
            refs[-1][:, (at_ref[0] + s) % n] = refs[s][...]

    out = jax.ShapeDtypeStruct((tall, n, lines, width), BF16)
    return call(kernel, out, at[None], *pieces)


def mix(mine, other, weight, core):
    half = weight.shape[0] // 2

    def kernel(c_ref, m_ref, t_ref, w_ref, o_ref):
        first = w_ref[pl.ds(c_ref[0] * half, half)]
        second = w_ref[pl.ds((1 - c_ref[0]) * half, half)]
        o_ref[...] = (
            jnp.dot(m_ref[...], first, preferred_element_type=F32)
            + jnp.dot(t_ref[...], second, preferred_element_type=F32)
        ).astype(BF16)

    out = jax.ShapeDtypeStruct((mine.shape[0], weight.shape[1]), BF16)
    flops = 4 * mine.size * weight.shape[1]
    return call(kernel, out, core[None], mine, other, weight, flops=flops)


def body(tokens, query_weight, key_weight, value_weight, out_weight, chosen, live_length):
    rows = tokens.shape[0]
    per_dev = rows // BLOCK
    planes, high, low, wide = (lax.axis_size(a) for a in ("dp", "zh", "zl", "y"))
    x_at, h_at, l_at, y_at = (lax.axis_index(a) for a in ("dp", "zh", "zl", "y"))
    tall = high * low
    owners = tall * wide
    me = lax.axis_index(KV)

    part, cargo = pack(query_weight, key_weight, value_weight, out_weight, x_at, planes, tall)
    column = lax.all_to_all(cargo, TALL, 0, 0, tiled=True)
    parts = spread(part, "zh")
    every = copy_for_each(column, ("dp", "y"))
    every = every.reshape(planes, wide, tall, cargo.shape[1], HD)
    parts = spread(joined(parts, h_at), "zl")
    paired = project_pair(tokens, every)
    local_blocks = paired.reshape(per_dev, BLOCK, paired.shape[1])
    column_blocks = lax.all_gather(local_blocks, TALL, axis=0, tiled=True)

    q_small, o_small = columns_of(parts, l_at, query_weight.shape[0])
    q_pieces = spread(q_small, "y")
    o_pieces = spread(o_small, "dp")
    q_pieces = spread(turned(q_pieces, y_at).reshape(-1, HD), "dp")
    o_pieces = spread(full_columns(o_pieces, x_at, out_weight.shape[0]), "y")

    mates = jnp.stack(spread(chosen.reshape(-1), "y"))
    mates, chosen = lax.optimization_barrier((mates, chosen))
    depth = jnp.arange(tall, dtype=jnp.int32)
    readers = (h_at * low + l_at) * wide + (y_at + jnp.arange(wide, dtype=jnp.int32)) % wide
    asked = slots_wanted(mates, depth * wide + y_at, per_dev, readers)
    asked = jnp.maximum(asked, 0) + (depth * per_dev)[None, :, None]
    outgoing = pick_blocks(column_blocks, asked.reshape(wide, tall * CAP), y_at)
    incoming = lax.all_to_all(outgoing, "y", split_axis=0, concat_axis=0, tiled=True)

    safe = jnp.maximum(chosen, 0)
    wanted = slots_wanted(
        chosen.reshape(1, -1), jnp.arange(owners, dtype=jnp.int32), per_dev, me[None]
    )[0]
    holder = safe // per_dev
    local_of = safe % per_dev
    match = (wanted[None, None, :, :] == local_of[:, :, None, None]) & (
        jnp.arange(owners, dtype=jnp.int32)[None, None, :, None] == holder[:, :, None, None]
    )
    slot = jnp.sum(
        jnp.where(match, jnp.arange(CAP, dtype=jnp.int32)[None, None, None], 0), axis=(2, 3)
    )
    far = owners * CAP
    remote_at = ((holder % wide) * tall + holder // wide) * CAP + slot
    position = jnp.where(holder == me, far + local_of, remote_at)
    key_pos = key_positions(chosen)
    facts = jnp.stack([me * rows, live_length[0], x_at]).astype(jnp.int32)

    queries = project_queries(tokens, q_pieces, outgoing[0, 0, :16, :HD])
    attended = attend(
        queries,
        incoming.reshape(far, BLOCK, paired.shape[1]),
        local_blocks,
        position,
        key_pos,
        facts,
    )
    other = from_ahead(attended, "tp", 1)
    out_full = whole_rows(o_pieces, y_at)
    out_full = out_full.reshape(-1, out_full.shape[-1])
    return mix(attended, other, out_full, lax.axis_index("tp"))


def solution(mesh):
    split = Mesh(
        mesh.devices.reshape(mesh.shape["dp"], 4, 4, 4, mesh.shape["tp"]),
        ("dp", "zh", "zl", "y", "tp"),
    )
    placed = (
        P(DP_KV, None),
        P(KV, "tp"),
        P(KV, "tp"),
        P(KV, "tp"),
        P(KV, "tp"),
        P(DP_KV, None),
        P("dp"),
    )

    return jax.shard_map(
        body, mesh=split, in_specs=placed, out_specs=P(DP_KV, "tp"), check_vma=False
    )
```

```python
import jax
import jax.numpy as jnp
from jax import lax
from jax.experimental import pallas as pl
from jax.experimental.pallas import tpu as pltpu
from jax.sharding import Mesh
from jax.sharding import PartitionSpec as P


HD = 128
BLOCK = 32
CAP = 2
NEVER = 1 << 30
TALL = ("zh", "zl")
KV = ("zh", "zl", "y")
DP_KV = ("dp", "zh", "zl", "y")
F32 = jnp.float32
BF16 = jnp.bfloat16


def call(kernel, out_shape, *args, scratch=(), flops=0):
    spaces = [
        pl.BlockSpec(memory_space=pltpu.SMEM if a.dtype == jnp.int32 and a.ndim < 3 else pltpu.VMEM)
        for a in args
    ]
    return pl.pallas_call(
        kernel,
        out_shape=out_shape,
        in_specs=spaces,
        out_specs=jax.tree.map(lambda _: pl.BlockSpec(memory_space=pltpu.VMEM), out_shape),
        scratch_shapes=list(scratch),
        compiler_params=pltpu.CompilerParams(vmem_limit_bytes=40 << 20),
        cost_estimate=pl.CostEstimate(flops=flops, bytes_accessed=0, transcendentals=0),
    )(*args)


def copy_for_each(shard, axis):
    count = lax.axis_size(axis)
    return lax.all_to_all(
        jnp.broadcast_to(shard[None], (count, *shard.shape)), axis, 0, 0, tiled=True
    )


def from_ahead(x, axis, step):
    n = lax.axis_size(axis)
    return lax.ppermute(x, axis, [((i + step) % n, i) for i in range(n)])


def spread(x, axis):
    steps = range(1, lax.axis_size(axis))
    return [x, *(from_ahead(x, axis, s) for s in steps)]


def slots_wanted(chosen, owners, per_dev, readers):
    ids = owners[:, None] * per_dev + jnp.arange(per_dev, dtype=jnp.int32)[None, :]
    hits = chosen[:, :, None, None] == ids[None, None]
    needed = jnp.any(hits, axis=1) & (owners[None, :] != readers[:, None])[:, :, None]
    ranks = jnp.cumsum(needed.astype(jnp.int32), axis=2)
    local_ids = jnp.arange(per_dev, dtype=jnp.int32)
    lists = []
    for slot in range(CAP):
        marked = needed & (ranks == slot + 1)
        found = jnp.any(marked, axis=2)
        lists.append(jnp.where(found, jnp.sum(jnp.where(marked, local_ids, 0), axis=2), -1))
    return jnp.stack(lists, axis=2)


def pack(key_weight, value_weight, out_weight, x_at, planes, tall):
    rows = key_weight.shape[0]
    lines, wide_out = out_weight.shape
    small = rows // planes
    groups = wide_out // planes // HD

    def kernel(x_ref, k_hbm, v_hbm, o_hbm, part_ref, cargo_ref, *scratch):
        held, sems = scratch[:3], scratch[3]
        copies = [
            pltpu.make_async_copy(src, dst, sems.at[i])
            for i, (src, dst) in enumerate(zip((k_hbm, v_hbm, o_hbm), held, strict=True))
        ]
        for copy in copies:
            copy.start()
        for copy in copies:
            copy.wait()
        k_ref, v_ref, o_ref = held
        for i in range(groups):
            first = pl.multiple_of((x_ref[0] * groups + i) * HD, HD)
            part_ref[i * lines : (i + 1) * lines] = o_ref[:, pl.ds(first, HD)]
        first = pl.multiple_of(x_ref[0] * small, small)
        keys = k_ref[pl.ds(first, small)]
        values = v_ref[pl.ds(first, small)]
        for z in range(tall):
            cargo_ref[z, :small] = keys
            cargo_ref[z, small:] = values

    weights = (key_weight, value_weight, out_weight)
    outs = (
        jax.ShapeDtypeStruct((groups * lines, HD), BF16),
        jax.ShapeDtypeStruct((tall, 2 * small, HD), BF16),
    )
    return pl.pallas_call(
        kernel,
        out_shape=outs,
        in_specs=[pl.BlockSpec(memory_space=pltpu.SMEM)] + [pl.BlockSpec(memory_space=pl.ANY)] * 3,
        out_specs=(pl.BlockSpec(memory_space=pltpu.VMEM),) * 2,
        scratch_shapes=[pltpu.VMEM(w.shape, BF16) for w in weights]
        + [pltpu.SemaphoreType.DMA((3,))],
        name="pack",
    )(x_at[None], *weights)


def joined(pieces, at):
    n = len(pieces)

    def kernel(at_ref, *refs):
        for s in range(n):
            refs[-1][(at_ref[0] + s) % n] = refs[s][...]

    out = jax.ShapeDtypeStruct((n, *pieces[0].shape), BF16)
    return call(kernel, out, at[None], *pieces)


def columns_of(pieces, at):
    n = len(pieces)
    high, rows, _ = pieces[0].shape

    def kernel(at_ref, *refs):
        for s in range(n):
            for h in range(high):
                refs[-1][h * n + (at_ref[0] + s) % n] = refs[s][h]

    out = jax.ShapeDtypeStruct((high * n, rows, HD), BF16)
    return call(kernel, out, at[None], *pieces)


def project_pair(tokens, every):
    planes, wide, tall, both, _ = every.shape
    small = both // 2
    deep = planes * wide * small

    def kernel(t_ref, w_ref, o_ref):
        total = jnp.zeros(o_ref.shape, F32)
        for z in range(tall):
            lines = [(x, y) for y in range(wide) for x in range(planes)]
            keys = jnp.concatenate([w_ref[x, y, z, :small] for x, y in lines], axis=0)
            values = jnp.concatenate([w_ref[x, y, z, small:] for x, y in lines], axis=0)
            total += jnp.dot(
                t_ref[:, z * deep : (z + 1) * deep],
                jnp.concatenate([keys, values], axis=1),
                preferred_element_type=F32,
            )
        o_ref[...] = total.astype(BF16)

    out = jax.ShapeDtypeStruct((tokens.shape[0], 2 * HD), BF16)
    flops = 2 * tokens.size * 2 * HD
    return call(kernel, out, tokens, every, flops=flops)


def project_queries(tokens, pieces, at, tile):
    n = len(pieces)
    tall, lines, width = pieces[0].shape

    def kernel(at_ref, t_ref, *refs):
        o_ref, w_s = refs[-2], refs[-1]
        for s in range(n):
            w_s[:, (at_ref[0] + s) % n] = refs[s][...]
        o_ref[...] = jnp.dot(
            t_ref[...], w_s[...].reshape(tall * n * lines, width), preferred_element_type=F32
        ).astype(BF16)

    return call(
        kernel,
        jax.ShapeDtypeStruct((tokens.shape[0], width), BF16),
        at[None],
        tokens,
        *pieces,
        tile,
        scratch=(pltpu.VMEM((tall, n, lines, width), BF16),),
        flops=2 * tokens.size * width,
    )


def full_rows(pieces, at, lines):
    n = len(pieces)
    tall, held, _ = pieces[0].shape
    groups = held // lines

    def kernel(at_ref, *refs):
        for s in range(n):
            y = (at_ref[0] + s) % n
            for i in range(groups):
                refs[-1][:, y, :, i * HD : (i + 1) * HD] = refs[s][:, i * lines : (i + 1) * lines]

    out = jax.ShapeDtypeStruct((tall, n, lines, groups * HD), BF16)
    return call(kernel, out, at[None], *pieces)


def key_positions(chosen):
    per_dev, nsel = chosen.shape

    def kernel(c_ref, o_ref):
        lane = lax.broadcasted_iota(jnp.int32, (1, nsel * BLOCK), 1)
        for j in range(per_dev):
            row = jnp.zeros((1, nsel * BLOCK), jnp.int32)
            for n in range(nsel):
                first = jnp.where(c_ref[j, n] >= 0, c_ref[j, n] * BLOCK, NEVER)
                row = jnp.where(lane // BLOCK == n, first, row)
            o_ref[j] = row + lane % BLOCK

    out = jax.ShapeDtypeStruct((per_dev, 1, nsel * BLOCK), jnp.int32)
    return call(kernel, out, chosen)


def pick_blocks(blocks, asked, at):
    wide, count = asked.shape

    def kernel(asked_ref, at_ref, b_ref, o_ref):
        for s in range(wide):
            for i in range(count):
                o_ref[(at_ref[0] + s) % wide, i] = b_ref[asked_ref[s, i]]

    out = jax.ShapeDtypeStruct((wide, count, *blocks.shape[1:]), BF16)
    return call(kernel, out, asked, at[None], blocks)


def attend(queries, incoming, local_blocks, position, key_pos, facts):
    rows, width = queries.shape
    heads = width // HD
    far = incoming.shape[0]
    per_dev, nsel = position.shape
    keys = nsel * BLOCK

    def kernel(f_ref, p_ref, q_ref, in_ref, own_ref, kp_ref, o_ref, tab, k_s, v_s):
        tab[:far] = in_ref[...]
        tab[far:] = own_ref[...]
        for j in range(per_dev):
            for n in range(nsel):
                block = tab[p_ref[j, n]]
                k_s[j % 2, n * BLOCK : (n + 1) * BLOCK] = block[:, :HD]
                v_s[j % 2, n * BLOCK : (n + 1) * BLOCK] = block[:, HD:]
            mine = slice(j * BLOCK, (j + 1) * BLOCK)
            q = jnp.concatenate(
                [q_ref[mine, h * HD : (h + 1) * HD] for h in range(heads)], axis=0
            )
            scores = lax.dot_general(
                q, k_s[j % 2], (((1,), (1,)), ((), ())), preferred_element_type=F32
            ) * HD ** (-0.5)
            line = lax.broadcasted_iota(jnp.int32, (heads * BLOCK, 1), 0) % BLOCK
            at = f_ref[0] + j * BLOCK + line
            masked = jnp.where(kp_ref[j] <= at, scores, -jnp.inf)
            top = jnp.max(masked, axis=1, keepdims=True)
            weights = jnp.exp(masked - top)
            total = jnp.sum(weights, axis=1, keepdims=True)
            summed = jnp.dot(weights.astype(BF16), v_s[j % 2], preferred_element_type=F32)
            result = jnp.where(at < f_ref[1], summed / total, 0.0).astype(BF16)
            for h in range(heads):
                o_ref[mine, h * HD : (h + 1) * HD] = result[h * BLOCK : (h + 1) * BLOCK]

    return call(
        kernel,
        jax.ShapeDtypeStruct((rows, width), BF16),
        facts,
        position,
        queries,
        incoming,
        local_blocks,
        key_pos,
        scratch=(
            pltpu.VMEM((far + per_dev, BLOCK, 2 * HD), BF16),
            pltpu.VMEM((2, keys, HD), BF16),
            pltpu.VMEM((2, keys, HD), BF16),
        ),
        flops=4 * rows * keys * width,
    )


def mix(mine, other, pieces, places):
    n = len(pieces)
    rows, width = pieces[0].shape
    half = rows // 2

    def kernel(p_ref, m_ref, t_ref, *refs):
        for s in range(n):
            first = pl.multiple_of(((p_ref[0] + s) % n) * width, width)
            refs[n][:, pl.ds(first, width)] = (
                jnp.dot(
                    m_ref[...], refs[s][pl.ds(p_ref[1] * half, half)], preferred_element_type=F32
                )
                + jnp.dot(
                    t_ref[...],
                    refs[s][pl.ds((1 - p_ref[1]) * half, half)],
                    preferred_element_type=F32,
                )
            ).astype(BF16)

    out = jax.ShapeDtypeStruct((mine.shape[0], n * width), BF16)
    flops = 4 * mine.size * n * width
    return call(kernel, out, places, mine, other, *pieces, flops=flops)


def body(tokens, query_weight, key_weight, value_weight, out_weight, chosen, live_length):
    rows = tokens.shape[0]
    per_dev = rows // BLOCK
    planes, high, low, wide = (lax.axis_size(a) for a in ("dp", "zh", "zl", "y"))
    x_at, h_at, l_at, y_at = (lax.axis_index(a) for a in ("dp", "zh", "zl", "y"))
    tall = high * low
    owners = tall * wide
    me = lax.axis_index(KV)

    q_column = lax.all_gather(query_weight, TALL, axis=0, tiled=True)
    part, cargo = pack(key_weight, value_weight, out_weight, x_at, planes, tall)
    column = lax.all_to_all(cargo, TALL, 0, 0, tiled=True)
    parts = spread(part, "zh")
    every = copy_for_each(column, ("dp", "y"))
    every = every.reshape(planes, wide, tall, cargo.shape[1], HD)
    parts = spread(joined(parts, h_at), "zl")
    paired = project_pair(tokens, every)
    local_blocks = paired.reshape(per_dev, BLOCK, paired.shape[1])
    column_blocks = lax.all_gather(local_blocks, TALL, axis=0, tiled=True)

    q_pieces = spread(q_column, "y")
    q_pieces = [p.reshape(tall, -1, p.shape[1]) for p in q_pieces]
    o_pieces = spread(columns_of(parts, l_at), "y")
    o_tall = full_rows(o_pieces, y_at, out_weight.shape[0])
    o_pieces = spread(o_tall.reshape(-1, o_tall.shape[-1]), "dp")

    key_pos = key_positions(chosen)

    mates = jnp.stack(spread(chosen.reshape(-1), "y"))
    mates, chosen = lax.optimization_barrier((mates, chosen))
    depth = jnp.arange(tall, dtype=jnp.int32)
    readers = (h_at * low + l_at) * wide + (y_at + jnp.arange(wide, dtype=jnp.int32)) % wide
    asked = slots_wanted(mates, depth * wide + y_at, per_dev, readers)
    asked = jnp.maximum(asked, 0) + (depth * per_dev)[None, :, None]
    outgoing = pick_blocks(column_blocks, asked.reshape(wide, tall * CAP), y_at)
    incoming = lax.all_to_all(outgoing, "y", split_axis=0, concat_axis=0, tiled=True)

    safe = jnp.maximum(chosen, 0)
    wanted = slots_wanted(
        chosen.reshape(1, -1), jnp.arange(owners, dtype=jnp.int32), per_dev, me[None]
    )[0]
    holder = safe // per_dev
    local_of = safe % per_dev
    match = (wanted[None, None, :, :] == local_of[:, :, None, None]) & (
        jnp.arange(owners, dtype=jnp.int32)[None, None, :, None] == holder[:, :, None, None]
    )
    slot = jnp.sum(
        jnp.where(match, jnp.arange(CAP, dtype=jnp.int32)[None, None, None], 0), axis=(2, 3)
    )
    far = owners * CAP
    remote_at = ((holder % wide) * tall + holder // wide) * CAP + slot
    position = jnp.where(holder == me, far + local_of, remote_at)
    facts = jnp.stack([me * rows, live_length[0]]).astype(jnp.int32)

    queries = project_queries(tokens, q_pieces, y_at, outgoing[0, 0, :16, :HD])
    attended = attend(
        queries,
        incoming.reshape(far, BLOCK, paired.shape[1]),
        local_blocks,
        position,
        key_pos,
        facts,
    )
    other = from_ahead(attended, "tp", 1)
    return mix(attended, other, o_pieces, jnp.stack([x_at, lax.axis_index("tp")]))


def solution(mesh):
    split = Mesh(
        mesh.devices.reshape(mesh.shape["dp"], 4, 4, 4, mesh.shape["tp"]),
        ("dp", "zh", "zl", "y", "tp"),
    )
    placed = (
        P(DP_KV, None),
        P(KV, "tp"),
        P(KV, "tp"),
        P(KV, "tp"),
        P(KV, "tp"),
        P(DP_KV, None),
        P("dp"),
    )

    return jax.shard_map(
        body, mesh=split, in_specs=placed, out_specs=P(DP_KV, "tp"), check_vma=False
    )
```

```python
import jax
import jax.numpy as jnp
from jax import lax
from jax.experimental import pallas as pl
from jax.experimental.pallas import tpu as pltpu
from jax.sharding import Mesh
from jax.sharding import PartitionSpec as P


HD = 128
BLOCK = 32
CAP = 2
NEVER = 1 << 30
KV = ("kv_0", "kv_1")
DP_KV = ("dp", "kv_0", "kv_1")
F32 = jnp.float32
BF16 = jnp.bfloat16


def call(kernel, out_shape, *args, scratch=(), flops=0):
    spaces = [
        pl.BlockSpec(memory_space=pltpu.SMEM if a.dtype == jnp.int32 and a.ndim < 3 else pltpu.VMEM)
        for a in args
    ]
    return pl.pallas_call(
        kernel,
        out_shape=out_shape,
        in_specs=spaces,
        out_specs=jax.tree.map(lambda _: pl.BlockSpec(memory_space=pltpu.VMEM), out_shape),
        scratch_shapes=list(scratch),
        compiler_params=pltpu.CompilerParams(vmem_limit_bytes=40 << 20),
        cost_estimate=pl.CostEstimate(flops=flops, bytes_accessed=0, transcendentals=0),
    )(*args)


def copy_for_each(shard, axis):
    count = lax.axis_size(axis)
    return lax.all_to_all(
        jnp.broadcast_to(shard[None], (count, *shard.shape)), axis, 0, 0, tiled=True
    )


def from_ahead(x, axis, step):
    n = lax.axis_size(axis)
    return lax.ppermute(x, axis, [((i + step) % n, i) for i in range(n)])


def spread(x, axis):
    steps = range(1, lax.axis_size(axis))
    return [x, *(from_ahead(x, axis, s) for s in steps)]


def after(*values):
    return lax.optimization_barrier(values)


def slots_wanted(chosen, owners, per_dev, me):
    ids = owners[:, None] * per_dev + jnp.arange(per_dev, dtype=jnp.int32)[None, :]
    hits = chosen.reshape(-1)[:, None, None] == ids[None]
    needed = jnp.any(hits, axis=0) & (owners != me)[:, None]
    ranks = jnp.cumsum(needed.astype(jnp.int32), axis=1)
    local_ids = jnp.arange(per_dev, dtype=jnp.int32)[None, :]
    lists = []
    for slot in range(CAP):
        marked = needed & (ranks == slot + 1)
        found = jnp.any(marked, axis=1)
        lists.append(jnp.where(found, jnp.sum(jnp.where(marked, local_ids, 0), axis=1), -1))
    return jnp.stack(lists, axis=1)


def pack(query_weight, key_weight, value_weight, out_weight, x_at, planes, tall):
    rows = key_weight.shape[0]
    lines, wide_out = out_weight.shape
    small = rows // planes
    q_groups = query_weight.shape[1] // 2 // HD
    o_groups = wide_out // 2 // HD

    def kernel(x_ref, q_hbm, k_hbm, v_hbm, o_hbm, half_ref, cargo_ref, *scratch):
        held, sems = scratch[:4], scratch[4]
        copies = [
            pltpu.make_async_copy(src, dst, sems.at[i])
            for i, (src, dst) in enumerate(zip((q_hbm, k_hbm, v_hbm, o_hbm), held, strict=True))
        ]
        for copy in copies:
            copy.start()
        for copy in copies:
            copy.wait()
        q_ref, k_ref, v_ref, o_ref = held
        parity = x_ref[0] % 2
        for i in range(q_groups):
            first = pl.multiple_of((parity * q_groups + i) * HD, HD)
            half_ref[i * rows : (i + 1) * rows] = q_ref[:, pl.ds(first, HD)]
        base = q_groups * rows
        for i in range(o_groups):
            first = pl.multiple_of((parity * o_groups + i) * HD, HD)
            half_ref[base + i * lines : base + (i + 1) * lines] = o_ref[:, pl.ds(first, HD)]
        first = pl.multiple_of(x_ref[0] * small, small)
        keys = k_ref[pl.ds(first, small)]
        values = v_ref[pl.ds(first, small)]
        for z in range(tall):
            cargo_ref[z, :small] = keys
            cargo_ref[z, small:] = values

    outs = (
        jax.ShapeDtypeStruct((q_groups * rows + o_groups * lines, HD), BF16),
        jax.ShapeDtypeStruct((tall, 2 * small, HD), BF16),
    )
    weights = (query_weight, key_weight, value_weight, out_weight)
    return pl.pallas_call(
        kernel,
        out_shape=outs,
        in_specs=[pl.BlockSpec(memory_space=pltpu.SMEM)] + [pl.BlockSpec(memory_space=pl.ANY)] * 4,
        out_specs=(pl.BlockSpec(memory_space=pltpu.VMEM),) * 2,
        scratch_shapes=[pltpu.VMEM(w.shape, BF16) for w in weights]
        + [pltpu.SemaphoreType.DMA((4,))],
        name="pack",
    )(x_at[None], *weights)


def project_pair(tokens, every):
    planes, wide, tall, both, _ = every.shape
    small = both // 2
    deep = planes * wide * small

    def kernel(t_ref, w_ref, o_ref):
        total = jnp.zeros(o_ref.shape, F32)
        for z in range(tall):
            lines = [(x, y) for y in range(wide) for x in range(planes)]
            keys = jnp.concatenate([w_ref[x, y, z, :small] for x, y in lines], axis=0)
            values = jnp.concatenate([w_ref[x, y, z, small:] for x, y in lines], axis=0)
            total += jnp.dot(
                t_ref[:, z * deep : (z + 1) * deep],
                jnp.concatenate([keys, values], axis=1),
                preferred_element_type=F32,
            )
        o_ref[...] = total.astype(BF16)

    out = jax.ShapeDtypeStruct((tokens.shape[0], 2 * HD), BF16)
    flops = 2 * tokens.size * 2 * HD
    return call(kernel, out, tokens, every, flops=flops)


def project_queries(tokens, pieces, tile):
    def kernel(t_ref, *refs):
        o_ref = refs[-1]
        for i in range(0, len(pieces), 2):
            w = jnp.concatenate([refs[i][...], refs[i + 1][...]], axis=1)
            o_ref[:, i * HD : (i + 2) * HD] = jnp.dot(
                t_ref[...], w, preferred_element_type=F32
            ).astype(BF16)

    width = len(pieces) * HD
    out = jax.ShapeDtypeStruct((tokens.shape[0], width), BF16)
    flops = 2 * tokens.size * width
    return call(kernel, out, tokens, *pieces, tile, flops=flops)


def turned(pieces, at):
    n = len(pieces)
    tall, lines, _ = pieces[0].shape
    columns = 2
    rows = lines // columns

    def kernel(at_ref, *refs):
        for s in range(n):
            y = (at_ref[0] + s) % n
            for i in range(columns):
                refs[-1][i, :, y] = refs[s][:, i * rows : (i + 1) * rows]

    out = jax.ShapeDtypeStruct((columns, tall, n, rows, HD), BF16)
    return call(kernel, out, at[None], *pieces)


def full_columns(own, ahead, behind, lines, parity):
    tall, held, _ = own.shape
    groups = held // lines

    def kernel(p_ref, own_ref, ahead_ref, behind_ref, o_ref):
        def put(half, i, value):
            first = pl.multiple_of((half * groups + i) * HD, HD)
            o_ref[:, :, pl.ds(first, HD)] = value

        for i in range(groups):
            put(p_ref[0], i, own_ref[:, i * lines : (i + 1) * lines])
        for i in range(groups // 2):
            cut = slice(i * lines, (i + 1) * lines)
            put(1 - p_ref[0], i, ahead_ref[:, cut])
            put(1 - p_ref[0], i + groups // 2, behind_ref[:, cut])

    out = jax.ShapeDtypeStruct((tall, lines, 2 * groups * HD), BF16)
    return call(kernel, out, parity[None], own, ahead, behind)


def key_positions(chosen):
    per_dev, nsel = chosen.shape

    def kernel(c_ref, o_ref):
        lane = lax.broadcasted_iota(jnp.int32, (1, nsel * BLOCK), 1)
        for j in range(per_dev):
            row = jnp.zeros((1, nsel * BLOCK), jnp.int32)
            for n in range(nsel):
                first = jnp.where(c_ref[j, n] >= 0, c_ref[j, n] * BLOCK, NEVER)
                row = jnp.where(lane // BLOCK == n, first, row)
            o_ref[j] = row + lane % BLOCK

    out = jax.ShapeDtypeStruct((per_dev, 1, nsel * BLOCK), jnp.int32)
    return call(kernel, out, chosen)


def pick_blocks(blocks, asked, per_dev):
    wide, count = asked.shape
    tall = count // CAP
    chunk = 4
    held = chunk * per_dev

    def kernel(asked_ref, b_hbm, o_ref, b_ref, sems):
        copies = [
            pltpu.make_async_copy(
                b_hbm.at[pl.ds(c * held, held)], b_ref.at[pl.ds(c * held, held)], sems.at[c]
            )
            for c in range(tall // chunk)
        ]
        for copy in copies:
            copy.start()
        for c, copy in enumerate(copies):
            copy.wait()
            for i in range(c * chunk * CAP, (c + 1) * chunk * CAP):
                for y in range(wide):
                    o_ref[y, i] = b_ref[asked_ref[y, i]]

    return pl.pallas_call(
        kernel,
        out_shape=jax.ShapeDtypeStruct((wide, count, *blocks.shape[1:]), BF16),
        in_specs=[pl.BlockSpec(memory_space=pltpu.SMEM), pl.BlockSpec(memory_space=pl.ANY)],
        out_specs=pl.BlockSpec(memory_space=pltpu.VMEM),
        scratch_shapes=[pltpu.VMEM(blocks.shape, BF16), pltpu.SemaphoreType.DMA((tall // chunk,))],
        name="pick_blocks",
    )(asked, blocks)


def attend(queries, incoming, local_blocks, position, key_pos, facts):
    rows, width = queries.shape
    heads = width // HD
    far = incoming.shape[0]
    per_dev, nsel = position.shape
    keys = nsel * BLOCK

    def kernel(f_ref, p_ref, q_ref, in_ref, own_ref, kp_ref, o_ref, tab, k_s, v_s):
        tab[:far] = in_ref[...]
        tab[far:] = own_ref[...]
        for j in range(per_dev):
            for n in range(nsel):
                block = tab[p_ref[j, n]]
                k_s[j % 2, n * BLOCK : (n + 1) * BLOCK] = block[:, :HD]
                v_s[j % 2, n * BLOCK : (n + 1) * BLOCK] = block[:, HD:]
            mine = slice(j * BLOCK, (j + 1) * BLOCK)
            q = jnp.concatenate(
                [q_ref[mine, h * HD : (h + 1) * HD] for h in range(heads)], axis=0
            )
            scores = lax.dot_general(
                q, k_s[j % 2], (((1,), (1,)), ((), ())), preferred_element_type=F32
            ) * HD ** (-0.5)
            line = lax.broadcasted_iota(jnp.int32, (heads * BLOCK, 1), 0) % BLOCK
            at = f_ref[0] + j * BLOCK + line
            masked = jnp.where(kp_ref[j] <= at, scores, -jnp.inf)
            top = jnp.max(masked, axis=1, keepdims=True)
            weights = jnp.exp(masked - top)
            total = jnp.sum(weights, axis=1, keepdims=True)
            summed = jnp.dot(weights.astype(BF16), v_s[j % 2], preferred_element_type=F32)
            result = jnp.where(at < f_ref[1], summed / total, 0.0).astype(BF16)
            for h in range(heads):
                first = pl.multiple_of(((f_ref[2] + h) % heads) * HD, HD)
                o_ref[mine, pl.ds(first, HD)] = result[h * BLOCK : (h + 1) * BLOCK]

    return call(
        kernel,
        jax.ShapeDtypeStruct((rows, width), BF16),
        facts,
        position,
        queries,
        incoming,
        local_blocks,
        key_pos,
        scratch=(
            pltpu.VMEM((far + per_dev, BLOCK, 2 * HD), BF16),
            pltpu.VMEM((2, keys, HD), BF16),
            pltpu.VMEM((2, keys, HD), BF16),
        ),
        flops=4 * rows * keys * width,
    )


def whole_rows(pieces, at, tile):
    n = len(pieces)
    tall, lines, width = pieces[0].shape

    def kernel(at_ref, *refs):
        for s in range(n):
            refs[-1][:, (at_ref[0] + s) % n] = refs[s][...]

    out = jax.ShapeDtypeStruct((tall, n, lines, width), BF16)
    return call(kernel, out, at[None], *pieces, tile)


def mix(mine, other, weight, core):
    half = weight.shape[0] // 2

    def kernel(c_ref, m_ref, t_ref, w_ref, o_ref):
        first = w_ref[pl.ds(c_ref[0] * half, half)]
        second = w_ref[pl.ds((1 - c_ref[0]) * half, half)]
        o_ref[...] = (
            jnp.dot(m_ref[...], first, preferred_element_type=F32)
            + jnp.dot(t_ref[...], second, preferred_element_type=F32)
        ).astype(BF16)

    out = jax.ShapeDtypeStruct((mine.shape[0], weight.shape[1]), BF16)
    flops = 4 * mine.size * weight.shape[1]
    return call(kernel, out, core[None], mine, other, weight, flops=flops)


def body(tokens, query_weight, key_weight, value_weight, out_weight, chosen, live_length):
    rows = tokens.shape[0]
    per_dev = rows // BLOCK
    planes, tall, wide = (lax.axis_size(a) for a in ("dp", "kv_0", "kv_1"))
    x_at, z_at, y_at = (lax.axis_index(a) for a in ("dp", "kv_0", "kv_1"))
    owners = tall * wide
    me = z_at * wide + y_at

    parity = x_at % 2
    lines = out_weight.shape[0]
    halves, cargo = pack(query_weight, key_weight, value_weight, out_weight, x_at, planes, tall)
    halves = lax.all_gather(halves, "kv_0", axis=0, tiled=False)

    pair_rows = cargo.shape[1]
    column = lax.all_to_all(cargo, "kv_0", 0, 0, tiled=True)
    every = copy_for_each(column, ("dp", "kv_1"))
    every = every.reshape(planes, wide, tall, pair_rows, HD)
    paired = project_pair(tokens, every)
    paired, halves, late_chosen = after(paired, halves, chosen)
    local_blocks = paired.reshape(per_dev, BLOCK, paired.shape[1])
    column_blocks = lax.all_gather(local_blocks, "kv_0", axis=0, tiled=True)

    q_lines = halves.shape[1] // 2
    q_pieces = spread(halves[:, :q_lines], "kv_1")
    o_own = halves[:, q_lines:]
    cut = o_own.shape[1] // 2
    o_ahead = from_ahead(o_own[:, :cut], "dp", 1)
    o_behind = from_ahead(o_own[:, cut:], "dp", -1)
    q_tall = turned(q_pieces, y_at).reshape(2, -1, HD)
    q_pieces = [
        q_tall[0], q_tall[1], from_ahead(q_tall[0], "dp", 1), from_ahead(q_tall[1], "dp", -1)
    ]
    o_pieces = spread(full_columns(o_own, o_ahead, o_behind, lines, parity), "kv_1")

    mates = spread(late_chosen, "kv_1")
    column_owners = jnp.arange(tall, dtype=jnp.int32) * wide + y_at
    asked = jnp.stack(
        [
            slots_wanted(mates[s], column_owners, per_dev, z_at * wide + (y_at + s) % wide)
            for s in range(wide)
        ]
    )
    asked = jnp.maximum(asked, 0) + (jnp.arange(tall, dtype=jnp.int32) * per_dev)[None, :, None]
    asked = jnp.roll(asked.reshape(wide, tall * CAP), y_at, axis=0)
    safe = jnp.maximum(late_chosen, 0)
    wanted = slots_wanted(late_chosen, jnp.arange(owners, dtype=jnp.int32), per_dev, me)
    holder = safe // per_dev
    local_of = safe % per_dev
    match = (wanted[None, None, :, :] == local_of[:, :, None, None]) & (
        jnp.arange(owners, dtype=jnp.int32)[None, None, :, None] == holder[:, :, None, None]
    )
    slot = jnp.sum(
        jnp.where(match, jnp.arange(CAP, dtype=jnp.int32)[None, None, None], 0), axis=(2, 3)
    )
    far = wide * tall * CAP
    remote_at = ((holder % wide) * tall + holder // wide) * CAP + slot
    position = jnp.where(holder == me, far + local_of, remote_at)
    key_pos = key_positions(late_chosen)
    facts = jnp.stack([me * rows, live_length[0], 2 * parity]).astype(jnp.int32)

    outgoing = pick_blocks(column_blocks, asked, per_dev)
    incoming = lax.all_to_all(outgoing, "kv_1", split_axis=0, concat_axis=0, tiled=True)
    queries = project_queries(tokens, q_pieces, outgoing[0, 0, :16, :HD])
    attended = attend(
        queries,
        incoming.reshape(far, BLOCK, paired.shape[1]),
        local_blocks,
        position,
        key_pos,
        facts,
    )
    other = from_ahead(attended, "tp", 1)
    out_full = whole_rows(o_pieces, y_at, queries[:16, :HD])
    out_full = out_full.reshape(-1, out_full.shape[-1])
    return mix(attended, other, out_full, lax.axis_index("tp"))


def solution(mesh):
    split = Mesh(
        mesh.devices.reshape(mesh.shape["dp"], 16, 4, mesh.shape["tp"]),
        ("dp", "kv_0", "kv_1", "tp"),
    )
    placed = (
        P(DP_KV, None),
        P(KV, "tp"),
        P(KV, "tp"),
        P(KV, "tp"),
        P(KV, "tp"),
        P(DP_KV, None),
        P("dp"),
    )

    return jax.shard_map(
        body, mesh=split, in_specs=placed, out_specs=P(DP_KV, "tp"), check_vma=False
    )
```

```python
import jax
import jax.numpy as jnp
from jax import lax
from jax.experimental import pallas as pl
from jax.experimental.pallas import tpu as pltpu
from jax.sharding import Mesh
from jax.sharding import PartitionSpec as P


HD = 128
BLOCK = 32
CAP = 2
NEVER = 1 << 30
TALL = ("zh", "zl")
KV = ("zh", "zl", "y")
DP_KV = ("dp", "zh", "zl", "y")
F32 = jnp.float32
BF16 = jnp.bfloat16


def call(kernel, out_shape, *args, scratch=(), flops=0):
    spaces = [
        pl.BlockSpec(memory_space=pltpu.SMEM if a.dtype == jnp.int32 and a.ndim < 3 else pltpu.VMEM)
        for a in args
    ]
    return pl.pallas_call(
        kernel,
        out_shape=out_shape,
        in_specs=spaces,
        out_specs=jax.tree.map(lambda _: pl.BlockSpec(memory_space=pltpu.VMEM), out_shape),
        scratch_shapes=list(scratch),
        compiler_params=pltpu.CompilerParams(vmem_limit_bytes=40 << 20),
        cost_estimate=pl.CostEstimate(flops=flops, bytes_accessed=0, transcendentals=0),
    )(*args)


def copy_for_each(shard, axis):
    count = lax.axis_size(axis)
    return lax.all_to_all(
        jnp.broadcast_to(shard[None], (count, *shard.shape)), axis, 0, 0, tiled=True
    )


def from_ahead(x, axis, step):
    n = lax.axis_size(axis)
    return lax.ppermute(x, axis, [((i + step) % n, i) for i in range(n)])


def spread(x, axis):
    steps = range(1, lax.axis_size(axis))
    return [x, *(from_ahead(x, axis, s) for s in steps)]


def slots_wanted(chosen, owners, per_dev, readers):
    ids = owners[:, None] * per_dev + jnp.arange(per_dev, dtype=jnp.int32)[None, :]
    hits = chosen[:, :, None, None] == ids[None, None]
    needed = jnp.any(hits, axis=1) & (owners[None, :] != readers[:, None])[:, :, None]
    ranks = jnp.cumsum(needed.astype(jnp.int32), axis=2)
    local_ids = jnp.arange(per_dev, dtype=jnp.int32)
    lists = []
    for slot in range(CAP):
        marked = needed & (ranks == slot + 1)
        found = jnp.any(marked, axis=2)
        lists.append(jnp.where(found, jnp.sum(jnp.where(marked, local_ids, 0), axis=2), -1))
    return jnp.stack(lists, axis=2)


def pack(query_weight, key_weight, value_weight, out_weight, x_at, planes, tall):
    rows = key_weight.shape[0]
    lines, wide_out = out_weight.shape
    small = rows // planes
    groups = wide_out // planes // HD

    def kernel(x_ref, q_hbm, k_hbm, v_hbm, o_hbm, part_ref, cargo_ref, *scratch):
        held, sems = scratch[:4], scratch[4]
        copies = [
            pltpu.make_async_copy(src, dst, sems.at[i])
            for i, (src, dst) in enumerate(zip((q_hbm, k_hbm, v_hbm, o_hbm), held, strict=True))
        ]
        for copy in copies:
            copy.start()
        for copy in copies:
            copy.wait()
        q_ref, k_ref, v_ref, o_ref = held
        part_ref[:rows] = q_ref[:, pl.ds(pl.multiple_of(x_ref[0] * HD, HD), HD)]
        for i in range(groups):
            first = pl.multiple_of((x_ref[0] * groups + i) * HD, HD)
            part_ref[rows + i * lines : rows + (i + 1) * lines] = o_ref[:, pl.ds(first, HD)]
        first = pl.multiple_of(x_ref[0] * small, small)
        keys = k_ref[pl.ds(first, small)]
        values = v_ref[pl.ds(first, small)]
        for z in range(tall):
            cargo_ref[z, :small] = keys
            cargo_ref[z, small:] = values

    weights = (query_weight, key_weight, value_weight, out_weight)
    outs = (
        jax.ShapeDtypeStruct((rows + groups * lines, HD), BF16),
        jax.ShapeDtypeStruct((tall, 2 * small, HD), BF16),
    )
    return pl.pallas_call(
        kernel,
        out_shape=outs,
        in_specs=[pl.BlockSpec(memory_space=pltpu.SMEM)] + [pl.BlockSpec(memory_space=pl.ANY)] * 4,
        out_specs=(pl.BlockSpec(memory_space=pltpu.VMEM),) * 2,
        scratch_shapes=[pltpu.VMEM(w.shape, BF16) for w in weights]
        + [pltpu.SemaphoreType.DMA((4,))],
        name="pack",
    )(x_at[None], *weights)


def joined(pieces, at):
    n = len(pieces)

    def kernel(at_ref, *refs):
        for s in range(n):
            refs[-1][(at_ref[0] + s) % n] = refs[s][...]

    out = jax.ShapeDtypeStruct((n, *pieces[0].shape), BF16)
    return call(kernel, out, at[None], *pieces)


def columns_of(pieces, at, rows, notes):
    n = len(pieces)
    high, both, _ = pieces[0].shape
    tall = high * n

    def kernel(at_ref, n_ref, *refs):
        q_ref, o_ref = refs[n], refs[n + 1]
        for s in range(n):
            for h in range(high):
                z = h * n + (at_ref[0] + s) % n
                q_ref[z] = refs[s][h, :rows]
                o_ref[z] = refs[s][h, rows:]
        o_ref[tall] = jnp.zeros((both - rows, HD), BF16)
        o_ref[tall, : n_ref.shape[0]] = n_ref[...]

    outs = (
        jax.ShapeDtypeStruct((tall, rows, HD), BF16),
        jax.ShapeDtypeStruct((tall + 1, both - rows, HD), BF16),
    )
    return call(kernel, outs, at[None], notes, *pieces)


def project_pair(tokens, every):
    planes, wide, tall, both, _ = every.shape
    small = both // 2
    deep = planes * wide * small

    def kernel(t_ref, w_ref, o_ref):
        total = jnp.zeros(o_ref.shape, F32)
        for z in range(tall):
            lines = [(x, y) for y in range(wide) for x in range(planes)]
            keys = jnp.concatenate([w_ref[x, y, z, :small] for x, y in lines], axis=0)
            values = jnp.concatenate([w_ref[x, y, z, small:] for x, y in lines], axis=0)
            total += jnp.dot(
                t_ref[:, z * deep : (z + 1) * deep],
                jnp.concatenate([keys, values], axis=1),
                preferred_element_type=F32,
            )
        o_ref[...] = total.astype(BF16)

    out = jax.ShapeDtypeStruct((tokens.shape[0], 2 * HD), BF16)
    flops = 2 * tokens.size * 2 * HD
    return call(kernel, out, tokens, every, flops=flops)


def project_queries(tokens, pieces, at, tile):
    n = len(pieces)
    tall, lines, width = pieces[0].shape

    def kernel(at_ref, t_ref, *refs):
        o_ref, w_s = refs[-2], refs[-1]
        for s in range(n):
            w_s[:, (at_ref[0] + s) % n] = refs[s][...]
        o_ref[...] = jnp.dot(
            t_ref[...], w_s[...].reshape(tall * n * lines, width), preferred_element_type=F32
        ).astype(BF16)

    return call(
        kernel,
        jax.ShapeDtypeStruct((tokens.shape[0], width), BF16),
        at[None],
        tokens,
        *pieces,
        tile,
        scratch=(pltpu.VMEM((tall, n, lines, width), BF16),),
        flops=2 * tokens.size * width,
    )


def full_columns(pieces, at, lines):
    n = len(pieces)
    tall, held, _ = pieces[0].shape
    groups = held // lines

    def kernel(at_ref, *refs):
        for s in range(n):
            for i in range(groups):
                first = pl.multiple_of((((at_ref[0] + s) % n) * groups + i) * HD, HD)
                refs[n][:, :, pl.ds(first, HD)] = refs[s][:, i * lines : (i + 1) * lines]

    out = jax.ShapeDtypeStruct((tall, lines, n * groups * HD), BF16)
    return call(kernel, out, at[None], *pieces)


def full_rows(pieces, at, lines):
    n = len(pieces)
    tall, held = pieces[0].shape[0] - 1, pieces[0].shape[1]
    groups = held // lines

    def kernel(at_ref, *refs):
        for s in range(n):
            y = (at_ref[0] + s) % n
            for i in range(groups):
                cut = refs[s][:tall, i * lines : (i + 1) * lines]
                refs[-1][:, y, :, i * HD : (i + 1) * HD] = cut

    out = jax.ShapeDtypeStruct((tall, n, lines, groups * HD), BF16)
    return call(kernel, out, at[None], *pieces)


def key_positions(chosen):
    per_dev, nsel = chosen.shape

    def kernel(c_ref, o_ref):
        lane = lax.broadcasted_iota(jnp.int32, (1, nsel * BLOCK), 1)
        for j in range(per_dev):
            row = jnp.zeros((1, nsel * BLOCK), jnp.int32)
            for n in range(nsel):
                first = jnp.where(c_ref[j, n] >= 0, c_ref[j, n] * BLOCK, NEVER)
                row = jnp.where(lane // BLOCK == n, first, row)
            o_ref[j] = row + lane % BLOCK

    out = jax.ShapeDtypeStruct((per_dev, 1, nsel * BLOCK), jnp.int32)
    return call(kernel, out, chosen)


def pick_blocks(blocks, asked, at):
    wide, count = asked.shape

    def kernel(asked_ref, at_ref, b_ref, o_ref):
        for s in range(wide):
            for i in range(count):
                o_ref[(at_ref[0] + s) % wide, i] = b_ref[asked_ref[s, i]]

    out = jax.ShapeDtypeStruct((wide, count, *blocks.shape[1:]), BF16)
    return call(kernel, out, asked, at[None], blocks)


def attend(queries, incoming, local_blocks, position, key_pos, facts):
    rows, width = queries.shape
    heads = width // HD
    far = incoming.shape[0]
    per_dev, nsel = position.shape
    keys = nsel * BLOCK

    def kernel(f_ref, p_ref, q_ref, in_ref, own_ref, kp_ref, o_ref, tab, k_s, v_s):
        tab[:far] = in_ref[...]
        tab[far:] = own_ref[...]
        for j in range(per_dev):
            for n in range(nsel):
                block = tab[p_ref[j, n]]
                k_s[j % 2, n * BLOCK : (n + 1) * BLOCK] = block[:, :HD]
                v_s[j % 2, n * BLOCK : (n + 1) * BLOCK] = block[:, HD:]
            mine = slice(j * BLOCK, (j + 1) * BLOCK)
            q = jnp.concatenate(
                [q_ref[mine, h * HD : (h + 1) * HD] for h in range(heads)], axis=0
            )
            scores = lax.dot_general(
                q, k_s[j % 2], (((1,), (1,)), ((), ())), preferred_element_type=F32
            ) * HD ** (-0.5)
            line = lax.broadcasted_iota(jnp.int32, (heads * BLOCK, 1), 0) % BLOCK
            at = f_ref[0] + j * BLOCK + line
            masked = jnp.where(kp_ref[j] <= at, scores, -jnp.inf)
            top = jnp.max(masked, axis=1, keepdims=True)
            weights = jnp.exp(masked - top)
            total = jnp.sum(weights, axis=1, keepdims=True)
            summed = jnp.dot(weights.astype(BF16), v_s[j % 2], preferred_element_type=F32)
            result = jnp.where(at < f_ref[1], summed / total, 0.0).astype(BF16)
            for h in range(heads):
                o_ref[mine, h * HD : (h + 1) * HD] = result[h * BLOCK : (h + 1) * BLOCK]

    return call(
        kernel,
        jax.ShapeDtypeStruct((rows, width), BF16),
        facts,
        position,
        queries,
        incoming,
        local_blocks,
        key_pos,
        scratch=(
            pltpu.VMEM((far + per_dev, BLOCK, 2 * HD), BF16),
            pltpu.VMEM((2, keys, HD), BF16),
            pltpu.VMEM((2, keys, HD), BF16),
        ),
        flops=4 * rows * keys * width,
    )


def mix(mine, other, pieces, places):
    n = len(pieces)
    rows, width = pieces[0].shape
    half = rows // 2

    def kernel(p_ref, m_ref, t_ref, *refs):
        for s in range(n):
            first = pl.multiple_of(((p_ref[0] + s) % n) * width, width)
            refs[n][:, pl.ds(first, width)] = (
                jnp.dot(
                    m_ref[...], refs[s][pl.ds(p_ref[1] * half, half)], preferred_element_type=F32
                )
                + jnp.dot(
                    t_ref[...],
                    refs[s][pl.ds((1 - p_ref[1]) * half, half)],
                    preferred_element_type=F32,
                )
            ).astype(BF16)

    out = jax.ShapeDtypeStruct((mine.shape[0], n * width), BF16)
    flops = 4 * mine.size * n * width
    return call(kernel, out, places, mine, other, *pieces, flops=flops)


def body(tokens, query_weight, key_weight, value_weight, out_weight, chosen, live_length):
    rows = tokens.shape[0]
    per_dev = rows // BLOCK
    planes, high, low, wide = (lax.axis_size(a) for a in ("dp", "zh", "zl", "y"))
    x_at, h_at, l_at, y_at = (lax.axis_index(a) for a in ("dp", "zh", "zl", "y"))
    tall = high * low
    owners = tall * wide
    me = lax.axis_index(KV)

    part, cargo = pack(query_weight, key_weight, value_weight, out_weight, x_at, planes, tall)
    column = lax.all_to_all(cargo, TALL, 0, 0, tiled=True)
    parts = spread(part, "zh")
    every = copy_for_each(column, ("dp", "y"))
    every = every.reshape(planes, wide, tall, cargo.shape[1], HD)
    parts = spread(joined(parts, h_at), "zl")
    paired = project_pair(tokens, every)
    local_blocks = paired.reshape(per_dev, BLOCK, paired.shape[1])
    column_blocks = lax.all_gather(local_blocks, TALL, axis=0, tiled=True)

    notes = jnp.stack([chosen // per_dev, chosen % per_dev]).reshape(2, -1)
    notes = jnp.pad(notes.astype(BF16), ((0, 14), (0, 0)))
    lines = query_weight.shape[0]
    q_small, o_small = columns_of(parts, l_at, lines, notes)
    q_pieces = spread(q_small, "dp")
    o_pieces = spread(o_small, "y")
    q_pieces = spread(full_columns(q_pieces, x_at, lines), "y")
    heard = jnp.stack([p[tall, :2] for p in o_pieces]).astype(jnp.int32)
    mates = heard[:, 0] * per_dev + heard[:, 1]
    o_tall = full_rows(o_pieces, y_at, out_weight.shape[0])
    o_pieces = spread(o_tall.reshape(-1, o_tall.shape[-1]), "dp")

    key_pos = key_positions(chosen)

    mates, chosen = lax.optimization_barrier((mates, chosen))
    depth = jnp.arange(tall, dtype=jnp.int32)
    readers = (h_at * low + l_at) * wide + (y_at + jnp.arange(wide, dtype=jnp.int32)) % wide
    asked = slots_wanted(mates, depth * wide + y_at, per_dev, readers)
    asked = jnp.maximum(asked, 0) + (depth * per_dev)[None, :, None]
    outgoing = pick_blocks(column_blocks, asked.reshape(wide, tall * CAP), y_at)
    incoming = lax.all_to_all(outgoing, "y", split_axis=0, concat_axis=0, tiled=True)

    safe = jnp.maximum(chosen, 0)
    wanted = slots_wanted(
        chosen.reshape(1, -1), jnp.arange(owners, dtype=jnp.int32), per_dev, me[None]
    )[0]
    holder = safe // per_dev
    local_of = safe % per_dev
    match = (wanted[None, None, :, :] == local_of[:, :, None, None]) & (
        jnp.arange(owners, dtype=jnp.int32)[None, None, :, None] == holder[:, :, None, None]
    )
    slot = jnp.sum(
        jnp.where(match, jnp.arange(CAP, dtype=jnp.int32)[None, None, None], 0), axis=(2, 3)
    )
    far = owners * CAP
    remote_at = ((holder % wide) * tall + holder // wide) * CAP + slot
    position = jnp.where(holder == me, far + local_of, remote_at)
    facts = jnp.stack([me * rows, live_length[0]]).astype(jnp.int32)

    queries = project_queries(tokens, q_pieces, y_at, outgoing[0, 0, :16, :HD])
    attended = attend(
        queries,
        incoming.reshape(far, BLOCK, paired.shape[1]),
        local_blocks,
        position,
        key_pos,
        facts,
    )
    other = from_ahead(attended, "tp", 1)
    return mix(attended, other, o_pieces, jnp.stack([x_at, lax.axis_index("tp")]))


def solution(mesh):
    split = Mesh(
        mesh.devices.reshape(mesh.shape["dp"], 4, 4, 4, mesh.shape["tp"]),
        ("dp", "zh", "zl", "y", "tp"),
    )
    placed = (
        P(DP_KV, None),
        P(KV, "tp"),
        P(KV, "tp"),
        P(KV, "tp"),
        P(KV, "tp"),
        P(DP_KV, None),
        P("dp"),
    )

    return jax.shard_map(
        body, mesh=split, in_specs=placed, out_specs=P(DP_KV, "tp"), check_vma=False
    )
```

```python
import jax
import jax.numpy as jnp
from jax import lax
from jax.experimental import pallas as pl
from jax.experimental.pallas import tpu as pltpu
from jax.sharding import Mesh
from jax.sharding import PartitionSpec as P


HD = 128
BLOCK = 32
CAP = 2
NEVER = 1 << 30
TALL = ("zh", "zl")
KV = ("zh", "zl", "y")
DP_KV = ("dp", "zh", "zl", "y")
F32 = jnp.float32
BF16 = jnp.bfloat16


def call(kernel, out_shape, *args, scratch=(), flops=0):
    spaces = [
        pl.BlockSpec(memory_space=pltpu.SMEM if a.dtype == jnp.int32 and a.ndim < 3 else pltpu.VMEM)
        for a in args
    ]
    return pl.pallas_call(
        kernel,
        out_shape=out_shape,
        in_specs=spaces,
        out_specs=jax.tree.map(lambda _: pl.BlockSpec(memory_space=pltpu.VMEM), out_shape),
        scratch_shapes=list(scratch),
        compiler_params=pltpu.CompilerParams(vmem_limit_bytes=40 << 20),
        cost_estimate=pl.CostEstimate(flops=flops, bytes_accessed=0, transcendentals=0),
    )(*args)


def copy_for_each(shard, axis):
    count = lax.axis_size(axis)
    return lax.all_to_all(
        jnp.broadcast_to(shard[None], (count, *shard.shape)), axis, 0, 0, tiled=True
    )


def from_ahead(x, axis, step):
    n = lax.axis_size(axis)
    return lax.ppermute(x, axis, [((i + step) % n, i) for i in range(n)])


def spread(x, axis):
    steps = range(1, lax.axis_size(axis))
    return [x, *(from_ahead(x, axis, s) for s in steps)]


def slots_wanted(chosen, owners, per_dev, readers):
    ids = owners[:, None] * per_dev + jnp.arange(per_dev, dtype=jnp.int32)[None, :]
    hits = chosen[:, :, None, None] == ids[None, None]
    needed = jnp.any(hits, axis=1) & (owners[None, :] != readers[:, None])[:, :, None]
    ranks = jnp.cumsum(needed.astype(jnp.int32), axis=2)
    local_ids = jnp.arange(per_dev, dtype=jnp.int32)
    lists = []
    for slot in range(CAP):
        marked = needed & (ranks == slot + 1)
        found = jnp.any(marked, axis=2)
        lists.append(jnp.where(found, jnp.sum(jnp.where(marked, local_ids, 0), axis=2), -1))
    return jnp.stack(lists, axis=2)


def pack(query_weight, key_weight, value_weight, out_weight, x_at, planes, tall):
    rows = key_weight.shape[0]
    lines, wide_out = out_weight.shape
    small = rows // planes
    groups = wide_out // planes // HD

    def kernel(x_ref, q_hbm, k_hbm, v_hbm, o_hbm, part_ref, cargo_ref, *scratch):
        held, sems = scratch[:4], scratch[4]
        copies = [
            pltpu.make_async_copy(src, dst, sems.at[i])
            for i, (src, dst) in enumerate(zip((q_hbm, k_hbm, v_hbm, o_hbm), held, strict=True))
        ]
        for copy in copies:
            copy.start()
        for copy in copies:
            copy.wait()
        q_ref, k_ref, v_ref, o_ref = held
        part_ref[:rows] = q_ref[:, pl.ds(pl.multiple_of(x_ref[0] * HD, HD), HD)]
        for i in range(groups):
            first = pl.multiple_of((x_ref[0] * groups + i) * HD, HD)
            part_ref[rows + i * lines : rows + (i + 1) * lines] = o_ref[:, pl.ds(first, HD)]
        first = pl.multiple_of(x_ref[0] * small, small)
        keys = k_ref[pl.ds(first, small)]
        values = v_ref[pl.ds(first, small)]
        for z in range(tall):
            cargo_ref[z, :small] = keys
            cargo_ref[z, small:] = values

    weights = (query_weight, key_weight, value_weight, out_weight)
    outs = (
        jax.ShapeDtypeStruct((rows + groups * lines, HD), BF16),
        jax.ShapeDtypeStruct((tall, 2 * small, HD), BF16),
    )
    return pl.pallas_call(
        kernel,
        out_shape=outs,
        in_specs=[pl.BlockSpec(memory_space=pltpu.SMEM)] + [pl.BlockSpec(memory_space=pl.ANY)] * 4,
        out_specs=(pl.BlockSpec(memory_space=pltpu.VMEM),) * 2,
        scratch_shapes=[pltpu.VMEM(w.shape, BF16) for w in weights]
        + [pltpu.SemaphoreType.DMA((4,))],
        name="pack",
    )(x_at[None], *weights)


def joined(pieces, at):
    n = len(pieces)

    def kernel(at_ref, *refs):
        for s in range(n):
            refs[-1][(at_ref[0] + s) % n] = refs[s][...]

    out = jax.ShapeDtypeStruct((n, *pieces[0].shape), BF16)
    return call(kernel, out, at[None], *pieces)


def columns_of(pieces, at, rows, notes):
    n = len(pieces)
    high, both, _ = pieces[0].shape
    tall = high * n

    def kernel(at_ref, n_ref, *refs):
        q_ref, o_ref = refs[n], refs[n + 1]
        for s in range(n):
            for h in range(high):
                z = h * n + (at_ref[0] + s) % n
                q_ref[z] = refs[s][h, :rows]
                o_ref[z] = refs[s][h, rows:]
        o_ref[tall] = jnp.zeros((both - rows, HD), BF16)
        o_ref[tall, : n_ref.shape[0]] = n_ref[...]

    outs = (
        jax.ShapeDtypeStruct((tall, rows, HD), BF16),
        jax.ShapeDtypeStruct((tall + 1, both - rows, HD), BF16),
    )
    return call(kernel, outs, at[None], notes, *pieces)


def project_pair(tokens, every):
    planes, wide, tall, both, _ = every.shape
    small = both // 2
    deep = planes * wide * small

    chunk = 4

    def kernel(t_ref, w_hbm, o_ref, w_ref, sems):
        copies = [
            pltpu.make_async_copy(
                w_hbm.at[:, :, pl.ds(i * chunk, chunk)], w_ref.at[i], sems.at[i]
            )
            for i in range(tall // chunk)
        ]
        for copy in copies:
            copy.start()
        total = jnp.zeros(o_ref.shape, F32)
        lines = [(x, y) for y in range(wide) for x in range(planes)]
        for z in range(tall):
            i, j = z // chunk, z % chunk
            if j == 0:
                copies[i].wait()
            keys = jnp.concatenate([w_ref[i, x, y, j, :small] for x, y in lines], axis=0)
            values = jnp.concatenate([w_ref[i, x, y, j, small:] for x, y in lines], axis=0)
            total += jnp.dot(
                t_ref[:, z * deep : (z + 1) * deep],
                jnp.concatenate([keys, values], axis=1),
                preferred_element_type=F32,
            )
        o_ref[...] = total.astype(BF16)

    return pl.pallas_call(
        kernel,
        out_shape=jax.ShapeDtypeStruct((tokens.shape[0], 2 * HD), BF16),
        in_specs=[pl.BlockSpec(memory_space=pltpu.VMEM), pl.BlockSpec(memory_space=pl.ANY)],
        out_specs=pl.BlockSpec(memory_space=pltpu.VMEM),
        scratch_shapes=[
            pltpu.VMEM((tall // chunk, planes, wide, chunk, both, HD), BF16),
            pltpu.SemaphoreType.DMA((tall // chunk,)),
        ],
        compiler_params=pltpu.CompilerParams(vmem_limit_bytes=40 << 20),
        cost_estimate=pl.CostEstimate(
            flops=4 * tokens.size * HD, bytes_accessed=0, transcendentals=0
        ),
        name="project_pair",
    )(tokens, every)


def project_queries(tokens, pieces, at, tile):
    n = len(pieces)
    tall, lines, width = pieces[0].shape

    def kernel(at_ref, t_ref, *refs):
        o_ref, w_s = refs[-2], refs[-1]
        for s in range(n):
            w_s[:, (at_ref[0] + s) % n] = refs[s][...]
        o_ref[...] = jnp.dot(
            t_ref[...], w_s[...].reshape(tall * n * lines, width), preferred_element_type=F32
        ).astype(BF16)

    return call(
        kernel,
        jax.ShapeDtypeStruct((tokens.shape[0], width), BF16),
        at[None],
        tokens,
        *pieces,
        tile,
        scratch=(pltpu.VMEM((tall, n, lines, width), BF16),),
        flops=2 * tokens.size * width,
    )


def full_columns(pieces, at, lines):
    n = len(pieces)
    tall, held, _ = pieces[0].shape
    groups = held // lines

    def kernel(at_ref, *refs):
        for s in range(n):
            for i in range(groups):
                first = pl.multiple_of((((at_ref[0] + s) % n) * groups + i) * HD, HD)
                refs[n][:, :, pl.ds(first, HD)] = refs[s][:, i * lines : (i + 1) * lines]

    out = jax.ShapeDtypeStruct((tall, lines, n * groups * HD), BF16)
    return call(kernel, out, at[None], *pieces)


def full_rows(pieces, at, lines):
    n = len(pieces)
    tall, held = pieces[0].shape[0] - 1, pieces[0].shape[1]
    groups = held // lines

    def kernel(at_ref, *refs):
        for s in range(n):
            y = (at_ref[0] + s) % n
            for i in range(groups):
                cut = refs[s][:tall, i * lines : (i + 1) * lines]
                refs[-1][:, y, :, i * HD : (i + 1) * HD] = cut

    out = jax.ShapeDtypeStruct((tall, n, lines, groups * HD), BF16)
    return call(kernel, out, at[None], *pieces)


def key_positions(chosen):
    per_dev, nsel = chosen.shape

    def kernel(c_ref, o_ref):
        lane = lax.broadcasted_iota(jnp.int32, (1, nsel * BLOCK), 1)
        for j in range(per_dev):
            row = jnp.zeros((1, nsel * BLOCK), jnp.int32)
            for n in range(nsel):
                first = jnp.where(c_ref[j, n] >= 0, c_ref[j, n] * BLOCK, NEVER)
                row = jnp.where(lane // BLOCK == n, first, row)
            o_ref[j] = row + lane % BLOCK

    out = jax.ShapeDtypeStruct((per_dev, 1, nsel * BLOCK), jnp.int32)
    return call(kernel, out, chosen)


def pick_blocks(blocks, asked, at):
    wide, count = asked.shape

    def kernel(asked_ref, at_ref, b_ref, o_ref):
        for s in range(wide):
            for i in range(count):
                o_ref[(at_ref[0] + s) % wide, i] = b_ref[asked_ref[s, i]]

    out = jax.ShapeDtypeStruct((wide, count, *blocks.shape[1:]), BF16)
    return call(kernel, out, asked, at[None], blocks)


def attend(queries, incoming, local_blocks, position, key_pos, facts):
    rows, width = queries.shape
    heads = width // HD
    far = incoming.shape[0]
    per_dev, nsel = position.shape
    keys = nsel * BLOCK

    def kernel(f_ref, p_ref, q_ref, in_ref, own_ref, kp_ref, o_ref, tab, k_s, v_s):
        tab[:far] = in_ref[...]
        tab[far:] = own_ref[...]
        for j in range(per_dev):
            for n in range(nsel):
                block = tab[p_ref[j, n]]
                k_s[j % 2, n * BLOCK : (n + 1) * BLOCK] = block[:, :HD]
                v_s[j % 2, n * BLOCK : (n + 1) * BLOCK] = block[:, HD:]
            mine = slice(j * BLOCK, (j + 1) * BLOCK)
            q = jnp.concatenate(
                [q_ref[mine, h * HD : (h + 1) * HD] for h in range(heads)], axis=0
            )
            scores = lax.dot_general(
                q, k_s[j % 2], (((1,), (1,)), ((), ())), preferred_element_type=F32
            ) * HD ** (-0.5)
            line = lax.broadcasted_iota(jnp.int32, (heads * BLOCK, 1), 0) % BLOCK
            at = f_ref[0] + j * BLOCK + line
            masked = jnp.where(kp_ref[j] <= at, scores, -jnp.inf)
            top = jnp.max(masked, axis=1, keepdims=True)
            weights = jnp.exp(masked - top)
            total = jnp.sum(weights, axis=1, keepdims=True)
            summed = jnp.dot(weights.astype(BF16), v_s[j % 2], preferred_element_type=F32)
            result = jnp.where(at < f_ref[1], summed / total, 0.0).astype(BF16)
            for h in range(heads):
                o_ref[mine, h * HD : (h + 1) * HD] = result[h * BLOCK : (h + 1) * BLOCK]

    return call(
        kernel,
        jax.ShapeDtypeStruct((rows, width), BF16),
        facts,
        position,
        queries,
        incoming,
        local_blocks,
        key_pos,
        scratch=(
            pltpu.VMEM((far + per_dev, BLOCK, 2 * HD), BF16),
            pltpu.VMEM((2, keys, HD), BF16),
            pltpu.VMEM((2, keys, HD), BF16),
        ),
        flops=4 * rows * keys * width,
    )


def mix(mine, other, pieces, places):
    n = len(pieces)
    rows, width = pieces[0].shape
    half = rows // 2

    def kernel(p_ref, m_ref, t_ref, *refs):
        o_ref, w_s, sems = refs[n:]
        copies = [pltpu.make_async_copy(refs[s], w_s.at[s], sems.at[s]) for s in range(n)]
        for copy in copies:
            copy.start()
        for s, copy in enumerate(copies):
            copy.wait()
            first = pl.multiple_of(((p_ref[0] + s) % n) * width, width)
            o_ref[:, pl.ds(first, width)] = (
                jnp.dot(
                    m_ref[...], w_s[s, pl.ds(p_ref[1] * half, half)], preferred_element_type=F32
                )
                + jnp.dot(
                    t_ref[...],
                    w_s[s, pl.ds((1 - p_ref[1]) * half, half)],
                    preferred_element_type=F32,
                )
            ).astype(BF16)

    vmem = pl.BlockSpec(memory_space=pltpu.VMEM)
    return pl.pallas_call(
        kernel,
        out_shape=jax.ShapeDtypeStruct((mine.shape[0], n * width), BF16),
        in_specs=[pl.BlockSpec(memory_space=pltpu.SMEM), vmem, vmem]
        + [pl.BlockSpec(memory_space=pl.ANY)] * n,
        out_specs=vmem,
        scratch_shapes=[pltpu.VMEM((n, rows, width), BF16), pltpu.SemaphoreType.DMA((n,))],
        compiler_params=pltpu.CompilerParams(vmem_limit_bytes=40 << 20),
        cost_estimate=pl.CostEstimate(
            flops=4 * mine.size * n * width, bytes_accessed=0, transcendentals=0
        ),
        name="mix",
    )(places, mine, other, *pieces)


def body(tokens, query_weight, key_weight, value_weight, out_weight, chosen, live_length):
    rows = tokens.shape[0]
    per_dev = rows // BLOCK
    planes, high, low, wide = (lax.axis_size(a) for a in ("dp", "zh", "zl", "y"))
    x_at, h_at, l_at, y_at = (lax.axis_index(a) for a in ("dp", "zh", "zl", "y"))
    tall = high * low
    owners = tall * wide
    me = lax.axis_index(KV)

    part, cargo = pack(query_weight, key_weight, value_weight, out_weight, x_at, planes, tall)
    column = lax.all_to_all(cargo, TALL, 0, 0, tiled=True)
    parts = spread(part, "zh")
    every = copy_for_each(column, ("dp", "y"))
    every = every.reshape(planes, wide, tall, cargo.shape[1], HD)
    parts = spread(joined(parts, h_at), "zl")
    paired = project_pair(tokens, every)
    local_blocks = paired.reshape(per_dev, BLOCK, paired.shape[1])
    column_blocks = lax.all_gather(local_blocks, TALL, axis=0, tiled=True)

    notes = jnp.stack([chosen // per_dev, chosen % per_dev]).reshape(2, -1)
    notes = jnp.pad(notes.astype(BF16), ((0, 14), (0, 0)))
    lines = query_weight.shape[0]
    q_small, o_small = columns_of(parts, l_at, lines, notes)
    q_pieces = spread(q_small, "dp")
    o_pieces = spread(o_small, "y")
    q_pieces = spread(full_columns(q_pieces, x_at, lines), "y")
    heard = jnp.stack([p[tall, :2] for p in o_pieces]).astype(jnp.int32)
    mates = heard[:, 0] * per_dev + heard[:, 1]
    o_tall = full_rows(o_pieces, y_at, out_weight.shape[0])
    o_pieces = spread(o_tall.reshape(-1, o_tall.shape[-1]), "dp")

    key_pos = key_positions(chosen)

    mates, chosen = lax.optimization_barrier((mates, chosen))
    depth = jnp.arange(tall, dtype=jnp.int32)
    readers = (h_at * low + l_at) * wide + (y_at + jnp.arange(wide, dtype=jnp.int32)) % wide
    asked = slots_wanted(mates, depth * wide + y_at, per_dev, readers)
    asked = jnp.maximum(asked, 0) + (depth * per_dev)[None, :, None]
    outgoing = pick_blocks(column_blocks, asked.reshape(wide, tall * CAP), y_at)
    incoming = lax.all_to_all(outgoing, "y", split_axis=0, concat_axis=0, tiled=True)

    safe = jnp.maximum(chosen, 0)
    wanted = slots_wanted(
        chosen.reshape(1, -1), jnp.arange(owners, dtype=jnp.int32), per_dev, me[None]
    )[0]
    holder = safe // per_dev
    local_of = safe % per_dev
    match = (wanted[None, None, :, :] == local_of[:, :, None, None]) & (
        jnp.arange(owners, dtype=jnp.int32)[None, None, :, None] == holder[:, :, None, None]
    )
    slot = jnp.sum(
        jnp.where(match, jnp.arange(CAP, dtype=jnp.int32)[None, None, None], 0), axis=(2, 3)
    )
    far = owners * CAP
    remote_at = ((holder % wide) * tall + holder // wide) * CAP + slot
    position = jnp.where(holder == me, far + local_of, remote_at)
    facts = jnp.stack([me * rows, live_length[0]]).astype(jnp.int32)

    queries = project_queries(tokens, q_pieces, y_at, outgoing[0, 0, :16, :HD])
    attended = attend(
        queries,
        incoming.reshape(far, BLOCK, paired.shape[1]),
        local_blocks,
        position,
        key_pos,
        facts,
    )
    other = from_ahead(attended, "tp", 1)
    return mix(attended, other, o_pieces, jnp.stack([x_at, lax.axis_index("tp")]))


def solution(mesh):
    split = Mesh(
        mesh.devices.reshape(mesh.shape["dp"], 4, 4, 4, mesh.shape["tp"]),
        ("dp", "zh", "zl", "y", "tp"),
    )
    placed = (
        P(DP_KV, None),
        P(KV, "tp"),
        P(KV, "tp"),
        P(KV, "tp"),
        P(KV, "tp"),
        P(DP_KV, None),
        P("dp"),
    )

    return jax.shard_map(
        body, mesh=split, in_specs=placed, out_specs=P(DP_KV, "tp"), check_vma=False
    )
```

```python
import jax
import jax.numpy as jnp
from jax import lax
from jax.experimental import pallas as pl
from jax.experimental.pallas import tpu as pltpu
from jax.sharding import Mesh
from jax.sharding import PartitionSpec as P


HD = 128
BLOCK = 32
CAP = 2
NEVER = 1 << 30
TALL = ("zh", "zl")
KV = ("zh", "zl", "y")
DP_KV = ("dp", "zh", "zl", "y")
F32 = jnp.float32
BF16 = jnp.bfloat16


def call(kernel, out_shape, *args, scratch=(), flops=0):
    spaces = [
        pl.BlockSpec(memory_space=pltpu.SMEM if a.dtype == jnp.int32 and a.ndim < 3 else pltpu.VMEM)
        for a in args
    ]
    return pl.pallas_call(
        kernel,
        out_shape=out_shape,
        in_specs=spaces,
        out_specs=jax.tree.map(lambda _: pl.BlockSpec(memory_space=pltpu.VMEM), out_shape),
        scratch_shapes=list(scratch),
        compiler_params=pltpu.CompilerParams(vmem_limit_bytes=40 << 20),
        cost_estimate=pl.CostEstimate(flops=flops, bytes_accessed=0, transcendentals=0),
    )(*args)


def copy_for_each(shard, axis):
    count = lax.axis_size(axis)
    return lax.all_to_all(
        jnp.broadcast_to(shard[None], (count, *shard.shape)), axis, 0, 0, tiled=True
    )


def from_ahead(x, axis, step):
    n = lax.axis_size(axis)
    return lax.ppermute(x, axis, [((i + step) % n, i) for i in range(n)])


def spread(x, axis):
    steps = range(1, lax.axis_size(axis))
    return [x, *(from_ahead(x, axis, s) for s in steps)]


def slots_wanted(chosen, owners, per_dev, readers):
    ids = owners[:, None] * per_dev + jnp.arange(per_dev, dtype=jnp.int32)[None, :]
    hits = chosen[:, :, None, None] == ids[None, None]
    needed = jnp.any(hits, axis=1) & (owners[None, :] != readers[:, None])[:, :, None]
    ranks = jnp.cumsum(needed.astype(jnp.int32), axis=2)
    local_ids = jnp.arange(per_dev, dtype=jnp.int32)
    lists = []
    for slot in range(CAP):
        marked = needed & (ranks == slot + 1)
        found = jnp.any(marked, axis=2)
        lists.append(jnp.where(found, jnp.sum(jnp.where(marked, local_ids, 0), axis=2), -1))
    return jnp.stack(lists, axis=2)


def pack(query_weight, key_weight, value_weight, out_weight, x_at, planes, tall):
    rows = key_weight.shape[0]
    lines, wide_out = out_weight.shape
    small = rows // planes
    groups = wide_out // planes // HD

    def kernel(x_ref, q_hbm, k_hbm, v_hbm, o_hbm, part_ref, cargo_ref, *scratch):
        held, sems = scratch[:4], scratch[4]
        copies = [
            pltpu.make_async_copy(src, dst, sems.at[i])
            for i, (src, dst) in enumerate(zip((q_hbm, k_hbm, v_hbm, o_hbm), held, strict=True))
        ]
        for copy in copies:
            copy.start()
        for copy in copies:
            copy.wait()
        q_ref, k_ref, v_ref, o_ref = held
        part_ref[:rows] = q_ref[:, pl.ds(pl.multiple_of(x_ref[0] * HD, HD), HD)]
        for i in range(groups):
            first = pl.multiple_of((x_ref[0] * groups + i) * HD, HD)
            part_ref[rows + i * lines : rows + (i + 1) * lines] = o_ref[:, pl.ds(first, HD)]
        first = pl.multiple_of(x_ref[0] * small, small)
        keys = k_ref[pl.ds(first, small)]
        values = v_ref[pl.ds(first, small)]
        for z in range(tall):
            cargo_ref[z, :small] = keys
            cargo_ref[z, small:] = values

    weights = (query_weight, key_weight, value_weight, out_weight)
    outs = (
        jax.ShapeDtypeStruct((rows + groups * lines, HD), BF16),
        jax.ShapeDtypeStruct((tall, 2 * small, HD), BF16),
    )
    return pl.pallas_call(
        kernel,
        out_shape=outs,
        in_specs=[pl.BlockSpec(memory_space=pltpu.SMEM)] + [pl.BlockSpec(memory_space=pl.ANY)] * 4,
        out_specs=(pl.BlockSpec(memory_space=pltpu.VMEM),) * 2,
        scratch_shapes=[pltpu.VMEM(w.shape, BF16) for w in weights]
        + [pltpu.SemaphoreType.DMA((4,))],
        name="pack",
    )(x_at[None], *weights)


def joined(pieces, at):
    n = len(pieces)

    def kernel(at_ref, *refs):
        for s in range(n):
            refs[-1][(at_ref[0] + s) % n] = refs[s][...]

    out = jax.ShapeDtypeStruct((n, *pieces[0].shape), BF16)
    return call(kernel, out, at[None], *pieces)


def columns_of(pieces, at, rows, notes):
    n = len(pieces)
    high, both, _ = pieces[0].shape
    tall = high * n

    def kernel(at_ref, n_ref, *refs):
        q_ref, o_ref = refs[n], refs[n + 1]
        for s in range(n):
            for h in range(high):
                z = h * n + (at_ref[0] + s) % n
                q_ref[z] = refs[s][h, :rows]
                o_ref[z] = refs[s][h, rows:]
        o_ref[tall] = jnp.zeros((both - rows, HD), BF16)
        o_ref[tall, : n_ref.shape[0]] = n_ref[...]

    outs = (
        jax.ShapeDtypeStruct((tall, rows, HD), BF16),
        jax.ShapeDtypeStruct((tall + 1, both - rows, HD), BF16),
    )
    return call(kernel, outs, at[None], notes, *pieces)


def project_pair(tokens, every):
    planes, wide, tall, both, _ = every.shape
    small = both // 2
    deep = planes * wide * small

    chunk = 4

    def kernel(t_ref, w_hbm, o_ref, w_ref, sems):
        copies = [
            pltpu.make_async_copy(
                w_hbm.at[:, :, pl.ds(i * chunk, chunk)], w_ref.at[i], sems.at[i]
            )
            for i in range(tall // chunk)
        ]
        for copy in copies:
            copy.start()
        total = jnp.zeros(o_ref.shape, F32)
        lines = [(x, y) for y in range(wide) for x in range(planes)]
        for z in range(tall):
            i, j = z // chunk, z % chunk
            if j == 0:
                copies[i].wait()
            keys = jnp.concatenate([w_ref[i, x, y, j, :small] for x, y in lines], axis=0)
            values = jnp.concatenate([w_ref[i, x, y, j, small:] for x, y in lines], axis=0)
            total += jnp.dot(
                t_ref[:, z * deep : (z + 1) * deep],
                jnp.concatenate([keys, values], axis=1),
                preferred_element_type=F32,
            )
        o_ref[...] = total.astype(BF16)

    return pl.pallas_call(
        kernel,
        out_shape=jax.ShapeDtypeStruct((tokens.shape[0], 2 * HD), BF16),
        in_specs=[pl.BlockSpec(memory_space=pltpu.VMEM), pl.BlockSpec(memory_space=pl.ANY)],
        out_specs=pl.BlockSpec(memory_space=pltpu.VMEM),
        scratch_shapes=[
            pltpu.VMEM((tall // chunk, planes, wide, chunk, both, HD), BF16),
            pltpu.SemaphoreType.DMA((tall // chunk,)),
        ],
        compiler_params=pltpu.CompilerParams(vmem_limit_bytes=40 << 20),
        cost_estimate=pl.CostEstimate(
            flops=4 * tokens.size * HD, bytes_accessed=0, transcendentals=0
        ),
        name="project_pair",
    )(tokens, every)


def project_queries(tokens, pieces, at, tile):
    n = len(pieces)
    tall, lines, width = pieces[0].shape

    def kernel(at_ref, t_ref, *refs):
        o_ref, w_s = refs[-2], refs[-1]
        for s in range(n):
            w_s[:, (at_ref[0] + s) % n] = refs[s][...]
        o_ref[...] = jnp.dot(
            t_ref[...], w_s[...].reshape(tall * n * lines, width), preferred_element_type=F32
        ).astype(BF16)

    return call(
        kernel,
        jax.ShapeDtypeStruct((tokens.shape[0], width), BF16),
        at[None],
        tokens,
        *pieces,
        tile,
        scratch=(pltpu.VMEM((tall, n, lines, width), BF16),),
        flops=2 * tokens.size * width,
    )


def full_columns(pieces, at, lines):
    n = len(pieces)
    tall, held, _ = pieces[0].shape
    groups = held // lines

    def kernel(at_ref, *refs):
        for s in range(n):
            for i in range(groups):
                first = pl.multiple_of((((at_ref[0] + s) % n) * groups + i) * HD, HD)
                refs[n][:, :, pl.ds(first, HD)] = refs[s][:, i * lines : (i + 1) * lines]

    out = jax.ShapeDtypeStruct((tall, lines, n * groups * HD), BF16)
    return call(kernel, out, at[None], *pieces)


def full_rows(pieces, at, lines):
    n = len(pieces)
    tall, held = pieces[0].shape[0] - 1, pieces[0].shape[1]
    groups = held // lines

    def kernel(at_ref, *refs):
        for s in range(n):
            y = (at_ref[0] + s) % n
            for i in range(groups):
                cut = refs[s][:tall, i * lines : (i + 1) * lines]
                refs[-1][:, y, :, i * HD : (i + 1) * HD] = cut

    out = jax.ShapeDtypeStruct((tall, n, lines, groups * HD), BF16)
    return call(kernel, out, at[None], *pieces)


def key_positions(chosen):
    per_dev, nsel = chosen.shape

    def kernel(c_ref, o_ref):
        lane = lax.broadcasted_iota(jnp.int32, (1, nsel * BLOCK), 1)
        for j in range(per_dev):
            row = jnp.zeros((1, nsel * BLOCK), jnp.int32)
            for n in range(nsel):
                first = jnp.where(c_ref[j, n] >= 0, c_ref[j, n] * BLOCK, NEVER)
                row = jnp.where(lane // BLOCK == n, first, row)
            o_ref[j] = row + lane % BLOCK

    out = jax.ShapeDtypeStruct((per_dev, 1, nsel * BLOCK), jnp.int32)
    return call(kernel, out, chosen)


def pick_blocks(blocks, asked, at):
    wide, count = asked.shape

    def kernel(asked_ref, at_ref, b_ref, o_ref):
        for s in range(wide):
            for i in range(count):
                o_ref[(at_ref[0] + s) % wide, i] = b_ref[asked_ref[s, i]]

    out = jax.ShapeDtypeStruct((wide, count, *blocks.shape[1:]), BF16)
    return call(kernel, out, asked, at[None], blocks)


def attend(queries, incoming, local_blocks, position, key_pos, facts, tile):
    rows, width = queries.shape
    heads = width // HD
    far = incoming.shape[0]
    per_dev, nsel = position.shape
    keys = nsel * BLOCK

    def kernel(f_ref, p_ref, q_ref, in_ref, own_ref, kp_ref, tile_ref, o_ref, tab, k_s, v_s):
        tab[:far] = in_ref[...]
        tab[far:] = own_ref[...]
        for j in range(per_dev):
            for n in range(nsel):
                block = tab[p_ref[j, n]]
                k_s[j % 2, n * BLOCK : (n + 1) * BLOCK] = block[:, :HD]
                v_s[j % 2, n * BLOCK : (n + 1) * BLOCK] = block[:, HD:]
            mine = slice(j * BLOCK, (j + 1) * BLOCK)
            q = jnp.concatenate(
                [q_ref[mine, h * HD : (h + 1) * HD] for h in range(heads)], axis=0
            )
            scores = lax.dot_general(
                q, k_s[j % 2], (((1,), (1,)), ((), ())), preferred_element_type=F32
            ) * HD ** (-0.5)
            line = lax.broadcasted_iota(jnp.int32, (heads * BLOCK, 1), 0) % BLOCK
            at = f_ref[0] + j * BLOCK + line
            masked = jnp.where(kp_ref[j] <= at, scores, -jnp.inf)
            top = jnp.max(masked, axis=1, keepdims=True)
            weights = jnp.exp(masked - top)
            total = jnp.sum(weights, axis=1, keepdims=True)
            summed = jnp.dot(weights.astype(BF16), v_s[j % 2], preferred_element_type=F32)
            result = jnp.where(at < f_ref[1], summed / total, 0.0).astype(BF16)
            for h in range(heads):
                o_ref[mine, h * HD : (h + 1) * HD] = result[h * BLOCK : (h + 1) * BLOCK]

    return call(
        kernel,
        jax.ShapeDtypeStruct((rows, width), BF16),
        facts,
        position,
        queries,
        incoming,
        local_blocks,
        key_pos,
        tile,
        scratch=(
            pltpu.VMEM((far + per_dev, BLOCK, 2 * HD), BF16),
            pltpu.VMEM((2, keys, HD), BF16),
            pltpu.VMEM((2, keys, HD), BF16),
        ),
        flops=4 * rows * keys * width,
    )


def staged(pieces, tile):
    n = len(pieces)

    def kernel(*refs):
        for s in range(n):
            refs[-1][s] = refs[s][...]

    out = jax.ShapeDtypeStruct((n, *pieces[0].shape), BF16)
    return call(kernel, out, *pieces, tile)


def mix(mine, other, weight, places):
    n, rows, width = weight.shape
    half = rows // 2

    def kernel(p_ref, m_ref, t_ref, w_ref, o_ref):
        for s in range(n):
            first = pl.multiple_of(((p_ref[0] + s) % n) * width, width)
            o_ref[:, pl.ds(first, width)] = (
                jnp.dot(
                    m_ref[...], w_ref[s, pl.ds(p_ref[1] * half, half)], preferred_element_type=F32
                )
                + jnp.dot(
                    t_ref[...],
                    w_ref[s, pl.ds((1 - p_ref[1]) * half, half)],
                    preferred_element_type=F32,
                )
            ).astype(BF16)

    out = jax.ShapeDtypeStruct((mine.shape[0], n * width), BF16)
    flops = 4 * mine.size * n * width
    return pl.pallas_call(
        kernel,
        out_shape=out,
        in_specs=[pl.BlockSpec(memory_space=pltpu.SMEM)]
        + [pl.BlockSpec(memory_space=pltpu.VMEM)] * 3,
        out_specs=pl.BlockSpec(memory_space=pltpu.VMEM),
        compiler_params=pltpu.CompilerParams(vmem_limit_bytes=40 << 20),
        cost_estimate=pl.CostEstimate(flops=flops, bytes_accessed=0, transcendentals=0),
        name="mix",
    )(places, mine, other, weight)


def body(tokens, query_weight, key_weight, value_weight, out_weight, chosen, live_length):
    rows = tokens.shape[0]
    per_dev = rows // BLOCK
    planes, high, low, wide = (lax.axis_size(a) for a in ("dp", "zh", "zl", "y"))
    x_at, h_at, l_at, y_at = (lax.axis_index(a) for a in ("dp", "zh", "zl", "y"))
    tall = high * low
    owners = tall * wide
    me = lax.axis_index(KV)

    part, cargo = pack(query_weight, key_weight, value_weight, out_weight, x_at, planes, tall)
    column = lax.all_to_all(cargo, TALL, 0, 0, tiled=True)
    parts = spread(part, "zh")
    every = copy_for_each(column, ("dp", "y"))
    every = every.reshape(planes, wide, tall, cargo.shape[1], HD)
    parts = spread(joined(parts, h_at), "zl")
    paired = project_pair(tokens, every)
    local_blocks = paired.reshape(per_dev, BLOCK, paired.shape[1])
    column_blocks = lax.all_gather(local_blocks, TALL, axis=0, tiled=True)

    notes = jnp.stack([chosen // per_dev, chosen % per_dev]).reshape(2, -1)
    notes = jnp.pad(notes.astype(BF16), ((0, 14), (0, 0)))
    lines = query_weight.shape[0]
    q_small, o_small = columns_of(parts, l_at, lines, notes)
    q_pieces = spread(q_small, "dp")
    o_pieces = spread(o_small, "y")
    q_pieces = spread(full_columns(q_pieces, x_at, lines), "y")
    heard = jnp.stack([p[tall, :2] for p in o_pieces]).astype(jnp.int32)
    mates = heard[:, 0] * per_dev + heard[:, 1]
    o_tall = full_rows(o_pieces, y_at, out_weight.shape[0])
    o_pieces = spread(o_tall.reshape(-1, o_tall.shape[-1]), "dp")

    key_pos = key_positions(chosen)

    mates, chosen = lax.optimization_barrier((mates, chosen))
    depth = jnp.arange(tall, dtype=jnp.int32)
    readers = (h_at * low + l_at) * wide + (y_at + jnp.arange(wide, dtype=jnp.int32)) % wide
    asked = slots_wanted(mates, depth * wide + y_at, per_dev, readers)
    asked = jnp.maximum(asked, 0) + (depth * per_dev)[None, :, None]
    outgoing = pick_blocks(column_blocks, asked.reshape(wide, tall * CAP), y_at)
    incoming = lax.all_to_all(outgoing, "y", split_axis=0, concat_axis=0, tiled=True)

    safe = jnp.maximum(chosen, 0)
    wanted = slots_wanted(
        chosen.reshape(1, -1), jnp.arange(owners, dtype=jnp.int32), per_dev, me[None]
    )[0]
    holder = safe // per_dev
    local_of = safe % per_dev
    match = (wanted[None, None, :, :] == local_of[:, :, None, None]) & (
        jnp.arange(owners, dtype=jnp.int32)[None, None, :, None] == holder[:, :, None, None]
    )
    slot = jnp.sum(
        jnp.where(match, jnp.arange(CAP, dtype=jnp.int32)[None, None, None], 0), axis=(2, 3)
    )
    far = owners * CAP
    remote_at = ((holder % wide) * tall + holder // wide) * CAP + slot
    position = jnp.where(holder == me, far + local_of, remote_at)
    facts = jnp.stack([me * rows, live_length[0]]).astype(jnp.int32)

    queries = project_queries(tokens, q_pieces, y_at, outgoing[0, 0, :16, :HD])
    out_full = staged(o_pieces, queries[:16, :HD])
    attended = attend(
        queries,
        incoming.reshape(far, BLOCK, paired.shape[1]),
        local_blocks,
        position,
        key_pos,
        facts,
        out_full[0, :16, :HD],
    )
    other = from_ahead(attended, "tp", 1)
    return mix(attended, other, out_full, jnp.stack([x_at, lax.axis_index("tp")]))


def solution(mesh):
    split = Mesh(
        mesh.devices.reshape(mesh.shape["dp"], 4, 4, 4, mesh.shape["tp"]),
        ("dp", "zh", "zl", "y", "tp"),
    )
    placed = (
        P(DP_KV, None),
        P(KV, "tp"),
        P(KV, "tp"),
        P(KV, "tp"),
        P(KV, "tp"),
        P(DP_KV, None),
        P("dp"),
    )

    return jax.shard_map(
        body, mesh=split, in_specs=placed, out_specs=P(DP_KV, "tp"), check_vma=False
    )
```
